32 devices in a mesh: sp: 4 (over z), fs: 4 (over y, x), tp: 2 (over core).
Axes of the slice: x: 2, y: 2, z: 4, core: 2. Of those that a mesh axis runs over, the one named last changes fastest.
Arguments:
- tokens: bfloat16 [4096, 2048], P('sp'), may hold values from -6 to 6
- norm_gain: float32 [2048], replicated, may hold values from 0.1 to 1.9
- w_query: bfloat16 [2048, 2048], P('sp', ('fs', 'tp')), may hold values from -3.6239223 to 3.6239223
- w_key: bfloat16 [2048, 512], P('sp', ('fs', 'tp')), may hold values from -0.088388348 to 0.088388348
- w_value: bfloat16 [2048, 512], P('sp', ('fs', 'tp')), may hold values from -0.8984375 to 0.8984375
- w_conv_in: bfloat16 [2048, 2048], P('sp', ('fs', 'tp')), may hold values from -0.125 to 0.125
- w_conv_gate: bfloat16 [2048, 2048], P('sp', ('fs', 'tp')), may hold values from -0.125 to 0.125
- conv_taps: bfloat16 [3, 2048], P(None, ('fs', 'tp')), may hold values from -3.5 to 3.5
- sink_logits: float32 [32], P(('fs', 'tp')), may hold values from 2 to 6
Outputs:
- mixed: bfloat16 [4096, 2048], P('sp', ('fs', 'tp'))
- log_sums: float32 [32, 4096], P(('fs', 'tp'), 'sp')
The draws below stay inside these ranges and needn't reach their ends.
All inputs are finite; a program needn't handle non-finite values.
Results may differ from the reference program's by a relative error of at most 0.0077.
Values may be sent and summed in bfloat16 or wider, within the bound.
A program may use at most 64 MiB of HBM per device.

```python
import math
import jax
import jax.numpy as jnp
from jax import lax

HEAD_DIM = 64
KV_HEADS = 8
GROUP = 4
HEADS = 32
D = 2048
WINDOW = 128
TAPS = 3
TOKENS = 4096


def shared_key_weight(key):
    base_draw = jax.random.normal(jax.random.fold_in(key, 101), (D, KV_HEADS * HEAD_DIM), jnp.float32)
    return jnp.clip(base_draw, -4.0, 4.0) / math.sqrt(D)


def draw_w_key(key, part):
    return shared_key_weight(key).astype(jnp.bfloat16)


def draw_w_query(key, part):
    noise_part = jnp.clip(jax.random.normal(jax.random.fold_in(key, 202), (D, HEADS * HEAD_DIM), jnp.float32), -4.0, 4.0) / math.sqrt(D)
    return noise_part.astype(jnp.bfloat16)


def block_levels(rng, extent, pieces, smallest, largest):
    level, own = 1.0, jax.random.fold_in(rng, 6)
    for position, parts in pieces:
        steps = jnp.exp(jax.random.uniform(jax.random.fold_in(own, position), (parts,), jnp.float32, smallest / len(pieces), largest / len(pieces)))
        level = level * jnp.repeat(steps, extent[position] // parts).reshape([-1 if axis == position else 1 for axis in range(len(extent))])
    return level


def noise(stream_key, extent, width, limit, cuts=(), held_as=jnp.bfloat16):
    result = width * jax.random.normal(stream_key, extent, jnp.float32)
    if cuts:
        result = result * block_levels(stream_key, extent, cuts, -0.22, 0.18)
    return jnp.clip(result, -limit, limit).astype(held_as)


def setup_inputs(seed: int = 0) -> dict:
    keys = jax.random.split(jax.random.key(seed), 10)
    return {
        "tokens": noise(keys[0], (TOKENS, D), 1.0, 6.0, ((0, 4),)),
        "norm_gain": jnp.clip(1.0 + 0.18 * jax.random.normal(keys[1], (D,), jnp.float32), 0.1, 1.9),
        "w_query": draw_w_query(jax.random.fold_in(keys[9], 71), 0),
        "w_key": draw_w_key(jax.random.fold_in(keys[9], 71), 0),
        "w_value": noise(keys[4], (D, KV_HEADS * HEAD_DIM), 0.15, 0.8984375, ((0, 4), (1, 8))),
        "w_conv_in": noise(keys[5], (D, D), D ** -0.5, 0.125, ((0, 4), (1, 8))),
        "w_conv_gate": noise(keys[6], (D, D), D ** -0.5, 0.125, ((0, 4), (1, 8))),
        "conv_taps": noise(keys[7], (TAPS, D), TAPS ** -0.5, 3.5, ((1, 8),)),
        "sink_logits": jnp.clip(2.0 + 4.0 * jax.random.uniform(keys[8], (HEADS,), jnp.float32) ** block_levels(keys[8], (HEADS,), ((0, 8),), -0.2, 0.2), 2.0, 6.0),
    }


EPS = 1e-06

def attend_group(query_blocks, key_span, value_span, sink_group, in_window):
    scores = jnp.einsum('nqgd,nkd->ngqk', query_blocks.astype(jnp.float32), key_span.astype(jnp.float32)) * HEAD_DIM ** (-0.5)
    scores = jnp.where(in_window[:, None], scores, -jnp.inf)
    sink_col = sink_group[None, :, None, None]
    row_top = jnp.maximum(lax.optimization_barrier(jnp.max(scores, axis=-1, keepdims=True)), sink_col)
    raised = jnp.exp(scores - row_top)
    row_sum = lax.optimization_barrier(jnp.sum(raised, axis=-1, keepdims=True)) + jnp.exp(sink_col - row_top)
    soft_weights = (raised / row_sum).astype(jnp.bfloat16)
    attended = jnp.einsum('ngqk,nkd->nqgd', soft_weights.astype(jnp.float32), value_span.astype(jnp.float32))
    return (attended, (row_top + jnp.log(row_sum))[..., 0])

def block_spans(rows_bf, blocks):
    shaped = rows_bf.reshape(blocks, WINDOW, KV_HEADS, HEAD_DIM)
    earlier = jnp.concatenate([jnp.zeros_like(shaped[:1]), shaped[:-1]], axis=0)
    return jnp.concatenate([earlier, shaped], axis=1).transpose(2, 0, 1, 3)

def reference(tokens, norm_gain, w_query, w_key, w_value, w_conv_in, w_conv_gate, conv_taps, sink_logits):
    widened = tokens.astype(jnp.float32)
    normed = (widened * lax.rsqrt(lax.optimization_barrier(jnp.mean(widened * widened, axis=-1, keepdims=True)) + EPS) * norm_gain).astype(jnp.bfloat16)
    query, key_rows, value_rows, conv_in, conv_gate = [jnp.dot(normed, weight, preferred_element_type=jnp.float32).astype(jnp.bfloat16) for weight in (w_query, w_key, w_value, w_conv_in, w_conv_gate)]
    blocks = TOKENS // WINDOW
    query_blocks = query.reshape(blocks, WINDOW, KV_HEADS, GROUP, HEAD_DIM).transpose(2, 0, 1, 3, 4)
    query_idx = jnp.arange(WINDOW)[:, None] + WINDOW
    key_idx = jnp.arange(2 * WINDOW)[None, :]
    offset_gap = query_idx - key_idx
    in_band = (offset_gap >= 0) & (offset_gap < WINDOW)
    block_idx = jnp.arange(blocks)[:, None, None]
    in_window = in_band[None] & ((block_idx > 0) | (key_idx[None] >= WINDOW))
    sink_table = sink_logits.reshape(KV_HEADS, GROUP)
    attended, log_sums = lax.map(lambda group_args: attend_group(group_args[0], group_args[1], group_args[2], group_args[3], in_window), (query_blocks, block_spans(key_rows, blocks), block_spans(value_rows, blocks), sink_table))
    attended = attended.transpose(1, 2, 0, 3, 4).reshape(TOKENS, HEADS * HEAD_DIM)
    log_sums = log_sums.transpose(0, 2, 1, 3).reshape(HEADS, TOKENS)
    padded = jnp.concatenate([jnp.zeros((TAPS - 1, D), jnp.bfloat16), conv_in], axis=0)
    conv_sum = jnp.zeros((TOKENS, D), jnp.float32)
    for tap_idx in range(TAPS):
        conv_sum = conv_sum + conv_taps[tap_idx].astype(jnp.float32) * padded[tap_idx:tap_idx + TOKENS].astype(jnp.float32)
    convolved = conv_gate.astype(jnp.float32) * conv_sum
    mixed = (attended + convolved).astype(jnp.bfloat16)
    return (mixed, log_sums)
```

```python
import functools

import jax
import jax.numpy as jnp
from jax import lax
from jax.experimental import pallas as pl
from jax.experimental.pallas import tpu as pltpu
from jax.sharding import PartitionSpec as P

HEAD_DIM = 64
WINDOW = 128
TAPS = 3
EPS = 1e-06
LANES = 128
PAD = 8
MESH = pl.DeviceIdType.MESH


def line_kernel(
    n, flip, tok_ref, gain_ref, *refs
):
    arrays = 5 if flip else 4
    shards = refs[:arrays]
    (
        taps_ref, sink_ref, mixed_ref, log_ref,
        tok, normed, kv_all, q_all, ci_all, cg_all, kv, query, attended, conv_in, gate_sum,
        tok_sem, own_sem, recv_sem, right_sem, left_sem, halo_send, halo_recv,
    ) = refs[arrays:]
    QUERY, CONV, GATE = arrays - 3, arrays - 2, arrays - 1
    me = lax.axis_index("sp")
    rows = tok.shape[0]
    depth = shards[QUERY].shape[0]
    wholes = (kv_all, kv_all, q_all, ci_all, cg_all)[5 - arrays :]
    has_left, has_right = me > 0, me < n - 1
    left, right = jnp.maximum(me - 1, 0), jnp.minimum(me + 1, n - 1)
    blocks = rows // WINDOW
    f32, bf16 = jnp.float32, jnp.bfloat16

    step_rows = rows // 4
    tok_copies = [
        pltpu.make_async_copy(
            tok_ref.at[pl.ds(i * step_rows, step_rows)], tok.at[pl.ds(i * step_rows, step_rows)], tok_sem.at[i]
        )
        for i in range(4)
    ]
    for copy in tok_copies:
        copy.start()

    def place(a, shard):
        at = pl.ds(pl.multiple_of(shard * depth, depth), depth)
        if flip and a < QUERY:
            return kv_all.at[pl.ds(a * HEAD_DIM, HEAD_DIM), at]
        return wholes[a].at[at]

    own_copies = [pltpu.make_async_copy(shards[a], place(a, me), own_sem.at[a]) for a in range(arrays)]
    for copy in own_copies:
        copy.start()

    barrier = pltpu.get_barrier_semaphore()

    @pl.when(has_left)
    def _():
        pl.semaphore_signal(barrier, inc=1, device_id={"sp": left}, device_id_type=MESH)

    @pl.when(has_right)
    def _():
        pl.semaphore_signal(barrier, inc=1, device_id={"sp": right}, device_id_type=MESH)

    pl.semaphore_wait(barrier, has_left.astype(jnp.int32) + has_right.astype(jnp.int32))

    def hop(a, shard, to_right, own=False):
        return pltpu.make_async_remote_copy(
            src_ref=shards[a] if own else place(a, shard),
            dst_ref=place(a, shard),
            send_sem=(right_sem if to_right else left_sem).at[a, shard],
            recv_sem=recv_sem.at[a, shard],
            device_id={"sp": right if to_right else left},
            device_id_type=MESH,
        )

    def send_own(a):
        @pl.when(has_right)
        def _():
            hop(a, me, True, True).start()

        @pl.when(has_left)
        def _():
            hop(a, me, False, True).start()

    def pass_on(a, first, last):
        def step(k, carry):
            @pl.when(me - k >= 0)
            def _():
                shard = me - k
                hop(a, shard, False).wait_recv()

                @pl.when(has_right)
                def _():
                    hop(a, shard, True).start()

            @pl.when(me + k < n)
            def _():
                shard = me + k
                hop(a, shard, True).wait_recv()

                @pl.when(has_left)
                def _():
                    hop(a, shard, False).start()

            return carry

        lax.fori_loop(first, last, step, 0)

    for a in range(GATE):
        send_own(a)

    norm_rows = 64
    for i in range(4):
        tok_copies[i].wait()

        @pl.loop(0, step_rows // norm_rows)
        def _(j):
            at = pl.ds(pl.multiple_of(i * step_rows + j * norm_rows, norm_rows), norm_rows)
            wide = tok[at, :].astype(f32)
            scale = lax.rsqrt(jnp.mean(wide * wide, axis=-1, keepdims=True) + EPS)
            normed[at, :] = (wide * scale * gain_ref[...]).astype(bf16)

    for copy in own_copies:
        copy.wait()

    tile = 256

    def project(a, store):
        @pl.loop(0, rows // tile)
        def _(i):
            base = pl.multiple_of(i * tile, tile)
            side = 1 if flip and a < QUERY else 0
            store(
                base,
                lax.dot_general(
                    normed[pl.ds(base, tile), :],
                    wholes[a][...],
                    (((1,), (side,)), ((), ())),
                    preferred_element_type=f32,
                ),
            )

    def halo(buffer, length, i):
        return pltpu.make_async_remote_copy(
            src_ref=buffer.at[pl.ds(rows, length)],
            dst_ref=buffer.at[pl.ds(0, length)],
            send_sem=halo_send.at[i],
            recv_sem=halo_recv.at[i],
            device_id={"sp": right},
            device_id_type=MESH,
        )

    for a in range(QUERY):
        pass_on(a, 1, n)
    send_own(GATE)

    def store_kv(base, value):
        kv[pl.ds(base + WINDOW, tile), :] = value.astype(bf16)

    project(0, store_kv)

    @pl.when(jnp.logical_not(has_left))
    def _():
        kv[pl.ds(0, WINDOW), :] = jnp.zeros((WINDOW, kv.shape[1]), bf16)
        conv_in[pl.ds(0, PAD), :] = jnp.zeros((PAD, conv_in.shape[1]), f32)

    pass_on(QUERY, 1, n)

    @pl.when(has_right)
    def _():
        halo(kv, WINDOW, 0).start()

    def store_query(base, value):
        query[pl.ds(base, tile), :] = value.astype(bf16)

    project(QUERY, store_query)

    heads = query.shape[1] // HEAD_DIM
    query_idx = lax.broadcasted_iota(jnp.int32, (WINDOW, 2 * WINDOW), 0)
    key_idx = lax.broadcasted_iota(jnp.int32, (WINDOW, 2 * WINDOW), 1)
    gap = query_idx + WINDOW - key_idx
    band = (gap >= 0) & (gap < WINDOW)
    lane = lax.broadcasted_iota(jnp.int32, (2 * WINDOW, LANES), 1)
    low = lane < HEAD_DIM
    stat_lane = lax.broadcasted_iota(jnp.int32, (WINDOW, LANES), 1)

    def attend(b, kept):
        base = pl.multiple_of(b * WINDOW, WINDOW)
        both = kv[pl.ds(base, 2 * WINDOW), :].astype(f32)
        turned = pltpu.roll(both, HEAD_DIM, 1)
        zero = jnp.zeros_like(both)
        keys = (jnp.where(low, both, zero).astype(bf16), jnp.where(low, zero, turned).astype(bf16))
        vals = (jnp.where(low, turned, zero).astype(bf16), jnp.where(low, zero, both).astype(bf16))
        stats = jnp.zeros((WINDOW, LANES), f32)
        for pair in range(heads // 2):
            cols = pl.ds(pair * LANES, LANES)
            q = query[pl.ds(base, WINDOW), cols]
            out = None
            for side in range(2):
                head = 2 * pair + side
                scores = lax.dot_general(
                    q, keys[side], (((1,), (1,)), ((), ())), preferred_element_type=f32
                ) * HEAD_DIM ** (-0.5)
                scores = jnp.where(kept, scores, -jnp.inf)
                sink = jnp.full((WINDOW, 1), sink_ref[head], f32)
                top = jnp.maximum(jnp.max(scores, axis=-1, keepdims=True), sink)
                raised = jnp.exp(scores - top)
                total = jnp.sum(raised, axis=-1, keepdims=True) + jnp.exp(sink - top)
                weights = (raised * (1.0 / total)).astype(bf16)
                part = jnp.dot(weights, vals[side], preferred_element_type=f32)
                out = part if out is None else out + part
                stats = jnp.where(stat_lane == head, top + jnp.log(total), stats)
            attended[pl.ds(base, WINDOW), cols] = out
        log_ref[:, pl.ds(base, WINDOW)] = jnp.transpose(stats)[:heads]

    def attend_range(first, last):
        @pl.loop(first, last)
        def _(b):
            attend(b, band)

    cut = [1 + (n - 1) * i // 3 for i in range(4)]
    mid = 1 + (blocks - 1) // 2
    attend_range(1, mid)
    pass_on(CONV, cut[0], cut[1])
    attend_range(mid, blocks)
    pass_on(CONV, cut[1], cut[2])

    @pl.when(has_left)
    def _():
        halo(kv, WINDOW, 0).wait_recv()

    attend(0, band & ((key_idx >= WINDOW) | has_left))
    pass_on(CONV, cut[2], cut[3])

    def store_conv(base, value):
        conv_in[pl.ds(base + PAD, tile), :] = value.astype(bf16).astype(f32)

    project(CONV, store_conv)
    early = min(2, n - 1)
    pass_on(GATE, 1, early)

    @pl.when(has_right)
    def _():
        halo(conv_in, PAD, 1).start()

    pass_on(GATE, early, n - 1)

    far = jnp.where(2 * me >= n, 0, n - 1)

    def gate_part(base, shard):
        at = pl.ds(pl.multiple_of(shard * depth, depth), depth)
        return jnp.dot(
            normed[pl.ds(base, tile), at], cg_all[at, :], preferred_element_type=f32
        )

    if flip:

        @pl.loop(0, rows // tile)
        def _(i):
            base = pl.multiple_of(i * tile, tile)
            part = gate_part(base, lax.rem(far + 1, n))
            for j in range(2, n):
                part = part + gate_part(base, lax.rem(far + j, n))
            gate_sum[pl.ds(base, tile), :] = part

    pass_on(GATE, n - 1, n)

    @pl.when(has_left)
    def _():
        halo(conv_in, PAD, 1).wait_recv()

    def store_mixed(base, value):
        gate = value.astype(bf16).astype(f32)
        taps = taps_ref[...].astype(f32)
        near = conv_in[pl.ds(base, tile + PAD), :]
        total = jnp.zeros_like(gate)
        for k in range(TAPS):
            start = PAD - TAPS + 1 + k
            total = total + taps[k : k + 1] * near[start : start + tile]
        mixed_ref[pl.ds(base, tile), :] = (attended[pl.ds(base, tile), :] + gate * total).astype(bf16)

    if flip:

        @pl.loop(0, rows // tile)
        def _(i):
            base = pl.multiple_of(i * tile, tile)
            store_mixed(base, gate_sum[pl.ds(base, tile), :] + gate_part(base, far))

    else:
        project(GATE, store_mixed)

    @pl.when(has_right)
    def _():
        halo(kv, WINDOW, 0).wait_send()
        halo(conv_in, PAD, 1).wait_send()

    for a in range(arrays):

        @pl.when(has_right)
        def _():
            @pl.loop(0, me + 1)
            def _(s):
                hop(a, s, True).wait_send()

        @pl.when(has_left)
        def _():
            @pl.loop(me, n)
            def _(s):
                hop(a, s, False).wait_send()


def paired_kernel(tok_ref, gain_ref, *refs):
    shards = refs[:5]
    (
        taps_ref, sink_ref, mixed_ref, log_ref,
        tok, normed, other, kv_all, q_all, conv_w0, conv_w1, kv, query, q_part, attended,
        conv_in0, conv_in1, gates, sums, conv_out, conv_back,
        tok_sem, own_sem, recv_sem, mate_sem, peer_sem, halo_send, halo_recv,
        x_send, x_recv, out_send, out_recv,
    ) = refs[5:]
    conv_w, conv_in = (conv_w0, conv_w1), (conv_in0, conv_in1)
    f32, bf16 = jnp.float32, jnp.bfloat16
    me, fs, tp = lax.axis_index("sp"), lax.axis_index("fs"), lax.axis_index("tp")
    low = me < 2
    end = (me == 0) | (me == 3)
    middle = jnp.logical_not(end)
    mate = me + 1 - 2 * lax.rem(me, 2)
    peer = jnp.where(end, 3 - mate, 3 - me)
    far = jnp.where(low, 3, 0)
    first = jnp.where(low, 0, 1)
    has_left, has_right = me > 0, me < 3
    right = jnp.minimum(me + 1, 3)
    across, along = fs + 1 - 2 * lax.rem(fs, 2), lax.rem(fs + 2, 4)
    diagonal = 3 - fs
    twin = 1 - tp
    rows = tok.shape[0]
    depth = shards[2].shape[0]
    blocks = rows // WINDOW
    K, V, Q, CI0, CG0, CI1, CG1 = range(7)

    parts = 8
    part_rows = rows // parts
    piece = part_rows // 2
    own_part = fs * 2 + tp

    def part_at(i):
        return lax.rem(own_part + i, parts)

    def rows_of(start, length):
        return pl.ds(pl.multiple_of(start, 16), length)

    tok_copies = []
    for i in range(parts):
        at = rows_of(part_at(i) * part_rows, part_rows)
        tok_copies.append(pltpu.make_async_copy(tok_ref.at[at], tok.at[at], tok_sem.at[i]))
    for copy in tok_copies:
        copy.start()

    def source(u):
        if u <= Q:
            return shards[u]
        half = (u - CI0) // 2
        return shards[3 + (u - CI0) % 2].at[:, pl.ds(half * LANES, LANES)]

    def place(u, shard):
        at = pl.ds(pl.multiple_of(shard * depth, depth), depth)
        if u < Q:
            return kv_all.at[pl.ds(u * HEAD_DIM, HEAD_DIM), at]
        if u == Q:
            return q_all.at[at]
        return conv_w[(u - CI0) // 2].at[at, pl.ds((u - CI0) % 2 * LANES, LANES)]

    own_copies = [pltpu.make_async_copy(source(u), place(u, me), own_sem.at[u]) for u in range(7)]
    for u in (K, V, Q):
        own_copies[u].start()

    @pl.when(middle)
    def _():
        for u in (CI0, CG0, CI1, CG1):
            own_copies[u].start()

    barrier = pltpu.get_barrier_semaphore()

    def greet(**device):
        pl.semaphore_signal(barrier, inc=1, device_id=device, device_id_type=MESH)

    greet(sp=mate)

    @pl.when(middle)
    def _():
        greet(sp=peer)
        greet(fs=across)
        greet(fs=along)
        greet(tp=twin)

    pl.semaphore_wait(barrier, jnp.where(middle, 5, 1))

    def hop(u, shard, to_mate, own=False):
        return pltpu.make_async_remote_copy(
            src_ref=source(u) if own else place(u, shard),
            dst_ref=place(u, shard),
            send_sem=(mate_sem if to_mate else peer_sem).at[u, shard],
            recv_sem=recv_sem.at[u, shard],
            device_id={"sp": mate if to_mate else peer},
            device_id_type=MESH,
        )

    def arrived(u, shard):
        hop(u, shard, True).wait_recv()

    for u in (K, V, Q):
        hop(u, me, True, True).start()

    @pl.when(middle)
    def _():
        for u in (K, V, Q):
            hop(u, me, False, True).start()

    def norm_part(i):
        tok_copies[i].wait()
        norm_rows = 64

        @pl.loop(0, part_rows // norm_rows)
        def _(j):
            at = rows_of(part_at(i) * part_rows + j * norm_rows, norm_rows)
            wide = tok[at, :].astype(f32)
            scale = lax.rsqrt(jnp.mean(wide * wide, axis=-1, keepdims=True) + EPS)
            normed[at, :] = (wide * scale * gain_ref[...]).astype(bf16)

    def piece_at(part, h):
        return rows_of(part * part_rows + h * piece, piece)

    def piece_copy(buffer, part, h, i, **device):
        at = piece_at(part, h)
        return pltpu.make_async_remote_copy(
            src_ref=buffer.at[at],
            dst_ref=other.at[at],
            send_sem=x_send.at[i],
            recv_sem=x_recv.at[part * 2 + h],
            device_id=device,
            device_id_type=MESH,
        )

    def piece_arrived(part, h):
        piece_copy(other, part, h, 0, sp=mate).wait_recv()

    across_part, along_part, diagonal_part = across * 2 + tp, along * 2 + tp, diagonal * 2 + tp
    relays = (
        (own_part, 0, ("tp", "fs_across", "fs_along")),
        (own_part, 1, ("tp", "fs_across", "fs_along")),
        (across_part, 0, ("tp", "fs_along")),
        (along_part, 0, ("tp",)),
        (across_part, 1, ("tp",)),
        (along_part, 1, ("tp", "fs_across")),
        (diagonal_part, 0, ("tp",)),
        (diagonal_part, 1, ("tp",)),
    )
    devices = {"tp": {"tp": twin}, "fs_across": {"fs": across}, "fs_along": {"fs": along}}

    def relay_copies(j):
        base = sum(len(to) for _, _, to in relays[:j])
        part, h, to = relays[j]
        return [piece_copy(other, part, h, base + i, **devices[d]) for i, d in enumerate(to)]

    def relay(j):
        piece_arrived(relays[j][0], relays[j][1])
        for copy in relay_copies(j):
            copy.start()

    norm_part(0)
    norm_part(1)

    @pl.when(end)
    def _():
        for h in range(2):
            piece_copy(normed, own_part, h, h, sp=mate).start()
        for u in (CI0, CG0, CI1, CG1):
            hop(u, me, True, True).start()

    for i in range(2, parts):
        norm_part(i)

    for u in (K, V, Q):
        own_copies[u].wait()

    for u in (K, V):
        arrived(u, mate)

        @pl.when(middle)
        def _():
            hop(u, mate, False).start()

        arrived(u, peer)

        @pl.when(middle)
        def _():
            hop(u, peer, True).start()

    arrived(Q, mate)

    @pl.when(middle)
    def _():
        hop(Q, mate, False).start()
        for u in (CI0, CG0, CI1):
            hop(u, me, False, True).start()

    arrived(Q, peer)

    @pl.when(middle)
    def _():
        hop(Q, peer, True).start()

    for u in (K, V):
        arrived(u, far)

        @pl.when(middle)
        def _():
            hop(u, far, True).start()

    tile = 256

    @pl.loop(0, rows // tile)
    def _(i):
        base = pl.multiple_of(i * tile, tile)
        kv[pl.ds(base + WINDOW, tile), :] = lax.dot_general(
            normed[pl.ds(base, tile), :], kv_all[...], (((1,), (1,)), ((), ())), preferred_element_type=f32
        ).astype(bf16)

    def halo(buffer, start, length, i):
        return pltpu.make_async_remote_copy(
            src_ref=buffer.at[pl.ds(start, length)],
            dst_ref=buffer.at[pl.ds(0, length)],
            send_sem=halo_send.at[i],
            recv_sem=halo_recv.at[i],
            device_id={"sp": right},
            device_id_type=MESH,
        )

    kv_halo = halo(kv, rows, WINDOW, 0)

    @pl.when(jnp.logical_not(has_left))
    def _():
        kv[pl.ds(0, WINDOW), :] = jnp.zeros((WINDOW, kv.shape[1]), bf16)

    early = pl.ds(pl.multiple_of(first * depth, depth), 3 * depth)
    late = pl.ds(pl.multiple_of(far * depth, depth), depth)

    @pl.loop(0, rows // tile)
    def _(i):
        at = pl.ds(pl.multiple_of(i * tile, tile), tile)
        q_part[at, :] = jnp.dot(normed[at, early], q_all[early, :], preferred_element_type=f32)

    @pl.when(has_right)
    def _():
        kv_halo.start()

    @pl.when(middle)
    def _():
        relay(0)

    arrived(Q, far)

    @pl.when(middle)
    def _():
        hop(Q, far, True).start()

    @pl.loop(0, rows // tile)
    def _(i):
        at = pl.ds(pl.multiple_of(i * tile, tile), tile)
        query[at, :] = (
            q_part[at, :] + jnp.dot(normed[at, late], q_all[late, :], preferred_element_type=f32)
        ).astype(bf16)

    heads = query.shape[1] // HEAD_DIM
    query_idx = lax.broadcasted_iota(jnp.int32, (WINDOW, 2 * WINDOW), 0)
    key_idx = lax.broadcasted_iota(jnp.int32, (WINDOW, 2 * WINDOW), 1)
    gap = query_idx + WINDOW - key_idx
    band = (gap >= 0) & (gap < WINDOW)
    lane = lax.broadcasted_iota(jnp.int32, (2 * WINDOW, LANES), 1)
    low_lanes = lane < HEAD_DIM
    stat_lane = lax.broadcasted_iota(jnp.int32, (WINDOW, LANES), 1)

    def attend(b, kept):
        base = pl.multiple_of(b * WINDOW, WINDOW)
        both = kv[pl.ds(base, 2 * WINDOW), :].astype(f32)
        turned = pltpu.roll(both, HEAD_DIM, 1)
        zero = jnp.zeros_like(both)
        keys = (jnp.where(low_lanes, both, zero).astype(bf16), jnp.where(low_lanes, zero, turned).astype(bf16))
        vals = (jnp.where(low_lanes, turned, zero).astype(bf16), jnp.where(low_lanes, zero, both).astype(bf16))
        stats = jnp.zeros((WINDOW, LANES), f32)
        for pair in range(heads // 2):
            cols = pl.ds(pair * LANES, LANES)
            q = query[pl.ds(base, WINDOW), cols]
            out = None
            for side in range(2):
                head = 2 * pair + side
                scores = lax.dot_general(
                    q, keys[side], (((1,), (1,)), ((), ())), preferred_element_type=f32
                ) * HEAD_DIM ** (-0.5)
                scores = jnp.where(kept, scores, -jnp.inf)
                sink = jnp.full((WINDOW, 1), sink_ref[head], f32)
                top = jnp.maximum(jnp.max(scores, axis=-1, keepdims=True), sink)
                raised = jnp.exp(scores - top)
                total = jnp.sum(raised, axis=-1, keepdims=True) + jnp.exp(sink - top)
                weights = (raised * (1.0 / total)).astype(bf16)
                part = jnp.dot(weights, vals[side], preferred_element_type=f32)
                out = part if out is None else out + part
                stats = jnp.where(stat_lane == head, top + jnp.log(total), stats)
            attended[pl.ds(base, WINDOW), cols] = out
        log_ref[:, pl.ds(base, WINDOW)] = jnp.transpose(stats)[:heads]

    def forward_conv(u):
        arrived(u, mate)
        hop(u, mate, False).start()

    def relay_far():
        forward_conv(CG0)
        hop(CG1, me, False, True).start()

    services = (
        (lambda: relay(1),),
        (lambda: relay(2), lambda: relay(3)),
        (lambda: forward_conv(CI0),),
        (relay_far,),
        (lambda: relay(4), lambda: relay(5)),
    )
    cuts = [1 + (blocks - 1) * i // len(services) for i in range(len(services) + 1)]
    for i, jobs in enumerate(services):

        @pl.loop(cuts[i], cuts[i + 1])
        def _(b):
            attend(b, band)

        @pl.when(middle)
        def _():
            for job in jobs:
                job()

    @pl.when(has_left)
    def _():
        kv_halo.wait_recv()

    attend(0, band & ((key_idx >= WINDOW) | has_left))

    own_base, mate_base = jnp.where(me == 1, rows, 0), jnp.where(me == 1, 0, rows)
    tiles = rows // tile

    def seq(base, i):
        return pl.multiple_of(base + i * tile, tile)

    def out_copy(half, i):
        at = (pl.ds(i * tile, tile), pl.ds(half * LANES, LANES))
        return pltpu.make_async_remote_copy(
            src_ref=conv_out.at[at],
            dst_ref=conv_back.at[at],
            send_sem=out_send.at[half * tiles + i],
            recv_sem=out_recv.at[half * tiles + i],
            device_id={"sp": mate},
            device_id_type=MESH,
        )

    def convolve(half, at, gate):
        taps = taps_ref[:, pl.ds(half * LANES, LANES)].astype(f32)
        near = conv_in[half][pl.ds(at, tile + PAD), :]
        total = jnp.zeros((tile, LANES), f32)
        for k in range(TAPS):
            start = PAD - TAPS + 1 + k
            total = total + taps[k : k + 1] * near[start : start + tile]
        return gate * total

    def split(half, at, value):
        value = value.astype(bf16).astype(f32)
        conv_in[half][pl.ds(at + PAD, tile), :] = value[:, :LANES]
        return value[:, LANES:]

    def convolution(half, product):
        def own_product(i):
            gates[pl.ds(i * tile, tile), :] = split(half, seq(own_base, i), product(0, i))

        own_product(tiles - 1)

        @pl.when(me == 1)
        def _():
            conv_in[half][pl.ds(0, PAD), :] = jnp.zeros((PAD, LANES), f32)
            halo(conv_in[half], 2 * rows, PAD, 1 + half).start()

        cols = pl.ds(half * LANES, LANES)
        for i in range(tiles):
            at = seq(mate_base, i)
            gate = split(half, at, product(1, i))
            conv_out[pl.ds(i * tile, tile), cols] = convolve(half, at, gate).astype(bf16)
            out_copy(half, i).start()
        for i in range(tiles - 1):
            own_product(i)

        @pl.when(me == 2)
        def _():
            halo(conv_in[half], 2 * rows, PAD, 1 + half).wait_recv()

        for i in range(tiles):
            at = pl.ds(i * tile, tile)
            convolved = convolve(half, seq(own_base, i), gates[at, :])
            mixed_ref[at, cols] = (attended[at, cols] + convolved).astype(bf16)

    sources = (normed, other)

    @pl.when(middle)
    def _():
        for u in (CI0, CG0, CI1, CG1):
            own_copies[u].wait()
        forward_conv(CI1)
        for shard in (peer, far):
            for u in (CI0, CG0):
                arrived(u, shard)
        forward_conv(CG1)
        relay(6)
        relay(7)
        for part in (fs * 2 + twin, across * 2 + twin, along * 2 + twin, diagonal * 2 + twin):
            for h in range(2):
                piece_arrived(part, h)

        def whole(which, i):
            at = pl.ds(i * tile, tile)
            return jnp.dot(sources[which][at, :], conv_w0[...], preferred_element_type=f32)

        convolution(0, whole)
        for u in (CI1, CG1):
            arrived(u, peer)
        for which in range(2):

            @pl.loop(0, tiles)
            def _(i):
                at = pl.ds(pl.multiple_of(i * tile, tile), tile)
                sums[which, at, :] = jnp.dot(
                    sources[which][at, early], conv_w1[early, :], preferred_element_type=f32
                )

        for u in (CI1, CG1):
            arrived(u, far)

        def finish(which, i):
            at = pl.ds(i * tile, tile)
            return sums[which, at, :] + jnp.dot(
                sources[which][at, late], conv_w1[late, :], preferred_element_type=f32
            )

        convolution(1, finish)

    @pl.when(end)
    def _():
        for half in range(2):
            for i in range(tiles):
                at = (pl.ds(i * tile, tile), pl.ds(half * LANES, LANES))
                out_copy(half, i).wait_recv()
                mixed_ref[at] = (attended[at] + conv_back[at].astype(f32)).astype(bf16)

    @pl.when(has_right)
    def _():
        kv_halo.wait_send()

    for u in (K, V, Q):
        hop(u, me, True, True).wait_send()

    @pl.when(end)
    def _():
        for h in range(2):
            piece_copy(normed, own_part, h, h, sp=mate).wait_send()
        for u in (CI0, CG0, CI1, CG1):
            hop(u, me, True, True).wait_send()

    @pl.when(middle)
    def _():
        for u in (K, V, Q):
            hop(u, peer, True).wait_send()
            hop(u, far, True).wait_send()
        for u in range(7):
            hop(u, me, False, True).wait_send()
            hop(u, mate, False).wait_send()
        for j in range(len(relays)):
            for copy in relay_copies(j):
                copy.wait_send()
        for half in range(2):
            for i in range(tiles):
                out_copy(half, i).wait_send()

        @pl.when(me == 1)
        def _():
            for half in range(2):
                halo(conv_in[half], 2 * rows, PAD, 1 + half).wait_send()


def paired_body(tokens, norm_gain, w_query, w_key, w_value, w_conv_in, w_conv_gate, conv_taps, sink_logits):
    rows, features = tokens.shape
    width = w_query.shape[1]
    f32, bf16 = jnp.float32, jnp.bfloat16
    hbm = pl.BlockSpec(memory_space=pltpu.HBM)
    vmem = pl.BlockSpec(memory_space=pltpu.VMEM)
    smem = pl.BlockSpec(memory_space=pltpu.SMEM)
    dma = pltpu.SemaphoreType.DMA
    tiles = rows // 256
    return pl.pallas_call(
        paired_kernel,
        out_shape=(
            pltpu.VMEM((rows, width), bf16),
            pltpu.VMEM((width // HEAD_DIM, rows), f32),
        ),
        in_specs=[hbm, vmem] + [hbm] * 5 + [vmem, smem],
        out_specs=(vmem, vmem),
        scratch_shapes=[
            pltpu.VMEM((rows, features), bf16),
            pltpu.VMEM((rows, features), bf16),
            pltpu.VMEM((rows, features), bf16),
            pltpu.VMEM((2 * HEAD_DIM, features), bf16),
            pltpu.VMEM((features, width), bf16),
            pltpu.VMEM((features, width), bf16),
            pltpu.VMEM((features, width), bf16),
            pltpu.VMEM((rows + WINDOW, 2 * HEAD_DIM), bf16),
            pltpu.VMEM((rows, width), bf16),
            pltpu.VMEM((rows, width), f32),
            pltpu.VMEM((rows, width), f32),
            pltpu.VMEM((2 * rows + PAD, LANES), f32),
            pltpu.VMEM((2 * rows + PAD, LANES), f32),
            pltpu.VMEM((rows, LANES), f32),
            pltpu.VMEM((2, rows, width), f32),
            pltpu.VMEM((rows, width), bf16),
            pltpu.VMEM((rows, width), bf16),
            dma((8,)),
            dma((7,)),
            dma((7, 4)),
            dma((7, 4)),
            dma((7, 4)),
            dma((3,)),
            dma((3,)),
            dma((14,)),
            dma((16,)),
            dma((2 * tiles,)),
            dma((2 * tiles,)),
        ],
        compiler_params=pltpu.CompilerParams(
            collective_id=0, has_side_effects=True, vmem_limit_bytes=59 << 20
        ),
        name="paired_attend_convolve",
    )(tokens, norm_gain.reshape(1, -1), w_key.T, w_value.T, w_query, w_conv_in, w_conv_gate, conv_taps, sink_logits)


def line_body(n, tokens, norm_gain, w_query, w_key, w_value, w_conv_in, w_conv_gate, conv_taps, sink_logits):
    rows, features = tokens.shape
    width, kv_width = w_query.shape[1], w_key.shape[1] + w_value.shape[1]
    assert w_key.shape[1] == HEAD_DIM and width % LANES == 0
    depth = w_query.shape[0]
    flip = depth % LANES == 0 and 2 < n <= 16
    if flip:
        w_kv, kv_shape = (w_key.T, w_value.T), (kv_width, features)
    else:
        w_kv, kv_shape = (jnp.concatenate([w_key, w_value], axis=1),), (features, kv_width)
    arrays = 3 + len(w_kv)
    f32, bf16 = jnp.float32, jnp.bfloat16
    hbm = pl.BlockSpec(memory_space=pltpu.HBM)
    vmem = pl.BlockSpec(memory_space=pltpu.VMEM)
    smem = pl.BlockSpec(memory_space=pltpu.SMEM)
    dma = pltpu.SemaphoreType.DMA
    return pl.pallas_call(
        functools.partial(line_kernel, n, flip),
        out_shape=(
            pltpu.VMEM((rows, width), bf16),
            pltpu.VMEM((width // HEAD_DIM, rows), f32),
        ),
        in_specs=[hbm, vmem] + [hbm] * arrays + [vmem, smem],
        out_specs=(vmem, vmem),
        scratch_shapes=[
            pltpu.VMEM((rows, features), bf16),
            pltpu.VMEM((rows, features), bf16),
            pltpu.VMEM(kv_shape, bf16),
            pltpu.VMEM((features, width), bf16),
            pltpu.VMEM((features, width), bf16),
            pltpu.VMEM((features, width), bf16),
            pltpu.VMEM((rows + WINDOW, kv_width), bf16),
            pltpu.VMEM((rows, width), bf16),
            pltpu.VMEM((rows, width), f32),
            pltpu.VMEM((rows + PAD, width), f32),
            pltpu.VMEM((rows, width), f32),
            dma((4,)),
            dma((arrays,)),
            dma((arrays, n)),
            dma((arrays, n)),
            dma((arrays, n)),
            dma((2,)),
            dma((2,)),
        ],
        compiler_params=pltpu.CompilerParams(
            collective_id=0, has_side_effects=True, vmem_limit_bytes=59 << 20
        ),
        name="gather_attend_convolve",
    )(tokens, norm_gain.reshape(1, -1), *w_kv, w_query, w_conv_in, w_conv_gate, conv_taps, sink_logits)


def body(n, fs, tp, *arrays):
    rows, width, depth = arrays[0].shape[0], arrays[2].shape[1], arrays[2].shape[0]
    square = n == 4 and fs == 4 and tp == 2
    if square and width == 2 * LANES and depth % LANES == 0 and rows % (8 * LANES) == 0:
        return paired_body(*arrays)
    return line_body(n, *arrays)


def solution(mesh):
    return jax.shard_map(
        functools.partial(body, mesh.shape["sp"], mesh.shape["fs"], mesh.shape["tp"]),
        mesh=mesh,
        in_specs=(
            P("sp", None),
            P(),
            P("sp", ("fs", "tp")),
            P("sp", ("fs", "tp")),
            P("sp", ("fs", "tp")),
            P("sp", ("fs", "tp")),
            P("sp", ("fs", "tp")),
            P(None, ("fs", "tp")),
            P(("fs", "tp")),
        ),
        out_specs=(P("sp", ("fs", "tp")), P(("fs", "tp"), "sp")),
        check_vma=False,
    )
```

```python
import functools

import jax
import jax.numpy as jnp
from jax import lax
from jax.experimental import pallas as pl
from jax.experimental.pallas import tpu as pltpu
from jax.sharding import PartitionSpec as P

HEAD_DIM = 64
WINDOW = 128
TAPS = 3
EPS = 1e-06
LANES = 128
PAD = 8
MESH = pl.DeviceIdType.MESH


def line_kernel(
    n, flip, tok_ref, gain_ref, *refs
):
    arrays = 5 if flip else 4
    shards = refs[:arrays]
    (
        taps_ref, sink_ref, mixed_ref, log_ref,
        tok, normed, kv_all, q_all, ci_all, cg_all, kv, query, attended, conv_in, gate_sum,
        tok_sem, own_sem, recv_sem, right_sem, left_sem, halo_send, halo_recv,
    ) = refs[arrays:]
    QUERY, CONV, GATE = arrays - 3, arrays - 2, arrays - 1
    me = lax.axis_index("sp")
    rows = tok.shape[0]
    depth = shards[QUERY].shape[0]
    wholes = (kv_all, kv_all, q_all, ci_all, cg_all)[5 - arrays :]
    has_left, has_right = me > 0, me < n - 1
    left, right = jnp.maximum(me - 1, 0), jnp.minimum(me + 1, n - 1)
    blocks = rows // WINDOW
    f32, bf16 = jnp.float32, jnp.bfloat16

    step_rows = rows // 4
    tok_copies = [
        pltpu.make_async_copy(
            tok_ref.at[pl.ds(i * step_rows, step_rows)], tok.at[pl.ds(i * step_rows, step_rows)], tok_sem.at[i]
        )
        for i in range(4)
    ]
    for copy in tok_copies:
        copy.start()

    def place(a, shard):
        at = pl.ds(pl.multiple_of(shard * depth, depth), depth)
        if flip and a < QUERY:
            return kv_all.at[pl.ds(a * HEAD_DIM, HEAD_DIM), at]
        return wholes[a].at[at]

    own_copies = [pltpu.make_async_copy(shards[a], place(a, me), own_sem.at[a]) for a in range(arrays)]
    for copy in own_copies:
        copy.start()

    barrier = pltpu.get_barrier_semaphore()

    @pl.when(has_left)
    def _():
        pl.semaphore_signal(barrier, inc=1, device_id={"sp": left}, device_id_type=MESH)

    @pl.when(has_right)
    def _():
        pl.semaphore_signal(barrier, inc=1, device_id={"sp": right}, device_id_type=MESH)

    pl.semaphore_wait(barrier, has_left.astype(jnp.int32) + has_right.astype(jnp.int32))

    def hop(a, shard, to_right, own=False):
        return pltpu.make_async_remote_copy(
            src_ref=shards[a] if own else place(a, shard),
            dst_ref=place(a, shard),
            send_sem=(right_sem if to_right else left_sem).at[a, shard],
            recv_sem=recv_sem.at[a, shard],
            device_id={"sp": right if to_right else left},
            device_id_type=MESH,
        )

    def send_own(a):
        @pl.when(has_right)
        def _():
            hop(a, me, True, True).start()

        @pl.when(has_left)
        def _():
            hop(a, me, False, True).start()

    def pass_on(a, first, last):
        def step(k, carry):
            @pl.when(me - k >= 0)
            def _():
                shard = me - k
                hop(a, shard, False).wait_recv()

                @pl.when(has_right)
                def _():
                    hop(a, shard, True).start()

            @pl.when(me + k < n)
            def _():
                shard = me + k
                hop(a, shard, True).wait_recv()

                @pl.when(has_left)
                def _():
                    hop(a, shard, False).start()

            return carry

        lax.fori_loop(first, last, step, 0)

    for a in range(GATE):
        send_own(a)

    norm_rows = 64
    for i in range(4):
        tok_copies[i].wait()

        @pl.loop(0, step_rows // norm_rows)
        def _(j):
            at = pl.ds(pl.multiple_of(i * step_rows + j * norm_rows, norm_rows), norm_rows)
            wide = tok[at, :].astype(f32)
            scale = lax.rsqrt(jnp.mean(wide * wide, axis=-1, keepdims=True) + EPS)
            normed[at, :] = (wide * scale * gain_ref[...]).astype(bf16)

    for copy in own_copies:
        copy.wait()

    tile = 256

    def project(a, store):
        @pl.loop(0, rows // tile)
        def _(i):
            base = pl.multiple_of(i * tile, tile)
            side = 1 if flip and a < QUERY else 0
            store(
                base,
                lax.dot_general(
                    normed[pl.ds(base, tile), :],
                    wholes[a][...],
                    (((1,), (side,)), ((), ())),
                    preferred_element_type=f32,
                ),
            )

    def halo(buffer, length, i):
        return pltpu.make_async_remote_copy(
            src_ref=buffer.at[pl.ds(rows, length)],
            dst_ref=buffer.at[pl.ds(0, length)],
            send_sem=halo_send.at[i],
            recv_sem=halo_recv.at[i],
            device_id={"sp": right},
            device_id_type=MESH,
        )

    for a in range(QUERY):
        pass_on(a, 1, n)
    send_own(GATE)

    def store_kv(base, value):
        kv[pl.ds(base + WINDOW, tile), :] = value.astype(bf16)

    project(0, store_kv)

    @pl.when(jnp.logical_not(has_left))
    def _():
        kv[pl.ds(0, WINDOW), :] = jnp.zeros((WINDOW, kv.shape[1]), bf16)
        conv_in[pl.ds(0, PAD), :] = jnp.zeros((PAD, conv_in.shape[1]), f32)

    pass_on(QUERY, 1, n)

    @pl.when(has_right)
    def _():
        halo(kv, WINDOW, 0).start()

    def store_query(base, value):
        query[pl.ds(base, tile), :] = value.astype(bf16)

    project(QUERY, store_query)

    heads = query.shape[1] // HEAD_DIM
    query_idx = lax.broadcasted_iota(jnp.int32, (WINDOW, 2 * WINDOW), 0)
    key_idx = lax.broadcasted_iota(jnp.int32, (WINDOW, 2 * WINDOW), 1)
    gap = query_idx + WINDOW - key_idx
    band = (gap >= 0) & (gap < WINDOW)
    lane = lax.broadcasted_iota(jnp.int32, (2 * WINDOW, LANES), 1)
    low = lane < HEAD_DIM
    stat_lane = lax.broadcasted_iota(jnp.int32, (WINDOW, LANES), 1)

    def attend(b, kept):
        base = pl.multiple_of(b * WINDOW, WINDOW)
        both = kv[pl.ds(base, 2 * WINDOW), :].astype(f32)
        turned = pltpu.roll(both, HEAD_DIM, 1)
        zero = jnp.zeros_like(both)
        keys = (jnp.where(low, both, zero).astype(bf16), jnp.where(low, zero, turned).astype(bf16))
        vals = (jnp.where(low, turned, zero).astype(bf16), jnp.where(low, zero, both).astype(bf16))
        stats = jnp.zeros((WINDOW, LANES), f32)
        for pair in range(heads // 2):
            cols = pl.ds(pair * LANES, LANES)
            q = query[pl.ds(base, WINDOW), cols]
            out = None
            for side in range(2):
                head = 2 * pair + side
                scores = lax.dot_general(
                    q, keys[side], (((1,), (1,)), ((), ())), preferred_element_type=f32
                ) * HEAD_DIM ** (-0.5)
                scores = jnp.where(kept, scores, -jnp.inf)
                sink = jnp.full((WINDOW, 1), sink_ref[head], f32)
                top = jnp.maximum(jnp.max(scores, axis=-1, keepdims=True), sink)
                raised = jnp.exp(scores - top)
                total = jnp.sum(raised, axis=-1, keepdims=True) + jnp.exp(sink - top)
                weights = (raised * (1.0 / total)).astype(bf16)
                part = jnp.dot(weights, vals[side], preferred_element_type=f32)
                out = part if out is None else out + part
                stats = jnp.where(stat_lane == head, top + jnp.log(total), stats)
            attended[pl.ds(base, WINDOW), cols] = out
        log_ref[:, pl.ds(base, WINDOW)] = jnp.transpose(stats)[:heads]

    def attend_range(first, last):
        @pl.loop(first, last)
        def _(b):
            attend(b, band)

    cut = [1 + (n - 1) * i // 3 for i in range(4)]
    mid = 1 + (blocks - 1) // 2
    attend_range(1, mid)
    pass_on(CONV, cut[0], cut[1])
    attend_range(mid, blocks)
    pass_on(CONV, cut[1], cut[2])

    @pl.when(has_left)
    def _():
        halo(kv, WINDOW, 0).wait_recv()

    attend(0, band & ((key_idx >= WINDOW) | has_left))
    pass_on(CONV, cut[2], cut[3])

    def store_conv(base, value):
        conv_in[pl.ds(base + PAD, tile), :] = value.astype(bf16).astype(f32)

    project(CONV, store_conv)
    early = min(2, n - 1)
    pass_on(GATE, 1, early)

    @pl.when(has_right)
    def _():
        halo(conv_in, PAD, 1).start()

    pass_on(GATE, early, n - 1)

    far = jnp.where(2 * me >= n, 0, n - 1)

    def gate_part(base, shard):
        at = pl.ds(pl.multiple_of(shard * depth, depth), depth)
        return jnp.dot(
            normed[pl.ds(base, tile), at], cg_all[at, :], preferred_element_type=f32
        )

    if flip:

        @pl.loop(0, rows // tile)
        def _(i):
            base = pl.multiple_of(i * tile, tile)
            part = gate_part(base, lax.rem(far + 1, n))
            for j in range(2, n):
                part = part + gate_part(base, lax.rem(far + j, n))
            gate_sum[pl.ds(base, tile), :] = part

    pass_on(GATE, n - 1, n)

    @pl.when(has_left)
    def _():
        halo(conv_in, PAD, 1).wait_recv()

    def store_mixed(base, value):
        gate = value.astype(bf16).astype(f32)
        taps = taps_ref[...].astype(f32)
        near = conv_in[pl.ds(base, tile + PAD), :]
        total = jnp.zeros_like(gate)
        for k in range(TAPS):
            start = PAD - TAPS + 1 + k
            total = total + taps[k : k + 1] * near[start : start + tile]
        mixed_ref[pl.ds(base, tile), :] = (attended[pl.ds(base, tile), :] + gate * total).astype(bf16)

    if flip:

        @pl.loop(0, rows // tile)
        def _(i):
            base = pl.multiple_of(i * tile, tile)
            store_mixed(base, gate_sum[pl.ds(base, tile), :] + gate_part(base, far))

    else:
        project(GATE, store_mixed)

    @pl.when(has_right)
    def _():
        halo(kv, WINDOW, 0).wait_send()
        halo(conv_in, PAD, 1).wait_send()

    for a in range(arrays):

        @pl.when(has_right)
        def _():
            @pl.loop(0, me + 1)
            def _(s):
                hop(a, s, True).wait_send()

        @pl.when(has_left)
        def _():
            @pl.loop(me, n)
            def _(s):
                hop(a, s, False).wait_send()


def paired_kernel(tok_ref, gain_ref, *refs):
    shards = refs[:5]
    (
        taps_ref, sink_ref, mixed_ref, log_ref,
        tok, normed, other, kv_all, q_all, stage, conv_w, kv, query, q_part, attended,
        conv_in, gates, convolved, sums, conv_out, conv_back, turned_taps, edge_out, edge_in,
        tok_sem, own_sem, recv_sem, mate_sem, peer_sem, halo_send, halo_recv,
        x_send, x_recv, out_send, out_recv,
    ) = refs[5:]
    f32, bf16 = jnp.float32, jnp.bfloat16
    me, fs, tp = lax.axis_index("sp"), lax.axis_index("fs"), lax.axis_index("tp")
    low = me < 2
    end = (me == 0) | (me == 3)
    middle = jnp.logical_not(end)
    mate = me + 1 - 2 * lax.rem(me, 2)
    peer = jnp.where(end, 3 - mate, 3 - me)
    far = jnp.where(low, 3, 0)
    first = jnp.where(low, 0, 1)
    has_left, has_right = me > 0, me < 3
    right = jnp.minimum(me + 1, 3)
    across, along = fs + 1 - 2 * lax.rem(fs, 2), lax.rem(fs + 2, 4)
    diagonal = 3 - fs
    twin = 1 - tp
    rows = tok.shape[0]
    depth = shards[2].shape[0]
    blocks = rows // WINDOW
    width = q_all.shape[1]
    widths = (width // 2, width // 4, width // 8, width // 8)
    groups = range(len(widths))
    channel = [sum(widths[:g]) for g in groups]
    K, V, Q, G0, G0_GATE, G1, G2, G3 = units = range(8)
    spans = {G0: (0, width // 2), G0_GATE: (width // 2, width // 2)}
    spans.update({G0_GATE + g: (2 * channel[g], 2 * widths[g]) for g in groups[1:]})
    units_of = ((G0, G0_GATE), (G1,), (G2,), (G3,))

    parts = 8
    part_rows = rows // parts
    piece = part_rows // 2
    own_part = fs * 2 + tp

    def part_at(i):
        return lax.rem(own_part + i, parts)

    def rows_of(start, length):
        return pl.ds(pl.multiple_of(start, 16), length)

    tok_copies = []
    for i in range(parts):
        at = rows_of(part_at(i) * part_rows, part_rows)
        tok_copies.append(pltpu.make_async_copy(tok_ref.at[at], tok.at[at], tok_sem.at[i]))
    for copy in tok_copies:
        copy.start()

    def shard_at(shard):
        return pl.ds(pl.multiple_of(shard * depth, depth), depth)

    def place(u, shard):
        at = shard_at(shard)
        if u < Q:
            return kv_all.at[pl.ds(u * HEAD_DIM, HEAD_DIM), at]
        if u == Q:
            return q_all.at[at]
        return conv_w.at[pl.ds(*spans[u]), at]

    own_copies = [pltpu.make_async_copy(shards[u], place(u, me), own_sem.at[u]) for u in (K, V, Q)]
    own_copies += [pltpu.make_async_copy(shards[3 + j], stage.at[j], own_sem.at[3 + j]) for j in range(2)]
    for copy in own_copies:
        copy.start()

    barrier = pltpu.get_barrier_semaphore()

    def greet(**device):
        pl.semaphore_signal(barrier, inc=1, device_id=device, device_id_type=MESH)

    greet(sp=mate)

    @pl.when(middle)
    def _():
        greet(sp=peer)
        greet(fs=across)
        greet(fs=along)
        greet(tp=twin)

    own_copies[3].wait()
    own_copies[4].wait()
    for j in range(2):
        for block in range(depth // LANES):
            turned = jnp.transpose(stage[j, pl.ds(block * LANES, LANES), :].astype(f32)).astype(bf16)
            at = pl.ds(pl.multiple_of(me * depth + block * LANES, LANES), LANES)
            for g in groups:
                to = pl.ds(2 * channel[g] + j * widths[g], widths[g])
                conv_w[to, at] = turned[channel[g] : channel[g] + widths[g]]
    taps = taps_ref[...].astype(f32)
    turned_taps[...] = jnp.transpose(jnp.concatenate([taps, jnp.zeros((8 - TAPS, width), f32)], axis=0))
    for u in (K, V, Q):
        own_copies[u].wait()

    pl.semaphore_wait(barrier, jnp.where(middle, 5, 1))

    def hop(u, shard, to_mate):
        return pltpu.make_async_remote_copy(
            src_ref=place(u, shard),
            dst_ref=place(u, shard),
            send_sem=(mate_sem if to_mate else peer_sem).at[u, shard],
            recv_sem=recv_sem.at[u, shard],
            device_id={"sp": mate if to_mate else peer},
            device_id_type=MESH,
        )

    def arrived(u, shard):
        hop(u, shard, True).wait_recv()

    for u in (K, V, Q):
        hop(u, me, True).start()

    @pl.when(middle)
    def _():
        for u in (K, V, Q):
            hop(u, me, False).start()

    def norm_part(i):
        tok_copies[i].wait()
        norm_rows = 64

        @pl.loop(0, part_rows // norm_rows)
        def _(j):
            at = rows_of(part_at(i) * part_rows + j * norm_rows, norm_rows)
            wide = tok[at, :].astype(f32)
            scale = lax.rsqrt(jnp.mean(wide * wide, axis=-1, keepdims=True) + EPS)
            normed[at, :] = (wide * scale * gain_ref[...]).astype(bf16)

    def piece_at(part, h):
        return rows_of(part * part_rows + h * piece, piece)

    def piece_copy(buffer, part, h, i, **device):
        at = piece_at(part, h)
        return pltpu.make_async_remote_copy(
            src_ref=buffer.at[at],
            dst_ref=other.at[at],
            send_sem=x_send.at[i],
            recv_sem=x_recv.at[part * 2 + h],
            device_id=device,
            device_id_type=MESH,
        )

    def piece_arrived(part, h):
        piece_copy(other, part, h, 0, sp=mate).wait_recv()

    across_part, along_part, diagonal_part = across * 2 + tp, along * 2 + tp, diagonal * 2 + tp
    relays = (
        (own_part, 0, ("tp", "fs_across", "fs_along")),
        (own_part, 1, ("tp", "fs_across", "fs_along")),
        (across_part, 0, ("tp", "fs_along")),
        (along_part, 0, ("tp",)),
        (across_part, 1, ("tp",)),
        (along_part, 1, ("tp", "fs_across")),
        (diagonal_part, 0, ("tp",)),
        (diagonal_part, 1, ("tp",)),
    )
    devices = {"tp": {"tp": twin}, "fs_across": {"fs": across}, "fs_along": {"fs": along}}

    def relay_copies(j):
        base = sum(len(to) for _, _, to in relays[:j])
        part, h, to = relays[j]
        return [piece_copy(other, part, h, base + i, **devices[d]) for i, d in enumerate(to)]

    def relay(j):
        piece_arrived(relays[j][0], relays[j][1])
        for copy in relay_copies(j):
            copy.start()

    norm_part(0)
    norm_part(1)

    @pl.when(end)
    def _():
        for h in range(2):
            piece_copy(normed, own_part, h, h, sp=mate).start()
        for u in units[G0:]:
            hop(u, me, True).start()

    for i in range(2, parts):
        norm_part(i)

    for u in (K, V):
        arrived(u, mate)

        @pl.when(middle)
        def _():
            hop(u, mate, False).start()

        arrived(u, peer)

        @pl.when(middle)
        def _():
            hop(u, peer, True).start()

    arrived(Q, mate)

    @pl.when(middle)
    def _():
        hop(Q, mate, False).start()
        for u in (G0, G0_GATE, G1):
            hop(u, me, False).start()

    arrived(Q, peer)

    @pl.when(middle)
    def _():
        hop(Q, peer, True).start()

    for u in (K, V):
        arrived(u, far)

        @pl.when(middle)
        def _():
            hop(u, far, True).start()

    tile = 256

    @pl.loop(0, rows // tile)
    def _(i):
        base = pl.multiple_of(i * tile, tile)
        kv[pl.ds(base + WINDOW, tile), :] = lax.dot_general(
            normed[pl.ds(base, tile), :], kv_all[...], (((1,), (1,)), ((), ())), preferred_element_type=f32
        ).astype(bf16)

    def halo(buffer, start, length, i):
        return pltpu.make_async_remote_copy(
            src_ref=buffer.at[pl.ds(start, length)],
            dst_ref=buffer.at[pl.ds(0, length)],
            send_sem=halo_send.at[i],
            recv_sem=halo_recv.at[i],
            device_id={"sp": right},
            device_id_type=MESH,
        )

    kv_halo = halo(kv, rows, WINDOW, 0)

    @pl.when(jnp.logical_not(has_left))
    def _():
        kv[pl.ds(0, WINDOW), :] = jnp.zeros((WINDOW, kv.shape[1]), bf16)

    early = pl.ds(pl.multiple_of(first * depth, depth), 3 * depth)
    late = pl.ds(pl.multiple_of(far * depth, depth), depth)

    @pl.loop(0, rows // tile)
    def _(i):
        at = pl.ds(pl.multiple_of(i * tile, tile), tile)
        q_part[at, :] = jnp.dot(normed[at, early], q_all[early, :], preferred_element_type=f32)

    @pl.when(has_right)
    def _():
        kv_halo.start()

    @pl.when(middle)
    def _():
        relay(0)

    arrived(Q, far)

    @pl.when(middle)
    def _():
        hop(Q, far, True).start()

    @pl.loop(0, rows // tile)
    def _(i):
        at = pl.ds(pl.multiple_of(i * tile, tile), tile)
        query[at, :] = (
            q_part[at, :] + jnp.dot(normed[at, late], q_all[late, :], preferred_element_type=f32)
        ).astype(bf16)

    heads = query.shape[1] // HEAD_DIM
    query_idx = lax.broadcasted_iota(jnp.int32, (WINDOW, 2 * WINDOW), 0)
    key_idx = lax.broadcasted_iota(jnp.int32, (WINDOW, 2 * WINDOW), 1)
    gap = query_idx + WINDOW - key_idx
    band = (gap >= 0) & (gap < WINDOW)
    lane = lax.broadcasted_iota(jnp.int32, (2 * WINDOW, LANES), 1)
    low_lanes = lane < HEAD_DIM
    stat_lane = lax.broadcasted_iota(jnp.int32, (WINDOW, LANES), 1)

    def attend(b, kept):
        base = pl.multiple_of(b * WINDOW, WINDOW)
        both = kv[pl.ds(base, 2 * WINDOW), :].astype(f32)
        turned = pltpu.roll(both, HEAD_DIM, 1)
        zero = jnp.zeros_like(both)
        keys = (jnp.where(low_lanes, both, zero).astype(bf16), jnp.where(low_lanes, zero, turned).astype(bf16))
        vals = (jnp.where(low_lanes, turned, zero).astype(bf16), jnp.where(low_lanes, zero, both).astype(bf16))
        stats = jnp.zeros((WINDOW, LANES), f32)
        for pair in range(heads // 2):
            cols = pl.ds(pair * LANES, LANES)
            q = query[pl.ds(base, WINDOW), cols]
            out = None
            for side in range(2):
                head = 2 * pair + side
                scores = lax.dot_general(
                    q, keys[side], (((1,), (1,)), ((), ())), preferred_element_type=f32
                ) * HEAD_DIM ** (-0.5)
                scores = jnp.where(kept, scores, -jnp.inf)
                sink = jnp.full((WINDOW, 1), sink_ref[head], f32)
                top = jnp.maximum(jnp.max(scores, axis=-1, keepdims=True), sink)
                raised = jnp.exp(scores - top)
                total = jnp.sum(raised, axis=-1, keepdims=True) + jnp.exp(sink - top)
                weights = (raised * (1.0 / total)).astype(bf16)
                part = jnp.dot(weights, vals[side], preferred_element_type=f32)
                out = part if out is None else out + part
                stats = jnp.where(stat_lane == head, top + jnp.log(total), stats)
            attended[pl.ds(base, WINDOW), cols] = out
        log_ref[:, pl.ds(base, WINDOW)] = jnp.transpose(stats)[:heads]

    def forward_conv(u):
        arrived(u, mate)
        hop(u, mate, False).start()

    def forward_rest():
        forward_conv(G1)
        hop(G2, me, False).start()
        hop(G3, me, False).start()

    services = (
        (lambda: relay(1),),
        (lambda: relay(2), lambda: relay(3)),
        (lambda: forward_conv(G0),),
        (lambda: forward_conv(G0_GATE),),
        (lambda: relay(4), lambda: relay(5)),
    )
    cuts = [1 + (blocks - 1) * i // len(services) for i in range(len(services) + 1)]
    for i, jobs in enumerate(services):

        @pl.loop(cuts[i], cuts[i + 1])
        def _(b):
            attend(b, band)

        @pl.when(middle)
        def _():
            for job in jobs:
                job()

    @pl.when(has_left)
    def _():
        kv_halo.wait_recv()

    attend(0, band & ((key_idx >= WINDOW) | has_left))

    own_base, mate_base = jnp.where(me == 1, rows, 0), jnp.where(me == 1, 0, rows)
    bases = (own_base, mate_base)
    sources = (normed, other)
    tiles = rows // tile
    OWN, MATE = 0, 1
    last = tiles - 1
    pair = pl.ds(pl.multiple_of(jnp.minimum(me, mate) * depth, depth), 2 * depth)
    rest = pl.ds(pl.multiple_of(jnp.minimum(peer, far) * depth, depth), 2 * depth)

    def tile_at(i):
        return pl.ds(i * tile if isinstance(i, int) else pl.multiple_of(i * tile, tile), tile)

    def out_copy(g, i):
        at = (pl.ds(channel[g], widths[g]), tile_at(i))
        return pltpu.make_async_remote_copy(
            src_ref=conv_out.at[at],
            dst_ref=conv_back.at[at],
            send_sem=out_send.at[g * tiles + i],
            recv_sem=out_recv.at[g * tiles + i],
            device_id={"sp": mate},
            device_id_type=MESH,
        )

    def edge_copy(g):
        return pltpu.make_async_remote_copy(
            src_ref=edge_out.at[g],
            dst_ref=edge_in.at[g],
            send_sem=halo_send.at[1 + g],
            recv_sem=halo_recv.at[1 + g],
            device_id={"sp": right},
            device_id_type=MESH,
        )

    def dot(which, i, start, length, at):
        return lax.dot_general(
            conv_w[pl.ds(start, length), at],
            sources[which][tile_at(i), at],
            (((1,), (1,)), ((), ())),
            preferred_element_type=f32,
        )

    def partial(which, i, g, at, fresh):
        start = 2 * channel[g]
        value = dot(which, i, start, 2 * width - start, at)
        to = pl.ds(start - 2 * widths[0], 2 * width - start)
        sums[which, to, tile_at(i)] = value if fresh else sums[which, to, tile_at(i)] + value

    def product(which, i, g, at):
        value = dot(which, i, 2 * channel[g], 2 * widths[g], at)
        if g:
            value = value + sums[which, pl.ds(2 * channel[g] - 2 * widths[0], 2 * widths[g]), tile_at(i)]
        value = value.astype(bf16).astype(f32)
        base = pl.multiple_of(bases[which] + LANES + i * tile, LANES)
        conv_in[pl.ds(channel[g], widths[g]), pl.ds(base, tile)] = value[: widths[g]]
        return value[widths[g] :]

    def convolve(which, i, g, gate):
        of = pl.ds(channel[g], widths[g])
        base = pl.multiple_of(bases[which] + i * tile, LANES)
        near = conv_in[of, pl.ds(base, tile + LANES)]
        total = jnp.zeros((widths[g], tile), f32)
        for k in range(TAPS):
            moved = near if k == TAPS - 1 else pltpu.roll(near, TAPS - 1 - k, 1)
            total = total + turned_taps[of, k : k + 1] * moved[:, LANES:]
        return gate * total

    def own_product(i, g, at):
        gates[pl.ds(channel[g], widths[g]), tile_at(i)] = product(OWN, i, g, at)

    def own_last(g, at):
        own_product(last, g, at)
        of = pl.ds(channel[g], widths[g])

        @pl.when(me == 1)
        def _():
            conv_in[of, pl.ds(0, LANES)] = jnp.zeros((widths[g], LANES), f32)
            edge = jnp.transpose(conv_in[of, pl.ds(2 * rows, LANES)])
            edge_out[g, :, pl.ds(0, widths[g])] = edge[LANES - PAD :]
            edge_copy(g).start()

    def mate_tiles(g, at):
        of = pl.ds(channel[g], widths[g])
        for i in range(tiles):
            conv_out[of, tile_at(i)] = convolve(MATE, i, g, product(MATE, i, g, at)).astype(bf16)
            out_copy(g, i).start()

    def own_tiles(g, at):
        of = pl.ds(channel[g], widths[g])

        @pl.loop(0, last)
        def _(i):
            own_product(i, g, at)

        @pl.when(me == 2)
        def _():
            edge_copy(g).wait_recv()
            edge = edge_in[g, :, pl.ds(0, widths[g])]
            edge = jnp.concatenate([jnp.zeros((LANES - PAD, widths[g]), f32), edge], axis=0)
            conv_in[of, pl.ds(0, LANES)] = jnp.transpose(edge)

        @pl.loop(0, tiles)
        def _(i):
            convolved[of, tile_at(i)] = convolve(OWN, i, g, gates[of, tile_at(i)])

    everything = pl.ds(0, conv_w.shape[1])

    def mix(half, source):
        cols = pl.ds(half * LANES, LANES)

        @pl.loop(0, rows // LANES)
        def _(i):
            at = pl.ds(pl.multiple_of(i * LANES, LANES), LANES)
            extra = jnp.transpose(source[cols, at].astype(f32))
            mixed_ref[at, cols] = (attended[at, cols] + extra).astype(bf16)

    @pl.when(middle)
    def _():
        forward_rest()
        for u in (G0, G0_GATE):
            arrived(u, peer)
            arrived(u, far)
        forward_conv(G2)
        forward_conv(G3)
        relay(6)
        relay(7)
        for part in (fs * 2 + twin, across * 2 + twin, along * 2 + twin, diagonal * 2 + twin):
            for h in range(2):
                piece_arrived(part, h)

        own_last(0, everything)
        mate_tiles(0, everything)
        partial(OWN, last, 1, pair, True)

        @pl.loop(0, tiles)
        def _(i):
            partial(MATE, i, 1, pair, True)

        arrived(G1, peer)
        arrived(G1, far)
        own_last(1, rest)
        mate_tiles(1, rest)
        own_tiles(0, everything)

        @pl.loop(0, last)
        def _(i):
            partial(OWN, i, 1, pair, True)

        arrived(G2, peer)
        arrived(G3, peer)
        partial(OWN, last, 2, shard_at(peer), False)

        @pl.loop(0, tiles)
        def _(i):
            partial(MATE, i, 2, shard_at(peer), False)

        for g in (2, 3):
            arrived(G0_GATE + g, far)
            own_last(g, shard_at(far))
            mate_tiles(g, shard_at(far))
        own_tiles(1, rest)

        @pl.loop(0, last)
        def _(i):
            partial(OWN, i, 2, shard_at(peer), False)

        for g in (2, 3):
            own_tiles(g, shard_at(far))
        for half in range(2):
            mix(half, convolved)

    @pl.when(end)
    def _():
        for i in range(tiles):
            out_copy(0, i).wait_recv()
        mix(0, conv_back)
        for g in groups[1:]:
            for i in range(tiles):
                out_copy(g, i).wait_recv()
        mix(1, conv_back)

    @pl.when(has_right)
    def _():
        kv_halo.wait_send()

    for u in (K, V, Q):
        hop(u, me, True).wait_send()

    @pl.when(end)
    def _():
        for h in range(2):
            piece_copy(normed, own_part, h, h, sp=mate).wait_send()
        for u in units[G0:]:
            hop(u, me, True).wait_send()

    @pl.when(middle)
    def _():
        for u in (K, V, Q):
            hop(u, peer, True).wait_send()
            hop(u, far, True).wait_send()
        for u in units:
            hop(u, me, False).wait_send()
            hop(u, mate, False).wait_send()
        for j in range(len(relays)):
            for copy in relay_copies(j):
                copy.wait_send()
        for g in groups:
            for i in range(tiles):
                out_copy(g, i).wait_send()

        @pl.when(me == 1)
        def _():
            for g in groups:
                edge_copy(g).wait_send()


def paired_body(tokens, norm_gain, w_query, w_key, w_value, w_conv_in, w_conv_gate, conv_taps, sink_logits):
    rows, features = tokens.shape
    width = w_query.shape[1]
    f32, bf16 = jnp.float32, jnp.bfloat16
    hbm = pl.BlockSpec(memory_space=pltpu.HBM)
    vmem = pl.BlockSpec(memory_space=pltpu.VMEM)
    smem = pl.BlockSpec(memory_space=pltpu.SMEM)
    dma = pltpu.SemaphoreType.DMA
    tiles = rows // 256
    return pl.pallas_call(
        paired_kernel,
        out_shape=(
            pltpu.VMEM((rows, width), bf16),
            pltpu.VMEM((width // HEAD_DIM, rows), f32),
        ),
        in_specs=[hbm, vmem] + [hbm] * 5 + [vmem, smem],
        out_specs=(vmem, vmem),
        scratch_shapes=[
            pltpu.VMEM((rows, features), bf16),
            pltpu.VMEM((rows, features), bf16),
            pltpu.VMEM((rows, features), bf16),
            pltpu.VMEM((2 * HEAD_DIM, features), bf16),
            pltpu.VMEM((features, width), bf16),
            pltpu.VMEM((2, w_query.shape[0], width), bf16),
            pltpu.VMEM((2 * width, features), bf16),
            pltpu.VMEM((rows + WINDOW, 2 * HEAD_DIM), bf16),
            pltpu.VMEM((rows, width), bf16),
            pltpu.VMEM((rows, width), f32),
            pltpu.VMEM((rows, width), f32),
            pltpu.VMEM((width, LANES + 2 * rows), f32),
            pltpu.VMEM((width, rows), f32),
            pltpu.VMEM((width, rows), f32),
            pltpu.VMEM((2, width, rows), f32),
            pltpu.VMEM((width, rows), bf16),
            pltpu.VMEM((width, rows), bf16),
            pltpu.VMEM((width, 8), f32),
            pltpu.VMEM((4, PAD, LANES), f32),
            pltpu.VMEM((4, PAD, LANES), f32),
            dma((8,)),
            dma((5,)),
            dma((8, 4)),
            dma((8, 4)),
            dma((8, 4)),
            dma((5,)),
            dma((5,)),
            dma((14,)),
            dma((16,)),
            dma((4 * tiles,)),
            dma((4 * tiles,)),
        ],
        compiler_params=pltpu.CompilerParams(
            collective_id=0, has_side_effects=True, vmem_limit_bytes=59 << 20
        ),
        name="paired_attend_convolve",
    )(tokens, norm_gain.reshape(1, -1), w_key.T, w_value.T, w_query, w_conv_in, w_conv_gate, conv_taps, sink_logits)


def line_body(n, tokens, norm_gain, w_query, w_key, w_value, w_conv_in, w_conv_gate, conv_taps, sink_logits):
    rows, features = tokens.shape
    width, kv_width = w_query.shape[1], w_key.shape[1] + w_value.shape[1]
    assert w_key.shape[1] == HEAD_DIM and width % LANES == 0
    depth = w_query.shape[0]
    flip = depth % LANES == 0 and 2 < n <= 16
    if flip:
        w_kv, kv_shape = (w_key.T, w_value.T), (kv_width, features)
    else:
        w_kv, kv_shape = (jnp.concatenate([w_key, w_value], axis=1),), (features, kv_width)
    arrays = 3 + len(w_kv)
    f32, bf16 = jnp.float32, jnp.bfloat16
    hbm = pl.BlockSpec(memory_space=pltpu.HBM)
    vmem = pl.BlockSpec(memory_space=pltpu.VMEM)
    smem = pl.BlockSpec(memory_space=pltpu.SMEM)
    dma = pltpu.SemaphoreType.DMA
    return pl.pallas_call(
        functools.partial(line_kernel, n, flip),
        out_shape=(
            pltpu.VMEM((rows, width), bf16),
            pltpu.VMEM((width // HEAD_DIM, rows), f32),
        ),
        in_specs=[hbm, vmem] + [hbm] * arrays + [vmem, smem],
        out_specs=(vmem, vmem),
        scratch_shapes=[
            pltpu.VMEM((rows, features), bf16),
            pltpu.VMEM((rows, features), bf16),
            pltpu.VMEM(kv_shape, bf16),
            pltpu.VMEM((features, width), bf16),
            pltpu.VMEM((features, width), bf16),
            pltpu.VMEM((features, width), bf16),
            pltpu.VMEM((rows + WINDOW, kv_width), bf16),
            pltpu.VMEM((rows, width), bf16),
            pltpu.VMEM((rows, width), f32),
            pltpu.VMEM((rows + PAD, width), f32),
            pltpu.VMEM((rows, width), f32),
            dma((4,)),
            dma((arrays,)),
            dma((arrays, n)),
            dma((arrays, n)),
            dma((arrays, n)),
            dma((2,)),
            dma((2,)),
        ],
        compiler_params=pltpu.CompilerParams(
            collective_id=0, has_side_effects=True, vmem_limit_bytes=59 << 20
        ),
        name="gather_attend_convolve",
    )(tokens, norm_gain.reshape(1, -1), *w_kv, w_query, w_conv_in, w_conv_gate, conv_taps, sink_logits)


def body(n, fs, tp, *arrays):
    rows, width, depth = arrays[0].shape[0], arrays[2].shape[1], arrays[2].shape[0]
    square = n == 4 and fs == 4 and tp == 2
    if square and width == 2 * LANES and depth % LANES == 0 and rows % (8 * LANES) == 0:
        return paired_body(*arrays)
    return line_body(n, *arrays)


def solution(mesh):
    return jax.shard_map(
        functools.partial(body, mesh.shape["sp"], mesh.shape["fs"], mesh.shape["tp"]),
        mesh=mesh,
        in_specs=(
            P("sp", None),
            P(),
            P("sp", ("fs", "tp")),
            P("sp", ("fs", "tp")),
            P("sp", ("fs", "tp")),
            P("sp", ("fs", "tp")),
            P("sp", ("fs", "tp")),
            P(None, ("fs", "tp")),
            P(("fs", "tp")),
        ),
        out_specs=(P("sp", ("fs", "tp")), P(("fs", "tp"), "sp")),
        check_vma=False,
    )
```

```python
import functools
import math

import jax
import jax.numpy as jnp
from jax import lax
from jax.experimental import pallas as pl
from jax.experimental.pallas import tpu as pltpu
from jax.sharding import PartitionSpec as P

HEAD_DIM = 64
WINDOW = 128
TAPS = 3
EPS = 1e-06
LANES = 128
PAD = 8
LOG2_E = math.log2(math.e)
LN_2 = math.log(2)
MESH = pl.DeviceIdType.MESH


def line_kernel(
    n, flip, tok_ref, gain_ref, *refs
):
    arrays = 5 if flip else 4
    shards = refs[:arrays]
    (
        taps_ref, sink_ref, mixed_ref, log_ref,
        tok, normed, kv_all, q_all, ci_all, cg_all, kv, query, attended, conv_in, gate_sum,
        tok_sem, own_sem, recv_sem, right_sem, left_sem, halo_send, halo_recv,
    ) = refs[arrays:]
    QUERY, CONV, GATE = arrays - 3, arrays - 2, arrays - 1
    me = lax.axis_index("sp")
    rows = tok.shape[0]
    depth = shards[QUERY].shape[0]
    wholes = (kv_all, kv_all, q_all, ci_all, cg_all)[5 - arrays :]
    has_left, has_right = me > 0, me < n - 1
    left, right = jnp.maximum(me - 1, 0), jnp.minimum(me + 1, n - 1)
    blocks = rows // WINDOW
    f32, bf16 = jnp.float32, jnp.bfloat16

    step_rows = rows // 4
    tok_copies = [
        pltpu.make_async_copy(
            tok_ref.at[pl.ds(i * step_rows, step_rows)], tok.at[pl.ds(i * step_rows, step_rows)], tok_sem.at[i]
        )
        for i in range(4)
    ]
    for copy in tok_copies:
        copy.start()

    def place(a, shard):
        at = pl.ds(pl.multiple_of(shard * depth, depth), depth)
        if flip and a < QUERY:
            return kv_all.at[pl.ds(a * HEAD_DIM, HEAD_DIM), at]
        return wholes[a].at[at]

    own_copies = [pltpu.make_async_copy(shards[a], place(a, me), own_sem.at[a]) for a in range(arrays)]
    for copy in own_copies:
        copy.start()

    barrier = pltpu.get_barrier_semaphore()

    @pl.when(has_left)
    def _():
        pl.semaphore_signal(barrier, inc=1, device_id={"sp": left}, device_id_type=MESH)

    @pl.when(has_right)
    def _():
        pl.semaphore_signal(barrier, inc=1, device_id={"sp": right}, device_id_type=MESH)

    pl.semaphore_wait(barrier, has_left.astype(jnp.int32) + has_right.astype(jnp.int32))

    def hop(a, shard, to_right, own=False):
        return pltpu.make_async_remote_copy(
            src_ref=shards[a] if own else place(a, shard),
            dst_ref=place(a, shard),
            send_sem=(right_sem if to_right else left_sem).at[a, shard],
            recv_sem=recv_sem.at[a, shard],
            device_id={"sp": right if to_right else left},
            device_id_type=MESH,
        )

    def send_own(a):
        @pl.when(has_right)
        def _():
            hop(a, me, True, True).start()

        @pl.when(has_left)
        def _():
            hop(a, me, False, True).start()

    def pass_on(a, first, last):
        def step(k, carry):
            @pl.when(me - k >= 0)
            def _():
                shard = me - k
                hop(a, shard, False).wait_recv()

                @pl.when(has_right)
                def _():
                    hop(a, shard, True).start()

            @pl.when(me + k < n)
            def _():
                shard = me + k
                hop(a, shard, True).wait_recv()

                @pl.when(has_left)
                def _():
                    hop(a, shard, False).start()

            return carry

        lax.fori_loop(first, last, step, 0)

    for a in range(GATE):
        send_own(a)

    norm_rows = 64
    for i in range(4):
        tok_copies[i].wait()

        @pl.loop(0, step_rows // norm_rows)
        def _(j):
            at = pl.ds(pl.multiple_of(i * step_rows + j * norm_rows, norm_rows), norm_rows)
            wide = tok[at, :].astype(f32)
            scale = lax.rsqrt(jnp.mean(wide * wide, axis=-1, keepdims=True) + EPS)
            normed[at, :] = (wide * scale * gain_ref[...]).astype(bf16)

    for copy in own_copies:
        copy.wait()

    tile = 256

    def project(a, store):
        @pl.loop(0, rows // tile)
        def _(i):
            base = pl.multiple_of(i * tile, tile)
            side = 1 if flip and a < QUERY else 0
            store(
                base,
                lax.dot_general(
                    normed[pl.ds(base, tile), :],
                    wholes[a][...],
                    (((1,), (side,)), ((), ())),
                    preferred_element_type=f32,
                ),
            )

    def halo(buffer, length, i):
        return pltpu.make_async_remote_copy(
            src_ref=buffer.at[pl.ds(rows, length)],
            dst_ref=buffer.at[pl.ds(0, length)],
            send_sem=halo_send.at[i],
            recv_sem=halo_recv.at[i],
            device_id={"sp": right},
            device_id_type=MESH,
        )

    for a in range(QUERY):
        pass_on(a, 1, n)
    send_own(GATE)

    def store_kv(base, value):
        kv[pl.ds(base + WINDOW, tile), :] = value.astype(bf16)

    project(0, store_kv)

    @pl.when(jnp.logical_not(has_left))
    def _():
        kv[pl.ds(0, WINDOW), :] = jnp.zeros((WINDOW, kv.shape[1]), bf16)
        conv_in[pl.ds(0, PAD), :] = jnp.zeros((PAD, conv_in.shape[1]), f32)

    pass_on(QUERY, 1, n)

    @pl.when(has_right)
    def _():
        halo(kv, WINDOW, 0).start()

    def store_query(base, value):
        query[pl.ds(base, tile), :] = value.astype(bf16)

    project(QUERY, store_query)

    heads = query.shape[1] // HEAD_DIM
    query_idx = lax.broadcasted_iota(jnp.int32, (WINDOW, 2 * WINDOW), 0)
    key_idx = lax.broadcasted_iota(jnp.int32, (WINDOW, 2 * WINDOW), 1)
    gap = query_idx + WINDOW - key_idx
    band = (gap >= 0) & (gap < WINDOW)
    lane = lax.broadcasted_iota(jnp.int32, (2 * WINDOW, LANES), 1)
    low = lane < HEAD_DIM
    stat_lane = lax.broadcasted_iota(jnp.int32, (WINDOW, LANES), 1)

    def attend(b, kept):
        base = pl.multiple_of(b * WINDOW, WINDOW)
        both = kv[pl.ds(base, 2 * WINDOW), :].astype(f32)
        turned = pltpu.roll(both, HEAD_DIM, 1)
        zero = jnp.zeros_like(both)
        keys = (jnp.where(low, both, zero).astype(bf16), jnp.where(low, zero, turned).astype(bf16))
        vals = (jnp.where(low, turned, zero).astype(bf16), jnp.where(low, zero, both).astype(bf16))
        stats = jnp.zeros((WINDOW, LANES), f32)
        for pair in range(heads // 2):
            cols = pl.ds(pair * LANES, LANES)
            q = query[pl.ds(base, WINDOW), cols]
            out = None
            for side in range(2):
                head = 2 * pair + side
                scores = lax.dot_general(
                    q, keys[side], (((1,), (1,)), ((), ())), preferred_element_type=f32
                ) * HEAD_DIM ** (-0.5)
                scores = jnp.where(kept, scores, -jnp.inf)
                sink = jnp.full((WINDOW, 1), sink_ref[head], f32)
                top = jnp.maximum(jnp.max(scores, axis=-1, keepdims=True), sink)
                raised = jnp.exp(scores - top)
                total = jnp.sum(raised, axis=-1, keepdims=True) + jnp.exp(sink - top)
                weights = (raised * (1.0 / total)).astype(bf16)
                part = jnp.dot(weights, vals[side], preferred_element_type=f32)
                out = part if out is None else out + part
                stats = jnp.where(stat_lane == head, top + jnp.log(total), stats)
            attended[pl.ds(base, WINDOW), cols] = out
        log_ref[:, pl.ds(base, WINDOW)] = jnp.transpose(stats)[:heads]

    def attend_range(first, last):
        @pl.loop(first, last)
        def _(b):
            attend(b, band)

    cut = [1 + (n - 1) * i // 3 for i in range(4)]
    mid = 1 + (blocks - 1) // 2
    attend_range(1, mid)
    pass_on(CONV, cut[0], cut[1])
    attend_range(mid, blocks)
    pass_on(CONV, cut[1], cut[2])

    @pl.when(has_left)
    def _():
        halo(kv, WINDOW, 0).wait_recv()

    attend(0, band & ((key_idx >= WINDOW) | has_left))
    pass_on(CONV, cut[2], cut[3])

    def store_conv(base, value):
        conv_in[pl.ds(base + PAD, tile), :] = value.astype(bf16).astype(f32)

    project(CONV, store_conv)
    early = min(2, n - 1)
    pass_on(GATE, 1, early)

    @pl.when(has_right)
    def _():
        halo(conv_in, PAD, 1).start()

    pass_on(GATE, early, n - 1)

    far = jnp.where(2 * me >= n, 0, n - 1)

    def gate_part(base, shard):
        at = pl.ds(pl.multiple_of(shard * depth, depth), depth)
        return jnp.dot(
            normed[pl.ds(base, tile), at], cg_all[at, :], preferred_element_type=f32
        )

    if flip:

        @pl.loop(0, rows // tile)
        def _(i):
            base = pl.multiple_of(i * tile, tile)
            part = gate_part(base, lax.rem(far + 1, n))
            for j in range(2, n):
                part = part + gate_part(base, lax.rem(far + j, n))
            gate_sum[pl.ds(base, tile), :] = part

    pass_on(GATE, n - 1, n)

    @pl.when(has_left)
    def _():
        halo(conv_in, PAD, 1).wait_recv()

    def store_mixed(base, value):
        gate = value.astype(bf16).astype(f32)
        taps = taps_ref[...].astype(f32)
        near = conv_in[pl.ds(base, tile + PAD), :]
        total = jnp.zeros_like(gate)
        for k in range(TAPS):
            start = PAD - TAPS + 1 + k
            total = total + taps[k : k + 1] * near[start : start + tile]
        mixed_ref[pl.ds(base, tile), :] = (attended[pl.ds(base, tile), :] + gate * total).astype(bf16)

    if flip:

        @pl.loop(0, rows // tile)
        def _(i):
            base = pl.multiple_of(i * tile, tile)
            store_mixed(base, gate_sum[pl.ds(base, tile), :] + gate_part(base, far))

    else:
        project(GATE, store_mixed)

    @pl.when(has_right)
    def _():
        halo(kv, WINDOW, 0).wait_send()
        halo(conv_in, PAD, 1).wait_send()

    for a in range(arrays):

        @pl.when(has_right)
        def _():
            @pl.loop(0, me + 1)
            def _(s):
                hop(a, s, True).wait_send()

        @pl.when(has_left)
        def _():
            @pl.loop(me, n)
            def _(s):
                hop(a, s, False).wait_send()


def paired_kernel(tok_ref, gain_ref, *refs):
    shards = refs[:5]
    (
        taps_ref, sink_ref, mixed_ref, log_ref,
        tok, normed, other, kv_all, q_all, stage, conv_w, kv, query, q_part, attended,
        conv_in, convolved, sums, conv_out, conv_back, turned_taps, edge_out, edge_in,
        tok_sem, own_sem, recv_sem, mate_sem, peer_sem, halo_send, halo_recv,
        x_send, x_recv, out_send, out_recv,
    ) = refs[5:]
    f32, bf16 = jnp.float32, jnp.bfloat16
    me, fs, tp = lax.axis_index("sp"), lax.axis_index("fs"), lax.axis_index("tp")
    low = me < 2
    end = (me == 0) | (me == 3)
    middle = jnp.logical_not(end)
    mate = me + 1 - 2 * lax.rem(me, 2)
    peer = jnp.where(end, 3 - mate, 3 - me)
    far = jnp.where(low, 3, 0)
    first = jnp.where(low, 0, 1)
    has_left, has_right = me > 0, me < 3
    right = jnp.minimum(me + 1, 3)
    across, along = fs + 1 - 2 * lax.rem(fs, 2), lax.rem(fs + 2, 4)
    diagonal = 3 - fs
    twin = 1 - tp
    rows = tok.shape[0]
    depth = shards[2].shape[0]
    blocks = rows // WINDOW
    width = q_all.shape[1]
    widths = (width // 4, width // 4, width // 4, width // 8, width // 8)
    groups = range(len(widths))
    channel = [sum(widths[:g]) for g in groups]
    K, V, Q, A, B, C, D, E = units = range(8)

    parts = 8
    part_rows = rows // parts
    pieces = 4
    piece = part_rows // pieces
    own_part = fs * 2 + tp

    def part_at(i):
        return lax.rem(own_part + i, parts)

    def rows_of(start, length):
        return pl.ds(pl.multiple_of(start, 16), length)

    tok_copies = []
    for i in range(parts):
        at = rows_of(part_at(i) * part_rows, part_rows)
        tok_copies.append(pltpu.make_async_copy(tok_ref.at[at], tok.at[at], tok_sem.at[i]))
    for copy in tok_copies:
        copy.start()

    def shard_at(shard):
        return pl.ds(pl.multiple_of(shard * depth, depth), depth)

    def place(u, shard):
        at = shard_at(shard)
        if u < Q:
            return kv_all.at[pl.ds(u * HEAD_DIM, HEAD_DIM), at]
        if u == Q:
            return q_all.at[at]
        return conv_w.at[pl.ds(2 * channel[u - A], 2 * widths[u - A]), at]

    own_copies = [pltpu.make_async_copy(shards[u], place(u, me), own_sem.at[u]) for u in (K, V, Q)]
    own_copies += [pltpu.make_async_copy(shards[3 + j], stage.at[j], own_sem.at[3 + j]) for j in range(2)]
    for copy in own_copies:
        copy.start()

    def norm_part(i):
        tok_copies[i].wait()
        norm_rows = 64

        @pl.loop(0, part_rows // norm_rows)
        def _(j):
            at = rows_of(part_at(i) * part_rows + j * norm_rows, norm_rows)
            wide = tok[at, :].astype(f32)
            scale = lax.rsqrt(jnp.mean(wide * wide, axis=-1, keepdims=True) + EPS)
            normed[at, :] = (wide * scale * gain_ref[...]).astype(bf16)

    barrier = pltpu.get_barrier_semaphore()

    def greet(**device):
        pl.semaphore_signal(barrier, inc=1, device_id=device, device_id_type=MESH)

    greet(sp=mate)

    @pl.when(middle)
    def _():
        greet(sp=peer)
        greet(fs=across)
        greet(fs=along)
        greet(tp=twin)

    norm_part(0)
    own_copies[3].wait()
    own_copies[4].wait()
    for j in range(2):
        for block in range(depth // LANES):
            turned = jnp.transpose(stage[j, pl.ds(block * LANES, LANES), :].astype(f32)).astype(bf16)
            at = pl.ds(pl.multiple_of(me * depth + block * LANES, LANES), LANES)
            for g in groups:
                to = pl.ds(2 * channel[g] + j * widths[g], widths[g])
                conv_w[to, at] = turned[channel[g] : channel[g] + widths[g]]
    taps = taps_ref[...].astype(f32)
    turned_taps[...] = jnp.transpose(jnp.concatenate([taps, jnp.zeros((8 - TAPS, width), f32)], axis=0))
    for u in (K, V, Q):
        own_copies[u].wait()

    pl.semaphore_wait(barrier, jnp.where(middle, 5, 1))

    def hop(u, shard, to_mate):
        return pltpu.make_async_remote_copy(
            src_ref=place(u, shard),
            dst_ref=place(u, shard),
            send_sem=(mate_sem if to_mate else peer_sem).at[u, shard],
            recv_sem=recv_sem.at[u, shard],
            device_id={"sp": mate if to_mate else peer},
            device_id_type=MESH,
        )

    def arrived(u, shard):
        hop(u, shard, True).wait_recv()

    def piece_at(part, h):
        return rows_of(part * part_rows + h * piece, piece)

    def piece_copy(buffer, part, h, i, **device):
        at = piece_at(part, h)
        return pltpu.make_async_remote_copy(
            src_ref=buffer.at[at],
            dst_ref=other.at[at],
            send_sem=x_send.at[i],
            recv_sem=x_recv.at[part * pieces + h],
            device_id=device,
            device_id_type=MESH,
        )

    def piece_arrived(part, h):
        piece_copy(other, part, h, 0, sp=mate).wait_recv()

    across_part, along_part, diagonal_part = across * 2 + tp, along * 2 + tp, diagonal * 2 + tp
    relays = [(own_part, h, ("tp", "fs_across", "fs_along")) for h in range(pieces)]
    relays += [(across_part, h, ("tp", "fs_along")[: 2 - h % 2]) for h in range(pieces)]
    relays += [(along_part, h, ("tp", "fs_across")[: 1 + h % 2]) for h in range(pieces)]
    relays += [(diagonal_part, h, ("tp",)) for h in range(pieces)]
    OWN_X, ACROSS, ALONG, DIAGONAL = (pieces * j for j in range(4))
    devices = {"tp": {"tp": twin}, "fs_across": {"fs": across}, "fs_along": {"fs": along}}

    def relay_copies(j):
        base = sum(len(to) for _, _, to in relays[:j])
        part, h, to = relays[j]
        return [piece_copy(other, part, h, base + i, **devices[d]) for i, d in enumerate(to)]

    def relay(*which):
        for j in which:
            piece_arrived(relays[j][0], relays[j][1])
            for copy in relay_copies(j):
                copy.start()

    def send(to_mate, shard, *which):
        for u in which:
            hop(u, shard, to_mate).start()

    def forward(to_mate, shard, *which):
        for u in which:
            arrived(u, shard)
            hop(u, shard, to_mate).start()

    def pieces_out(*which):
        for h in which:
            piece_copy(normed, own_part, h, h, sp=mate).start()

    @pl.when(end)
    def _():
        pieces_out(0, 1)
        send(True, me, K, V, Q)
        pieces_out(2, 3)
        send(True, me, A, B, C, D, E)

    @pl.when(middle)
    def _():
        send(False, me, K, V, Q, A)
        send(True, me, K, V, Q)

    for i in range(1, parts):
        norm_part(i)

    @pl.when(middle)
    def _():
        relay(OWN_X)
        forward(True, peer, K, V)
        relay(OWN_X + 1, ACROSS, ALONG)
        forward(False, mate, K, V)
        send(False, me, B)
        forward(True, peer, Q)
        relay(ACROSS + 1, ALONG + 1)
        forward(True, far, K)
        forward(False, mate, Q)
        send(False, me, C)
        forward(True, far, V)

    @pl.when(end)
    def _():
        for shard in (mate, peer, far):
            for u in (K, V):
                arrived(u, shard)

    tile = 512

    @pl.loop(0, rows // tile)
    def _(i):
        base = pl.multiple_of(i * tile, tile)
        kv[pl.ds(base + WINDOW, tile), :] = lax.dot_general(
            normed[pl.ds(base, tile), :], kv_all[...], (((1,), (1,)), ((), ())), preferred_element_type=f32
        ).astype(bf16)

    def halo(buffer, start, length, i):
        return pltpu.make_async_remote_copy(
            src_ref=buffer.at[pl.ds(start, length)],
            dst_ref=buffer.at[pl.ds(0, length)],
            send_sem=halo_send.at[i],
            recv_sem=halo_recv.at[i],
            device_id={"sp": right},
            device_id_type=MESH,
        )

    kv_halo = halo(kv, rows, WINDOW, 0)

    @pl.when(jnp.logical_not(has_left))
    def _():
        kv[pl.ds(0, WINDOW), :] = jnp.zeros((WINDOW, kv.shape[1]), bf16)

    @pl.when(middle)
    def _():
        relay(DIAGONAL, DIAGONAL + 1)

    @pl.when(end)
    def _():
        arrived(Q, mate)
        arrived(Q, peer)

    early = pl.ds(pl.multiple_of(first * depth, depth), 3 * depth)
    late = pl.ds(pl.multiple_of(far * depth, depth), depth)

    @pl.loop(0, rows // tile)
    def _(i):
        at = pl.ds(pl.multiple_of(i * tile, tile), tile)
        q_part[at, :] = jnp.dot(normed[at, early], q_all[early, :], preferred_element_type=f32)

    @pl.when(has_right)
    def _():
        kv_halo.start()

    @pl.when(middle)
    def _():
        relay(OWN_X + 2, OWN_X + 3, ACROSS + 2, ALONG + 2)
        forward(True, far, Q)
        forward(False, mate, A)

    @pl.when(end)
    def _():
        arrived(Q, far)

    @pl.loop(0, rows // tile)
    def _(i):
        at = pl.ds(pl.multiple_of(i * tile, tile), tile)
        query[at, :] = (
            q_part[at, :] + jnp.dot(normed[at, late], q_all[late, :], preferred_element_type=f32)
        ).astype(bf16)

    heads = query.shape[1] // HEAD_DIM
    query_idx = lax.broadcasted_iota(jnp.int32, (WINDOW, 2 * WINDOW), 0)
    key_idx = lax.broadcasted_iota(jnp.int32, (WINDOW, 2 * WINDOW), 1)
    gap = query_idx + WINDOW - key_idx
    band = (gap >= 0) & (gap < WINDOW)
    low_lanes = lax.broadcasted_iota(jnp.int32, (2 * WINDOW, LANES), 1) < HEAD_DIM
    lane = lax.broadcasted_iota(jnp.int32, (WINDOW, LANES), 1)
    low_half = lane < HEAD_DIM

    def attend(b, kept):
        base = pl.multiple_of(b * WINDOW, WINDOW)
        both = kv[pl.ds(base, 2 * WINDOW), :].astype(f32)
        turned = pltpu.roll(both, HEAD_DIM, 1)
        zero, one = jnp.zeros_like(both), jnp.ones_like(both)

        def lower(x):
            return jnp.where(low_lanes, x, zero)

        def upper(x):
            return jnp.where(low_lanes, zero, x)

        keys = jnp.concatenate([lower(both), upper(turned)], axis=0).astype(bf16)
        vals = jnp.concatenate([lower(turned), upper(both)], axis=0)
        ones = jnp.concatenate([lower(one), upper(one)], axis=0)
        vals = jnp.concatenate([vals, ones], axis=1).astype(bf16)
        stats = []
        for pair in range(heads // 2):
            cols = pl.ds(pair * LANES, LANES)
            scores = lax.dot_general(
                query[pl.ds(base, WINDOW), cols], keys, (((1,), (1,)), ((), ())), preferred_element_type=f32
            )
            sinks = [sink_ref[2 * pair + side] * LOG2_E for side in range(2)]
            tops, raised = [], []
            for side in range(2):
                part = scores[:, side * 2 * WINDOW : (side + 1) * 2 * WINDOW] * (HEAD_DIM ** (-0.5) * LOG2_E)
                part = jnp.where(kept, part, -jnp.inf)
                tops.append(jnp.maximum(jnp.max(part, axis=-1, keepdims=True), sinks[side]))
                raised.append(jnp.exp2(part - tops[side]).astype(bf16))
            out = jnp.dot(jnp.concatenate(raised, axis=1), vals, preferred_element_type=f32)
            top = jnp.where(low_half, tops[0], tops[1])
            total = out[:, LANES:] + jnp.exp2(jnp.where(low_half, sinks[0], sinks[1]) - top)
            attended[pl.ds(base, WINDOW), cols] = out[:, :LANES] / total
            stats.append(top * LN_2 + jnp.log(total))
        turned_stats = jnp.transpose(jnp.where(lax.rem(lane, 2) == 0, stats[0], stats[1]))
        for pair in range(2):
            for side in range(2):
                row = pair + side * HEAD_DIM
                head = 2 * pair + side
                log_ref[head : head + 1, pl.ds(base, WINDOW)] = turned_stats[row : row + 1]

    services = (
        lambda: relay(ACROSS + 3, ALONG + 3),
        lambda: forward(False, mate, B),
        lambda: relay(DIAGONAL + 2),
    )
    for i, job in enumerate(services):

        @pl.loop(i * (blocks // 2 - 1) // 3, (i + 1) * (blocks // 2 - 1) // 3)
        def _(j):
            attend(2 * j + 1, band)
            attend(2 * j + 2, band)

        @pl.when(middle)
        def _():
            job()

    @pl.when(has_left)
    def _():
        kv_halo.wait_recv()

    attend(blocks - 1, band)
    attend(0, band & ((key_idx >= WINDOW) | has_left))

    own_base, mate_base = jnp.where(me == 1, rows, 0), jnp.where(me == 1, 0, rows)
    bases = (own_base, mate_base)
    sources = (normed, other)
    tiles = rows // tile
    OWN, MATE = 0, 1
    last = tiles - 1
    def tile_at(i):
        return pl.ds(i * tile if isinstance(i, int) else pl.multiple_of(i * tile, tile), tile)

    def out_copy(g, i):
        at = (pl.ds(channel[g], widths[g]), tile_at(i))
        return pltpu.make_async_remote_copy(
            src_ref=conv_out.at[at],
            dst_ref=conv_back.at[at],
            send_sem=out_send.at[g * tiles + i],
            recv_sem=out_recv.at[g * tiles + i],
            device_id={"sp": mate},
            device_id_type=MESH,
        )

    def edge_copy(g):
        return pltpu.make_async_remote_copy(
            src_ref=edge_out.at[g],
            dst_ref=edge_in.at[g],
            send_sem=halo_send.at[1 + g],
            recv_sem=halo_recv.at[1 + g],
            device_id={"sp": right},
            device_id_type=MESH,
        )

    everything = pl.ds(0, conv_w.shape[1])

    def dot(which, tokens, start, length, at):
        return lax.dot_general(
            conv_w[pl.ds(start, length), at],
            sources[which][tokens, at],
            (((1,), (1,)), ((), ())),
            preferred_element_type=f32,
        )

    small = 3
    small_start = 2 * channel[small]
    small_rows = 2 * width - small_start

    def partial(which, i):
        sums[which, :, tile_at(i)] = dot(which, tile_at(i), small_start, small_rows, early)

    def keep(g, at, value):
        value = value.astype(bf16).astype(f32)
        conv_in[pl.ds(channel[g], widths[g]), pl.ds(pl.multiple_of(at + LANES, LANES), value.shape[1])] = value[: widths[g]]
        return value[widths[g] :]

    def convolve(g, at, gate):
        of = pl.ds(channel[g], widths[g])
        near = conv_in[of, pl.ds(pl.multiple_of(at, LANES), tile + LANES)]
        total = jnp.zeros((widths[g], tile), f32)
        for k in range(TAPS):
            moved = near if k == TAPS - 1 else pltpu.roll(near, TAPS - 1 - k, 1)
            total = total + turned_taps[of, k : k + 1] * moved[:, LANES:]
        return gate * total

    def own_edge(g):
        of = pl.ds(channel[g], widths[g])
        tokens = pl.ds(rows - LANES, LANES)
        keep(g, own_base + rows - LANES, dot(OWN, tokens, 2 * channel[g], 2 * widths[g], everything))

        @pl.when(me == 1)
        def _():
            conv_in[of, pl.ds(0, LANES)] = jnp.zeros((widths[g], LANES), f32)
            edge = jnp.transpose(conv_in[of, pl.ds(2 * rows, LANES)])
            edge_out[g, :, pl.ds(0, widths[g])] = edge[LANES - PAD :]
            edge_copy(g).start()

    def mate_tiles(g):
        of = pl.ds(channel[g], widths[g])
        for i in range(tiles):
            at = mate_base + i * tile
            if g < small:
                value = dot(MATE, tile_at(i), 2 * channel[g], 2 * widths[g], everything)
            else:
                value = dot(MATE, tile_at(i), 2 * channel[g], 2 * widths[g], late)
                value = value + sums[MATE, pl.ds(2 * channel[g] - small_start, 2 * widths[g]), tile_at(i)]
            conv_out[of, tile_at(i)] = convolve(g, at, keep(g, at, value)).astype(bf16)
            out_copy(g, i).start()

    def own_tiles(*which):
        @pl.when(me == 2)
        def _():
            for g in which:
                of = pl.ds(channel[g], widths[g])
                edge_copy(g).wait_recv()
                edge = edge_in[g, :, pl.ds(0, widths[g])]
                edge = jnp.concatenate([jnp.zeros((LANES - PAD, widths[g]), f32), edge], axis=0)
                conv_in[of, pl.ds(0, LANES)] = jnp.transpose(edge)

        start = 2 * channel[which[0]]
        length = sum(2 * widths[g] for g in which)
        for i in range(tiles):
            at = own_base + i * tile
            value = dot(OWN, tile_at(i), start, length, everything)
            for g in which:
                row = 2 * channel[g] - start
                gate = keep(g, at, value[row : row + 2 * widths[g]])
                convolved[pl.ds(channel[g], widths[g]), tile_at(i)] = convolve(g, at, gate)

    def mix(half, source):
        cols = pl.ds(half * LANES, LANES)

        @pl.loop(0, rows // LANES)
        def _(i):
            at = pl.ds(pl.multiple_of(i * LANES, LANES), LANES)
            extra = jnp.transpose(source[cols, at].astype(f32))
            mixed_ref[at, cols] = (attended[at, cols] + extra).astype(bf16)

    @pl.when(middle)
    def _():
        forward(False, mate, C)
        send(False, me, D, E)
        relay(DIAGONAL + 3)
        for part in (fs * 2 + twin, across * 2 + twin, along * 2 + twin, diagonal * 2 + twin):
            for h in range(pieces):
                piece_arrived(part, h)

        def ready(*which):
            for u in which:
                arrived(u, peer)
                arrived(u, far)

        for g in range(2):
            ready(A + g)
            own_edge(g)
            mate_tiles(g)
        forward(False, mate, D, E)
        own_tiles(0, 1)
        mix(0, convolved)
        ready(C)
        own_edge(2)
        mate_tiles(2)
        arrived(D, peer)
        arrived(E, peer)
        for i in range(tiles):
            partial(MATE, i)
        for g in (3, 4):
            arrived(A + g, far)
            own_edge(g)
            mate_tiles(g)
        own_tiles(2)
        own_tiles(3, 4)
        mix(1, convolved)

    @pl.when(end)
    def _():
        for half in range(2):
            for g in (groups[:2], groups[2:])[half]:
                for i in range(tiles):
                    out_copy(g, i).wait_recv()
            mix(half, conv_back)

    @pl.when(has_right)
    def _():
        kv_halo.wait_send()

    for u in (K, V, Q):
        hop(u, me, True).wait_send()

    @pl.when(end)
    def _():
        for h in range(pieces):
            piece_copy(normed, own_part, h, h, sp=mate).wait_send()
        for u in units[A:]:
            hop(u, me, True).wait_send()

    @pl.when(middle)
    def _():
        for u in (K, V, Q):
            hop(u, peer, True).wait_send()
            hop(u, far, True).wait_send()
        for u in units:
            hop(u, me, False).wait_send()
            hop(u, mate, False).wait_send()
        for j in range(len(relays)):
            for copy in relay_copies(j):
                copy.wait_send()
        for g in groups:
            for i in range(tiles):
                out_copy(g, i).wait_send()

        @pl.when(me == 1)
        def _():
            for g in groups:
                edge_copy(g).wait_send()


def paired_body(tokens, norm_gain, w_query, w_key, w_value, w_conv_in, w_conv_gate, conv_taps, sink_logits):
    rows, features = tokens.shape
    width = w_query.shape[1]
    f32, bf16 = jnp.float32, jnp.bfloat16
    hbm = pl.BlockSpec(memory_space=pltpu.HBM)
    vmem = pl.BlockSpec(memory_space=pltpu.VMEM)
    smem = pl.BlockSpec(memory_space=pltpu.SMEM)
    dma = pltpu.SemaphoreType.DMA
    tiles = rows // 512
    return pl.pallas_call(
        paired_kernel,
        out_shape=(
            pltpu.VMEM((rows, width), bf16),
            pltpu.VMEM((width // HEAD_DIM, rows), f32),
        ),
        in_specs=[hbm, vmem] + [hbm] * 5 + [vmem, smem],
        out_specs=(vmem, vmem),
        scratch_shapes=[
            pltpu.VMEM((rows, features), bf16),
            pltpu.VMEM((rows, features), bf16),
            pltpu.VMEM((rows, features), bf16),
            pltpu.VMEM((2 * HEAD_DIM, features), bf16),
            pltpu.VMEM((features, width), bf16),
            pltpu.VMEM((2, w_query.shape[0], width), bf16),
            pltpu.VMEM((2 * width, features), bf16),
            pltpu.VMEM((rows + WINDOW, 2 * HEAD_DIM), bf16),
            pltpu.VMEM((rows, width), bf16),
            pltpu.VMEM((rows, width), f32),
            pltpu.VMEM((rows, width), f32),
            pltpu.VMEM((width, LANES + 2 * rows), f32),
            pltpu.VMEM((width, rows), f32),
            pltpu.VMEM((2, width // 2, rows), f32),
            pltpu.VMEM((width, rows), bf16),
            pltpu.VMEM((width, rows), bf16),
            pltpu.VMEM((width, 8), f32),
            pltpu.VMEM((5, PAD, LANES), f32),
            pltpu.VMEM((5, PAD, LANES), f32),
            dma((8,)),
            dma((5,)),
            dma((8, 4)),
            dma((8, 4)),
            dma((8, 4)),
            dma((6,)),
            dma((6,)),
            dma((28,)),
            dma((32,)),
            dma((5 * tiles,)),
            dma((5 * tiles,)),
        ],
        compiler_params=pltpu.CompilerParams(
            collective_id=0, has_side_effects=True, vmem_limit_bytes=59 << 20
        ),
        name="paired_attend_convolve",
    )(tokens, norm_gain.reshape(1, -1), w_key.T, w_value.T, w_query, w_conv_in, w_conv_gate, conv_taps, sink_logits)


def line_body(n, tokens, norm_gain, w_query, w_key, w_value, w_conv_in, w_conv_gate, conv_taps, sink_logits):
    rows, features = tokens.shape
    width, kv_width = w_query.shape[1], w_key.shape[1] + w_value.shape[1]
    assert w_key.shape[1] == HEAD_DIM and width % LANES == 0
    depth = w_query.shape[0]
    flip = depth % LANES == 0 and 2 < n <= 16
    if flip:
        w_kv, kv_shape = (w_key.T, w_value.T), (kv_width, features)
    else:
        w_kv, kv_shape = (jnp.concatenate([w_key, w_value], axis=1),), (features, kv_width)
    arrays = 3 + len(w_kv)
    f32, bf16 = jnp.float32, jnp.bfloat16
    hbm = pl.BlockSpec(memory_space=pltpu.HBM)
    vmem = pl.BlockSpec(memory_space=pltpu.VMEM)
    smem = pl.BlockSpec(memory_space=pltpu.SMEM)
    dma = pltpu.SemaphoreType.DMA
    return pl.pallas_call(
        functools.partial(line_kernel, n, flip),
        out_shape=(
            pltpu.VMEM((rows, width), bf16),
            pltpu.VMEM((width // HEAD_DIM, rows), f32),
        ),
        in_specs=[hbm, vmem] + [hbm] * arrays + [vmem, smem],
        out_specs=(vmem, vmem),
        scratch_shapes=[
            pltpu.VMEM((rows, features), bf16),
            pltpu.VMEM((rows, features), bf16),
            pltpu.VMEM(kv_shape, bf16),
            pltpu.VMEM((features, width), bf16),
            pltpu.VMEM((features, width), bf16),
            pltpu.VMEM((features, width), bf16),
            pltpu.VMEM((rows + WINDOW, kv_width), bf16),
            pltpu.VMEM((rows, width), bf16),
            pltpu.VMEM((rows, width), f32),
            pltpu.VMEM((rows + PAD, width), f32),
            pltpu.VMEM((rows, width), f32),
            dma((4,)),
            dma((arrays,)),
            dma((arrays, n)),
            dma((arrays, n)),
            dma((arrays, n)),
            dma((2,)),
            dma((2,)),
        ],
        compiler_params=pltpu.CompilerParams(
            collective_id=0, has_side_effects=True, vmem_limit_bytes=59 << 20
        ),
        name="gather_attend_convolve",
    )(tokens, norm_gain.reshape(1, -1), *w_kv, w_query, w_conv_in, w_conv_gate, conv_taps, sink_logits)


def body(n, fs, tp, *arrays):
    rows, width, depth = arrays[0].shape[0], arrays[2].shape[1], arrays[2].shape[0]
    square = n == 4 and fs == 4 and tp == 2
    if square and width == 2 * LANES and depth % LANES == 0 and rows % (8 * LANES) == 0:
        return paired_body(*arrays)
    return line_body(n, *arrays)


def solution(mesh):
    return jax.shard_map(
        functools.partial(body, mesh.shape["sp"], mesh.shape["fs"], mesh.shape["tp"]),
        mesh=mesh,
        in_specs=(
            P("sp", None),
            P(),
            P("sp", ("fs", "tp")),
            P("sp", ("fs", "tp")),
            P("sp", ("fs", "tp")),
            P("sp", ("fs", "tp")),
            P("sp", ("fs", "tp")),
            P(None, ("fs", "tp")),
            P(("fs", "tp")),
        ),
        out_specs=(P("sp", ("fs", "tp")), P(("fs", "tp"), "sp")),
        check_vma=False,
    )
```

```python
import functools
import math

import jax
import jax.numpy as jnp
from jax import lax
from jax.experimental import pallas as pl
from jax.experimental.pallas import tpu as pltpu
from jax.sharding import PartitionSpec as P

HEAD_DIM = 64
WINDOW = 128
TAPS = 3
EPS = 1e-06
LANES = 128
PAD = 8
LOG2_E = math.log2(math.e)
LN_2 = math.log(2)
MESH = pl.DeviceIdType.MESH


def line_kernel(
    n, flip, tok_ref, gain_ref, *refs
):
    arrays = 5 if flip else 4
    shards = refs[:arrays]
    (
        taps_ref, sink_ref, mixed_ref, log_ref,
        tok, normed, kv_all, q_all, ci_all, cg_all, kv, query, attended, conv_in, gate_sum,
        tok_sem, own_sem, recv_sem, right_sem, left_sem, halo_send, halo_recv,
    ) = refs[arrays:]
    QUERY, CONV, GATE = arrays - 3, arrays - 2, arrays - 1
    me = lax.axis_index("sp")
    rows = tok.shape[0]
    depth = shards[QUERY].shape[0]
    wholes = (kv_all, kv_all, q_all, ci_all, cg_all)[5 - arrays :]
    has_left, has_right = me > 0, me < n - 1
    left, right = jnp.maximum(me - 1, 0), jnp.minimum(me + 1, n - 1)
    blocks = rows // WINDOW
    f32, bf16 = jnp.float32, jnp.bfloat16

    step_rows = rows // 4
    tok_copies = [
        pltpu.make_async_copy(
            tok_ref.at[pl.ds(i * step_rows, step_rows)], tok.at[pl.ds(i * step_rows, step_rows)], tok_sem.at[i]
        )
        for i in range(4)
    ]
    for copy in tok_copies:
        copy.start()

    def place(a, shard):
        at = pl.ds(pl.multiple_of(shard * depth, depth), depth)
        if flip and a < QUERY:
            return kv_all.at[pl.ds(a * HEAD_DIM, HEAD_DIM), at]
        return wholes[a].at[at]

    own_copies = [pltpu.make_async_copy(shards[a], place(a, me), own_sem.at[a]) for a in range(arrays)]
    for copy in own_copies:
        copy.start()

    barrier = pltpu.get_barrier_semaphore()

    @pl.when(has_left)
    def _():
        pl.semaphore_signal(barrier, inc=1, device_id={"sp": left}, device_id_type=MESH)

    @pl.when(has_right)
    def _():
        pl.semaphore_signal(barrier, inc=1, device_id={"sp": right}, device_id_type=MESH)

    pl.semaphore_wait(barrier, has_left.astype(jnp.int32) + has_right.astype(jnp.int32))

    def hop(a, shard, to_right, own=False):
        return pltpu.make_async_remote_copy(
            src_ref=shards[a] if own else place(a, shard),
            dst_ref=place(a, shard),
            send_sem=(right_sem if to_right else left_sem).at[a, shard],
            recv_sem=recv_sem.at[a, shard],
            device_id={"sp": right if to_right else left},
            device_id_type=MESH,
        )

    def send_own(a):
        @pl.when(has_right)
        def _():
            hop(a, me, True, True).start()

        @pl.when(has_left)
        def _():
            hop(a, me, False, True).start()

    def pass_on(a, first, last):
        def step(k, carry):
            @pl.when(me - k >= 0)
            def _():
                shard = me - k
                hop(a, shard, False).wait_recv()

                @pl.when(has_right)
                def _():
                    hop(a, shard, True).start()

            @pl.when(me + k < n)
            def _():
                shard = me + k
                hop(a, shard, True).wait_recv()

                @pl.when(has_left)
                def _():
                    hop(a, shard, False).start()

            return carry

        lax.fori_loop(first, last, step, 0)

    for a in range(GATE):
        send_own(a)

    norm_rows = 64
    for i in range(4):
        tok_copies[i].wait()

        @pl.loop(0, step_rows // norm_rows)
        def _(j):
            at = pl.ds(pl.multiple_of(i * step_rows + j * norm_rows, norm_rows), norm_rows)
            wide = tok[at, :].astype(f32)
            scale = lax.rsqrt(jnp.mean(wide * wide, axis=-1, keepdims=True) + EPS)
            normed[at, :] = (wide * scale * gain_ref[...]).astype(bf16)

    for copy in own_copies:
        copy.wait()

    tile = 256

    def project(a, store):
        @pl.loop(0, rows // tile)
        def _(i):
            base = pl.multiple_of(i * tile, tile)
            side = 1 if flip and a < QUERY else 0
            store(
                base,
                lax.dot_general(
                    normed[pl.ds(base, tile), :],
                    wholes[a][...],
                    (((1,), (side,)), ((), ())),
                    preferred_element_type=f32,
                ),
            )

    def halo(buffer, length, i):
        return pltpu.make_async_remote_copy(
            src_ref=buffer.at[pl.ds(rows, length)],
            dst_ref=buffer.at[pl.ds(0, length)],
            send_sem=halo_send.at[i],
            recv_sem=halo_recv.at[i],
            device_id={"sp": right},
            device_id_type=MESH,
        )

    for a in range(QUERY):
        pass_on(a, 1, n)
    send_own(GATE)

    def store_kv(base, value):
        kv[pl.ds(base + WINDOW, tile), :] = value.astype(bf16)

    project(0, store_kv)

    @pl.when(jnp.logical_not(has_left))
    def _():
        kv[pl.ds(0, WINDOW), :] = jnp.zeros((WINDOW, kv.shape[1]), bf16)
        conv_in[pl.ds(0, PAD), :] = jnp.zeros((PAD, conv_in.shape[1]), f32)

    pass_on(QUERY, 1, n)

    @pl.when(has_right)
    def _():
        halo(kv, WINDOW, 0).start()

    def store_query(base, value):
        query[pl.ds(base, tile), :] = value.astype(bf16)

    project(QUERY, store_query)

    heads = query.shape[1] // HEAD_DIM
    query_idx = lax.broadcasted_iota(jnp.int32, (WINDOW, 2 * WINDOW), 0)
    key_idx = lax.broadcasted_iota(jnp.int32, (WINDOW, 2 * WINDOW), 1)
    gap = query_idx + WINDOW - key_idx
    band = (gap >= 0) & (gap < WINDOW)
    lane = lax.broadcasted_iota(jnp.int32, (2 * WINDOW, LANES), 1)
    low = lane < HEAD_DIM
    stat_lane = lax.broadcasted_iota(jnp.int32, (WINDOW, LANES), 1)

    def attend(b, kept):
        base = pl.multiple_of(b * WINDOW, WINDOW)
        both = kv[pl.ds(base, 2 * WINDOW), :].astype(f32)
        turned = pltpu.roll(both, HEAD_DIM, 1)
        zero = jnp.zeros_like(both)
        keys = (jnp.where(low, both, zero).astype(bf16), jnp.where(low, zero, turned).astype(bf16))
        vals = (jnp.where(low, turned, zero).astype(bf16), jnp.where(low, zero, both).astype(bf16))
        stats = jnp.zeros((WINDOW, LANES), f32)
        for pair in range(heads // 2):
            cols = pl.ds(pair * LANES, LANES)
            q = query[pl.ds(base, WINDOW), cols]
            out = None
            for side in range(2):
                head = 2 * pair + side
                scores = lax.dot_general(
                    q, keys[side], (((1,), (1,)), ((), ())), preferred_element_type=f32
                ) * HEAD_DIM ** (-0.5)
                scores = jnp.where(kept, scores, -jnp.inf)
                sink = jnp.full((WINDOW, 1), sink_ref[head], f32)
                top = jnp.maximum(jnp.max(scores, axis=-1, keepdims=True), sink)
                raised = jnp.exp(scores - top)
                total = jnp.sum(raised, axis=-1, keepdims=True) + jnp.exp(sink - top)
                weights = (raised * (1.0 / total)).astype(bf16)
                part = jnp.dot(weights, vals[side], preferred_element_type=f32)
                out = part if out is None else out + part
                stats = jnp.where(stat_lane == head, top + jnp.log(total), stats)
            attended[pl.ds(base, WINDOW), cols] = out
        log_ref[:, pl.ds(base, WINDOW)] = jnp.transpose(stats)[:heads]

    def attend_range(first, last):
        @pl.loop(first, last)
        def _(b):
            attend(b, band)

    cut = [1 + (n - 1) * i // 3 for i in range(4)]
    mid = 1 + (blocks - 1) // 2
    attend_range(1, mid)
    pass_on(CONV, cut[0], cut[1])
    attend_range(mid, blocks)
    pass_on(CONV, cut[1], cut[2])

    @pl.when(has_left)
    def _():
        halo(kv, WINDOW, 0).wait_recv()

    attend(0, band & ((key_idx >= WINDOW) | has_left))
    pass_on(CONV, cut[2], cut[3])

    def store_conv(base, value):
        conv_in[pl.ds(base + PAD, tile), :] = value.astype(bf16).astype(f32)

    project(CONV, store_conv)
    early = min(2, n - 1)
    pass_on(GATE, 1, early)

    @pl.when(has_right)
    def _():
        halo(conv_in, PAD, 1).start()

    pass_on(GATE, early, n - 1)

    far = jnp.where(2 * me >= n, 0, n - 1)

    def gate_part(base, shard):
        at = pl.ds(pl.multiple_of(shard * depth, depth), depth)
        return jnp.dot(
            normed[pl.ds(base, tile), at], cg_all[at, :], preferred_element_type=f32
        )

    if flip:

        @pl.loop(0, rows // tile)
        def _(i):
            base = pl.multiple_of(i * tile, tile)
            part = gate_part(base, lax.rem(far + 1, n))
            for j in range(2, n):
                part = part + gate_part(base, lax.rem(far + j, n))
            gate_sum[pl.ds(base, tile), :] = part

    pass_on(GATE, n - 1, n)

    @pl.when(has_left)
    def _():
        halo(conv_in, PAD, 1).wait_recv()

    def store_mixed(base, value):
        gate = value.astype(bf16).astype(f32)
        taps = taps_ref[...].astype(f32)
        near = conv_in[pl.ds(base, tile + PAD), :]
        total = jnp.zeros_like(gate)
        for k in range(TAPS):
            start = PAD - TAPS + 1 + k
            total = total + taps[k : k + 1] * near[start : start + tile]
        mixed_ref[pl.ds(base, tile), :] = (attended[pl.ds(base, tile), :] + gate * total).astype(bf16)

    if flip:

        @pl.loop(0, rows // tile)
        def _(i):
            base = pl.multiple_of(i * tile, tile)
            store_mixed(base, gate_sum[pl.ds(base, tile), :] + gate_part(base, far))

    else:
        project(GATE, store_mixed)

    @pl.when(has_right)
    def _():
        halo(kv, WINDOW, 0).wait_send()
        halo(conv_in, PAD, 1).wait_send()

    for a in range(arrays):

        @pl.when(has_right)
        def _():
            @pl.loop(0, me + 1)
            def _(s):
                hop(a, s, True).wait_send()

        @pl.when(has_left)
        def _():
            @pl.loop(me, n)
            def _(s):
                hop(a, s, False).wait_send()


def paired_kernel(tok_ref, gain_ref, *refs):
    shards = refs[:5]
    (
        taps_ref, sink_ref, mixed_ref, log_ref,
        tok, normed, other, kv_all, q_all, stage, conv_w, kv, query, q_part, attended,
        conv_in, convolved, sums, conv_out, conv_back, turned_taps, edge_out, edge_in,
        tok_sem, own_sem, recv_sem, mate_sem, peer_sem, halo_send, halo_recv,
        x_send, x_recv, out_send, out_recv,
    ) = refs[5:]
    f32, bf16 = jnp.float32, jnp.bfloat16
    me, fs, tp = lax.axis_index("sp"), lax.axis_index("fs"), lax.axis_index("tp")
    low = me < 2
    end = (me == 0) | (me == 3)
    middle = jnp.logical_not(end)
    mate = me + 1 - 2 * lax.rem(me, 2)
    peer = jnp.where(end, 3 - mate, 3 - me)
    far = jnp.where(low, 3, 0)
    first = jnp.where(low, 0, 1)
    has_left, has_right = me > 0, me < 3
    right = jnp.minimum(me + 1, 3)
    across, along = fs + 1 - 2 * lax.rem(fs, 2), lax.rem(fs + 2, 4)
    diagonal = 3 - fs
    twin = 1 - tp
    rows = tok.shape[0]
    depth = shards[2].shape[0]
    blocks = rows // WINDOW
    width = q_all.shape[1]
    widths = (width // 4, width // 4, width // 4, width // 8, width // 8)
    groups = range(len(widths))
    channel = [sum(widths[:g]) for g in groups]
    K, V, Q, A, B, C, D, E = units = range(8)

    parts = 8
    part_rows = rows // parts
    pieces = 4
    piece = part_rows // pieces
    own_part = fs * 2 + tp

    def part_at(i):
        return lax.rem(own_part + i, parts)

    def rows_of(start, length):
        return pl.ds(pl.multiple_of(start, 16), length)

    tok_copies = []
    for i in range(parts):
        at = rows_of(part_at(i) * part_rows, part_rows)
        tok_copies.append(pltpu.make_async_copy(tok_ref.at[at], tok.at[at], tok_sem.at[i]))
    for copy in tok_copies:
        copy.start()

    def shard_at(shard):
        return pl.ds(pl.multiple_of(shard * depth, depth), depth)

    def place(u, shard):
        at = shard_at(shard)
        if u < Q:
            return kv_all.at[pl.ds(u * HEAD_DIM, HEAD_DIM), at]
        if u == Q:
            return q_all.at[at]
        return conv_w.at[pl.ds(2 * channel[u - A], 2 * widths[u - A]), at]

    own_copies = [pltpu.make_async_copy(shards[u], place(u, me), own_sem.at[u]) for u in (K, V, Q)]
    own_copies += [pltpu.make_async_copy(shards[3 + j], stage.at[j], own_sem.at[3 + j]) for j in range(2)]
    for copy in own_copies:
        copy.start()

    def norm_part(i):
        tok_copies[i].wait()
        norm_rows = 64

        @pl.loop(0, part_rows // norm_rows)
        def _(j):
            at = rows_of(part_at(i) * part_rows + j * norm_rows, norm_rows)
            wide = tok[at, :].astype(f32)
            scale = lax.rsqrt(jnp.mean(wide * wide, axis=-1, keepdims=True) + EPS)
            normed[at, :] = (wide * scale * gain_ref[...]).astype(bf16)

    barrier = pltpu.get_barrier_semaphore()

    def greet(**device):
        pl.semaphore_signal(barrier, inc=1, device_id=device, device_id_type=MESH)

    greet(sp=mate)

    @pl.when(middle)
    def _():
        greet(sp=peer)
        greet(fs=across)
        greet(fs=along)
        greet(tp=twin)

    norm_part(0)
    own_copies[3].wait()
    own_copies[4].wait()
    for j in range(2):
        for block in range(depth // LANES):
            turned = jnp.transpose(stage[j, pl.ds(block * LANES, LANES), :].astype(f32)).astype(bf16)
            at = pl.ds(pl.multiple_of(me * depth + block * LANES, LANES), LANES)
            for g in groups:
                to = pl.ds(2 * channel[g] + j * widths[g], widths[g])
                conv_w[to, at] = turned[channel[g] : channel[g] + widths[g]]
    taps = taps_ref[...].astype(f32)
    turned_taps[...] = jnp.transpose(jnp.concatenate([taps, jnp.zeros((8 - TAPS, width), f32)], axis=0))
    for u in (K, V, Q):
        own_copies[u].wait()

    pl.semaphore_wait(barrier, jnp.where(middle, 5, 1))

    def hop(u, shard, to_mate):
        return pltpu.make_async_remote_copy(
            src_ref=place(u, shard),
            dst_ref=place(u, shard),
            send_sem=(mate_sem if to_mate else peer_sem).at[u, shard],
            recv_sem=recv_sem.at[u, shard],
            device_id={"sp": mate if to_mate else peer},
            device_id_type=MESH,
        )

    def arrived(u, shard):
        hop(u, shard, True).wait_recv()

    def piece_at(part, h):
        return rows_of(part * part_rows + h * piece, piece)

    def piece_copy(buffer, part, h, i, **device):
        at = piece_at(part, h)
        return pltpu.make_async_remote_copy(
            src_ref=buffer.at[at],
            dst_ref=other.at[at],
            send_sem=x_send.at[i],
            recv_sem=x_recv.at[part * pieces + h],
            device_id=device,
            device_id_type=MESH,
        )

    def piece_arrived(part, h):
        piece_copy(other, part, h, 0, sp=mate).wait_recv()

    across_part, along_part, diagonal_part = across * 2 + tp, along * 2 + tp, diagonal * 2 + tp
    relays = [(own_part, h, ("tp", "fs_across", "fs_along")) for h in range(pieces)]
    relays += [(across_part, h, ("tp", "fs_along")[: 2 - h % 2]) for h in range(pieces)]
    relays += [(along_part, h, ("tp", "fs_across")[: 1 + h % 2]) for h in range(pieces)]
    relays += [(diagonal_part, h, ("tp",)) for h in range(pieces)]
    OWN_X, ACROSS, ALONG, DIAGONAL = (pieces * j for j in range(4))
    devices = {"tp": {"tp": twin}, "fs_across": {"fs": across}, "fs_along": {"fs": along}}

    def relay_copies(j):
        base = sum(len(to) for _, _, to in relays[:j])
        part, h, to = relays[j]
        return [piece_copy(other, part, h, base + i, **devices[d]) for i, d in enumerate(to)]

    def relay(*which):
        for j in which:
            piece_arrived(relays[j][0], relays[j][1])
            for copy in relay_copies(j):
                copy.start()

    def send(to_mate, shard, *which):
        for u in which:
            hop(u, shard, to_mate).start()

    def forward(to_mate, shard, *which):
        for u in which:
            arrived(u, shard)
            hop(u, shard, to_mate).start()

    def pieces_out(*which):
        for h in which:
            piece_copy(normed, own_part, h, h, sp=mate).start()

    @pl.when(end)
    def _():
        pieces_out(*range(pieces))
        send(True, me, K, V, Q, A, B, C)

    @pl.when(middle)
    def _():
        send(False, me, K, V, Q, A, B, C)
        send(True, me, K, V, Q)

    for i in range(1, parts):
        norm_part(i)

    @pl.when(middle)
    def _():
        relay(OWN_X)
        forward(True, peer, K, V)
        relay(OWN_X + 1, ACROSS, ALONG)
        forward(True, peer, Q)
        relay(OWN_X + 2, ACROSS + 1, ALONG + 1, OWN_X + 3, ACROSS + 2, ALONG + 2)
        forward(False, mate, K, V)
        send(False, me, D, E)
        relay(ACROSS + 3, ALONG + 3, DIAGONAL, DIAGONAL + 1)
        forward(True, far, K, V)

    @pl.when(end)
    def _():
        for shard in (mate, peer, far):
            for u in (K, V):
                arrived(u, shard)

    tile = 512

    @pl.loop(0, rows // tile)
    def _(i):
        base = pl.multiple_of(i * tile, tile)
        kv[pl.ds(base + WINDOW, tile), :] = lax.dot_general(
            normed[pl.ds(base, tile), :], kv_all[...], (((1,), (1,)), ((), ())), preferred_element_type=f32
        ).astype(bf16)

    def halo(buffer, start, length, i):
        return pltpu.make_async_remote_copy(
            src_ref=buffer.at[pl.ds(start, length)],
            dst_ref=buffer.at[pl.ds(0, length)],
            send_sem=halo_send.at[i],
            recv_sem=halo_recv.at[i],
            device_id={"sp": right},
            device_id_type=MESH,
        )

    kv_halo = halo(kv, rows, WINDOW, 0)

    @pl.when(jnp.logical_not(has_left))
    def _():
        kv[pl.ds(0, WINDOW), :] = jnp.zeros((WINDOW, kv.shape[1]), bf16)

    @pl.when(has_right)
    def _():
        kv_halo.start()

    @pl.when(middle)
    def _():
        forward(False, mate, Q)

    @pl.when(end)
    def _():
        send(True, me, D, E)
        arrived(Q, mate)
        arrived(Q, peer)

    early = pl.ds(pl.multiple_of(first * depth, depth), 3 * depth)
    late = pl.ds(pl.multiple_of(far * depth, depth), depth)

    @pl.loop(0, rows // tile)
    def _(i):
        at = pl.ds(pl.multiple_of(i * tile, tile), tile)
        q_part[at, :] = jnp.dot(normed[at, early], q_all[early, :], preferred_element_type=f32)

    own_base, mate_base = jnp.where(me == 1, rows, 0), jnp.where(me == 1, 0, rows)
    bases = (own_base, mate_base)
    sources = (normed, other)
    tiles = rows // tile
    OWN, MATE = 0, 1
    last = tiles - 1
    def tile_at(i):
        return pl.ds(i * tile if isinstance(i, int) else pl.multiple_of(i * tile, tile), tile)

    def out_copy(g, i):
        at = (pl.ds(channel[g], widths[g]), tile_at(i))
        return pltpu.make_async_remote_copy(
            src_ref=conv_out.at[at],
            dst_ref=conv_back.at[at],
            send_sem=out_send.at[g * tiles + i],
            recv_sem=out_recv.at[g * tiles + i],
            device_id={"sp": mate},
            device_id_type=MESH,
        )

    def edge_copy(g):
        return pltpu.make_async_remote_copy(
            src_ref=edge_out.at[g],
            dst_ref=edge_in.at[g],
            send_sem=halo_send.at[1 + g],
            recv_sem=halo_recv.at[1 + g],
            device_id={"sp": right},
            device_id_type=MESH,
        )

    center = pl.ds(depth, 2 * depth)

    def dot(which, tokens, start, length, at):
        return lax.dot_general(
            conv_w[pl.ds(start, length), at],
            sources[which][tokens, at],
            (((1,), (1,)), ((), ())),
            preferred_element_type=f32,
        )

    def partial(which, u, v, at, fresh):
        start = 2 * channel[u - A]
        span = pl.ds(start, 2 * channel[v - A] + 2 * widths[v - A] - start)
        for i in range(tiles):
            value = dot(which, tile_at(i), span.start, span.size, at)
            sums[which, span, tile_at(i)] = value if fresh else sums[which, span, tile_at(i)] + value

    def product(which, tokens, start, length):
        return sums[which, pl.ds(start, length), tokens] + dot(which, tokens, start, length, late)

    def keep(g, at, value):
        value = value.astype(bf16).astype(f32)
        conv_in[pl.ds(channel[g], widths[g]), pl.ds(pl.multiple_of(at + LANES, LANES), value.shape[1])] = value[: widths[g]]
        return value[widths[g] :]

    def convolve(g, at, gate):
        of = pl.ds(channel[g], widths[g])
        near = conv_in[of, pl.ds(pl.multiple_of(at, LANES), tile + LANES)]
        total = jnp.zeros((widths[g], tile), f32)
        for k in range(TAPS):
            moved = near if k == TAPS - 1 else pltpu.roll(near, TAPS - 1 - k, 1)
            total = total + turned_taps[of, k : k + 1] * moved[:, LANES:]
        return gate * total

    def own_edge(g):
        of = pl.ds(channel[g], widths[g])
        tokens = pl.ds(rows - LANES, LANES)
        keep(g, own_base + rows - LANES, product(OWN, tokens, 2 * channel[g], 2 * widths[g]))

        @pl.when(me == 1)
        def _():
            conv_in[of, pl.ds(0, LANES)] = jnp.zeros((widths[g], LANES), f32)
            edge = jnp.transpose(conv_in[of, pl.ds(2 * rows, LANES)])
            edge_out[g, :, pl.ds(0, widths[g])] = edge[LANES - PAD :]
            edge_copy(g).start()

    def mate_tiles(g):
        of = pl.ds(channel[g], widths[g])
        for i in range(tiles):
            at = mate_base + i * tile
            value = product(MATE, tile_at(i), 2 * channel[g], 2 * widths[g])
            conv_out[of, tile_at(i)] = convolve(g, at, keep(g, at, value)).astype(bf16)
            out_copy(g, i).start()

    def own_tiles(*which):
        @pl.when(me == 2)
        def _():
            for g in which:
                of = pl.ds(channel[g], widths[g])
                edge_copy(g).wait_recv()
                edge = edge_in[g, :, pl.ds(0, widths[g])]
                edge = jnp.concatenate([jnp.zeros((LANES - PAD, widths[g]), f32), edge], axis=0)
                conv_in[of, pl.ds(0, LANES)] = jnp.transpose(edge)

        start = 2 * channel[which[0]]
        length = sum(2 * widths[g] for g in which)
        for i in range(tiles):
            at = own_base + i * tile
            value = product(OWN, tile_at(i), start, length)
            for g in which:
                row = 2 * channel[g] - start
                gate = keep(g, at, value[row : row + 2 * widths[g]])
                convolved[pl.ds(channel[g], widths[g]), tile_at(i)] = convolve(g, at, gate)

    def mix(half, i, source):
        cols = pl.ds(half * LANES, LANES)
        for j in range(tile // LANES):
            at = pl.ds(i * tile + j * LANES, LANES)
            extra = jnp.transpose(source[cols, at].astype(f32))
            mixed_ref[at, cols] = (attended[at, cols] + extra).astype(bf16)

    @pl.when(middle)
    def _():
        relay(DIAGONAL + 2)
        for u in units[A:]:
            arrived(u, peer)
        partial(OWN, A, E, center, True)
        forward(False, mate, A)
        relay(DIAGONAL + 3)
        for part in (fs * 2 + twin, across * 2 + twin, along * 2 + twin, diagonal * 2 + twin):
            for h in range(pieces):
                piece_arrived(part, h)
        partial(MATE, A, E, center, True)
        forward(False, mate, B)
        for which in (OWN, MATE):
            partial(which, A, B, shard_at(mate), False)
        forward(True, far, Q)

    @pl.when(end)
    def _():
        arrived(Q, far)

    @pl.loop(0, rows // tile)
    def _(i):
        at = pl.ds(pl.multiple_of(i * tile, tile), tile)
        query[at, :] = (
            q_part[at, :] + jnp.dot(normed[at, late], q_all[late, :], preferred_element_type=f32)
        ).astype(bf16)

    heads = query.shape[1] // HEAD_DIM
    query_idx = lax.broadcasted_iota(jnp.int32, (WINDOW, 2 * WINDOW), 0)
    key_idx = lax.broadcasted_iota(jnp.int32, (WINDOW, 2 * WINDOW), 1)
    gap = query_idx + WINDOW - key_idx
    band = (gap >= 0) & (gap < WINDOW)
    low_lanes = lax.broadcasted_iota(jnp.int32, (2 * WINDOW, LANES), 1) < HEAD_DIM
    lane = lax.broadcasted_iota(jnp.int32, (WINDOW, LANES), 1)
    low_half = lane < HEAD_DIM

    def attend(b, kept):
        base = pl.multiple_of(b * WINDOW, WINDOW)
        both = kv[pl.ds(base, 2 * WINDOW), :].astype(f32)
        turned = pltpu.roll(both, HEAD_DIM, 1)
        zero, one = jnp.zeros_like(both), jnp.ones_like(both)

        def lower(x):
            return jnp.where(low_lanes, x, zero)

        def upper(x):
            return jnp.where(low_lanes, zero, x)

        keys = jnp.concatenate([lower(both), upper(turned)], axis=0).astype(bf16)
        vals = jnp.concatenate([lower(turned), upper(both)], axis=0)
        ones = jnp.concatenate([lower(one), upper(one)], axis=0)
        vals = jnp.concatenate([vals, ones], axis=1).astype(bf16)
        stats = []
        for pair in range(heads // 2):
            cols = pl.ds(pair * LANES, LANES)
            scores = lax.dot_general(
                query[pl.ds(base, WINDOW), cols], keys, (((1,), (1,)), ((), ())), preferred_element_type=f32
            )
            sinks = [sink_ref[2 * pair + side] * LOG2_E for side in range(2)]
            tops, raised = [], []
            for side in range(2):
                part = scores[:, side * 2 * WINDOW : (side + 1) * 2 * WINDOW] * (HEAD_DIM ** (-0.5) * LOG2_E)
                part = jnp.where(kept, part, -jnp.inf)
                tops.append(jnp.maximum(jnp.max(part, axis=-1, keepdims=True), sinks[side]))
                raised.append(jnp.exp2(part - tops[side]).astype(bf16))
            out = jnp.dot(jnp.concatenate(raised, axis=1), vals, preferred_element_type=f32)
            top = jnp.where(low_half, tops[0], tops[1])
            total = out[:, LANES:] + jnp.exp2(jnp.where(low_half, sinks[0], sinks[1]) - top)
            attended[pl.ds(base, WINDOW), cols] = out[:, :LANES] / total
            stats.append(top * LN_2 + jnp.log(total))
        turned_stats = jnp.transpose(jnp.where(lax.rem(lane, 2) == 0, stats[0], stats[1]))
        for pair in range(2):
            for side in range(2):
                row = pair + side * HEAD_DIM
                head = 2 * pair + side
                log_ref[head : head + 1, pl.ds(base, WINDOW)] = turned_stats[row : row + 1]

    services = (
        lambda: forward(False, mate, C),
        lambda: None,
        lambda: forward(False, mate, D, E),
    )
    for i, job in enumerate(services):

        @pl.loop(i * (blocks // 2 - 1) // 3, (i + 1) * (blocks // 2 - 1) // 3)
        def _(j):
            attend(2 * j + 1, band)
            attend(2 * j + 2, band)

        @pl.when(middle)
        def _():
            job()

    @pl.when(has_left)
    def _():
        kv_halo.wait_recv()

    attend(blocks - 1, band)
    attend(0, band & ((key_idx >= WINDOW) | has_left))

    @pl.when(middle)
    def _():
        def finish(g):
            arrived(A + g, far)
            own_edge(g)
            mate_tiles(g)

        finish(0)
        for which in (MATE, OWN):
            partial(which, C, E, shard_at(mate), False)
        finish(1)
        own_tiles(0, 1)
        for i in range(tiles):
            mix(0, i, convolved)
        finish(2)
        finish(3)
        finish(4)
        own_tiles(2, 3, 4)
        for i in range(tiles):
            mix(1, i, convolved)

    @pl.when(end)
    def _():
        for half in range(2):
            for i in range(tiles):
                for g in (groups[:2], groups[2:])[half]:
                    out_copy(g, i).wait_recv()
                mix(half, i, conv_back)

    @pl.when(has_right)
    def _():
        kv_halo.wait_send()

    for u in (K, V, Q):
        hop(u, me, True).wait_send()

    @pl.when(end)
    def _():
        for h in range(pieces):
            piece_copy(normed, own_part, h, h, sp=mate).wait_send()
        for u in units[A:]:
            hop(u, me, True).wait_send()

    @pl.when(middle)
    def _():
        for u in (K, V, Q):
            hop(u, peer, True).wait_send()
            hop(u, far, True).wait_send()
        for u in units:
            hop(u, me, False).wait_send()
            hop(u, mate, False).wait_send()
        for j in range(len(relays)):
            for copy in relay_copies(j):
                copy.wait_send()
        for g in groups:
            for i in range(tiles):
                out_copy(g, i).wait_send()

        @pl.when(me == 1)
        def _():
            for g in groups:
                edge_copy(g).wait_send()


def paired_body(tokens, norm_gain, w_query, w_key, w_value, w_conv_in, w_conv_gate, conv_taps, sink_logits):
    rows, features = tokens.shape
    width = w_query.shape[1]
    f32, bf16 = jnp.float32, jnp.bfloat16
    hbm = pl.BlockSpec(memory_space=pltpu.HBM)
    vmem = pl.BlockSpec(memory_space=pltpu.VMEM)
    smem = pl.BlockSpec(memory_space=pltpu.SMEM)
    dma = pltpu.SemaphoreType.DMA
    tiles = rows // 512
    return pl.pallas_call(
        paired_kernel,
        out_shape=(
            pltpu.VMEM((rows, width), bf16),
            pltpu.VMEM((width // HEAD_DIM, rows), f32),
        ),
        in_specs=[hbm, vmem] + [hbm] * 5 + [vmem, smem],
        out_specs=(vmem, vmem),
        scratch_shapes=[
            pltpu.VMEM((rows, features), bf16),
            pltpu.VMEM((rows, features), bf16),
            pltpu.VMEM((rows, features), bf16),
            pltpu.VMEM((2 * HEAD_DIM, features), bf16),
            pltpu.VMEM((features, width), bf16),
            pltpu.VMEM((2, w_query.shape[0], width), bf16),
            pltpu.VMEM((2 * width, features), bf16),
            pltpu.VMEM((rows + WINDOW, 2 * HEAD_DIM), bf16),
            pltpu.VMEM((rows, width), bf16),
            pltpu.VMEM((rows, width), f32),
            pltpu.VMEM((rows, width), f32),
            pltpu.VMEM((width, LANES + 2 * rows), f32),
            pltpu.VMEM((width, rows), f32),
            pltpu.VMEM((2, 2 * width, rows), f32),
            pltpu.VMEM((width, rows), bf16),
            pltpu.VMEM((width, rows), bf16),
            pltpu.VMEM((width, 8), f32),
            pltpu.VMEM((5, PAD, LANES), f32),
            pltpu.VMEM((5, PAD, LANES), f32),
            dma((8,)),
            dma((5,)),
            dma((8, 4)),
            dma((8, 4)),
            dma((8, 4)),
            dma((6,)),
            dma((6,)),
            dma((28,)),
            dma((32,)),
            dma((5 * tiles,)),
            dma((5 * tiles,)),
        ],
        compiler_params=pltpu.CompilerParams(
            collective_id=0, has_side_effects=True, vmem_limit_bytes=59 << 20
        ),
        name="paired_attend_convolve",
    )(tokens, norm_gain.reshape(1, -1), w_key.T, w_value.T, w_query, w_conv_in, w_conv_gate, conv_taps, sink_logits)


def line_body(n, tokens, norm_gain, w_query, w_key, w_value, w_conv_in, w_conv_gate, conv_taps, sink_logits):
    rows, features = tokens.shape
    width, kv_width = w_query.shape[1], w_key.shape[1] + w_value.shape[1]
    assert w_key.shape[1] == HEAD_DIM and width % LANES == 0
    depth = w_query.shape[0]
    flip = depth % LANES == 0 and 2 < n <= 16
    if flip:
        w_kv, kv_shape = (w_key.T, w_value.T), (kv_width, features)
    else:
        w_kv, kv_shape = (jnp.concatenate([w_key, w_value], axis=1),), (features, kv_width)
    arrays = 3 + len(w_kv)
    f32, bf16 = jnp.float32, jnp.bfloat16
    hbm = pl.BlockSpec(memory_space=pltpu.HBM)
    vmem = pl.BlockSpec(memory_space=pltpu.VMEM)
    smem = pl.BlockSpec(memory_space=pltpu.SMEM)
    dma = pltpu.SemaphoreType.DMA
    return pl.pallas_call(
        functools.partial(line_kernel, n, flip),
        out_shape=(
            pltpu.VMEM((rows, width), bf16),
            pltpu.VMEM((width // HEAD_DIM, rows), f32),
        ),
        in_specs=[hbm, vmem] + [hbm] * arrays + [vmem, smem],
        out_specs=(vmem, vmem),
        scratch_shapes=[
            pltpu.VMEM((rows, features), bf16),
            pltpu.VMEM((rows, features), bf16),
            pltpu.VMEM(kv_shape, bf16),
            pltpu.VMEM((features, width), bf16),
            pltpu.VMEM((features, width), bf16),
            pltpu.VMEM((features, width), bf16),
            pltpu.VMEM((rows + WINDOW, kv_width), bf16),
            pltpu.VMEM((rows, width), bf16),
            pltpu.VMEM((rows, width), f32),
            pltpu.VMEM((rows + PAD, width), f32),
            pltpu.VMEM((rows, width), f32),
            dma((4,)),
            dma((arrays,)),
            dma((arrays, n)),
            dma((arrays, n)),
            dma((arrays, n)),
            dma((2,)),
            dma((2,)),
        ],
        compiler_params=pltpu.CompilerParams(
            collective_id=0, has_side_effects=True, vmem_limit_bytes=59 << 20
        ),
        name="gather_attend_convolve",
    )(tokens, norm_gain.reshape(1, -1), *w_kv, w_query, w_conv_in, w_conv_gate, conv_taps, sink_logits)


def body(n, fs, tp, *arrays):
    rows, width, depth = arrays[0].shape[0], arrays[2].shape[1], arrays[2].shape[0]
    square = n == 4 and fs == 4 and tp == 2
    if square and width == 2 * LANES and depth % LANES == 0 and rows % (8 * LANES) == 0:
        return paired_body(*arrays)
    return line_body(n, *arrays)


def solution(mesh):
    return jax.shard_map(
        functools.partial(body, mesh.shape["sp"], mesh.shape["fs"], mesh.shape["tp"]),
        mesh=mesh,
        in_specs=(
            P("sp", None),
            P(),
            P("sp", ("fs", "tp")),
            P("sp", ("fs", "tp")),
            P("sp", ("fs", "tp")),
            P("sp", ("fs", "tp")),
            P("sp", ("fs", "tp")),
            P(None, ("fs", "tp")),
            P(("fs", "tp")),
        ),
        out_specs=(P("sp", ("fs", "tp")), P(("fs", "tp"), "sp")),
        check_vma=False,
    )
```

```python
import functools
import math

import jax
import jax.numpy as jnp
from jax import lax
from jax.experimental import pallas as pl
from jax.experimental.pallas import tpu as pltpu
from jax.sharding import PartitionSpec as P

HEAD_DIM = 64
WINDOW = 128
TAPS = 3
EPS = 1e-06
LANES = 128
PAD = 8
LOG2_E = math.log2(math.e)
LN_2 = math.log(2)
MESH = pl.DeviceIdType.MESH


def line_kernel(
    n, flip, tok_ref, gain_ref, *refs
):
    arrays = 5 if flip else 4
    shards = refs[:arrays]
    (
        taps_ref, sink_ref, mixed_ref, log_ref,
        tok, normed, kv_all, q_all, ci_all, cg_all, kv, query, attended, conv_in, gate_sum,
        tok_sem, own_sem, recv_sem, right_sem, left_sem, halo_send, halo_recv,
    ) = refs[arrays:]
    QUERY, CONV, GATE = arrays - 3, arrays - 2, arrays - 1
    me = lax.axis_index("sp")
    rows = tok.shape[0]
    depth = shards[QUERY].shape[0]
    wholes = (kv_all, kv_all, q_all, ci_all, cg_all)[5 - arrays :]
    has_left, has_right = me > 0, me < n - 1
    left, right = jnp.maximum(me - 1, 0), jnp.minimum(me + 1, n - 1)
    blocks = rows // WINDOW
    f32, bf16 = jnp.float32, jnp.bfloat16

    step_rows = rows // 4
    tok_copies = [
        pltpu.make_async_copy(
            tok_ref.at[pl.ds(i * step_rows, step_rows)], tok.at[pl.ds(i * step_rows, step_rows)], tok_sem.at[i]
        )
        for i in range(4)
    ]
    for copy in tok_copies:
        copy.start()

    def place(a, shard):
        at = pl.ds(pl.multiple_of(shard * depth, depth), depth)
        if flip and a < QUERY:
            return kv_all.at[pl.ds(a * HEAD_DIM, HEAD_DIM), at]
        return wholes[a].at[at]

    own_copies = [pltpu.make_async_copy(shards[a], place(a, me), own_sem.at[a]) for a in range(arrays)]
    for copy in own_copies:
        copy.start()

    barrier = pltpu.get_barrier_semaphore()

    @pl.when(has_left)
    def _():
        pl.semaphore_signal(barrier, inc=1, device_id={"sp": left}, device_id_type=MESH)

    @pl.when(has_right)
    def _():
        pl.semaphore_signal(barrier, inc=1, device_id={"sp": right}, device_id_type=MESH)

    pl.semaphore_wait(barrier, has_left.astype(jnp.int32) + has_right.astype(jnp.int32))

    def hop(a, shard, to_right, own=False):
        return pltpu.make_async_remote_copy(
            src_ref=shards[a] if own else place(a, shard),
            dst_ref=place(a, shard),
            send_sem=(right_sem if to_right else left_sem).at[a, shard],
            recv_sem=recv_sem.at[a, shard],
            device_id={"sp": right if to_right else left},
            device_id_type=MESH,
        )

    def send_own(a):
        @pl.when(has_right)
        def _():
            hop(a, me, True, True).start()

        @pl.when(has_left)
        def _():
            hop(a, me, False, True).start()

    def pass_on(a, first, last):
        def step(k, carry):
            @pl.when(me - k >= 0)
            def _():
                shard = me - k
                hop(a, shard, False).wait_recv()

                @pl.when(has_right)
                def _():
                    hop(a, shard, True).start()

            @pl.when(me + k < n)
            def _():
                shard = me + k
                hop(a, shard, True).wait_recv()

                @pl.when(has_left)
                def _():
                    hop(a, shard, False).start()

            return carry

        lax.fori_loop(first, last, step, 0)

    for a in range(GATE):
        send_own(a)

    norm_rows = 64
    for i in range(4):
        tok_copies[i].wait()

        @pl.loop(0, step_rows // norm_rows)
        def _(j):
            at = pl.ds(pl.multiple_of(i * step_rows + j * norm_rows, norm_rows), norm_rows)
            wide = tok[at, :].astype(f32)
            scale = lax.rsqrt(jnp.mean(wide * wide, axis=-1, keepdims=True) + EPS)
            normed[at, :] = (wide * scale * gain_ref[...]).astype(bf16)

    for copy in own_copies:
        copy.wait()

    tile = 256

    def project(a, store):
        @pl.loop(0, rows // tile)
        def _(i):
            base = pl.multiple_of(i * tile, tile)
            side = 1 if flip and a < QUERY else 0
            store(
                base,
                lax.dot_general(
                    normed[pl.ds(base, tile), :],
                    wholes[a][...],
                    (((1,), (side,)), ((), ())),
                    preferred_element_type=f32,
                ),
            )

    def halo(buffer, length, i):
        return pltpu.make_async_remote_copy(
            src_ref=buffer.at[pl.ds(rows, length)],
            dst_ref=buffer.at[pl.ds(0, length)],
            send_sem=halo_send.at[i],
            recv_sem=halo_recv.at[i],
            device_id={"sp": right},
            device_id_type=MESH,
        )

    for a in range(QUERY):
        pass_on(a, 1, n)
    send_own(GATE)

    def store_kv(base, value):
        kv[pl.ds(base + WINDOW, tile), :] = value.astype(bf16)

    project(0, store_kv)

    @pl.when(jnp.logical_not(has_left))
    def _():
        kv[pl.ds(0, WINDOW), :] = jnp.zeros((WINDOW, kv.shape[1]), bf16)
        conv_in[pl.ds(0, PAD), :] = jnp.zeros((PAD, conv_in.shape[1]), f32)

    pass_on(QUERY, 1, n)

    @pl.when(has_right)
    def _():
        halo(kv, WINDOW, 0).start()

    def store_query(base, value):
        query[pl.ds(base, tile), :] = value.astype(bf16)

    project(QUERY, store_query)

    heads = query.shape[1] // HEAD_DIM
    query_idx = lax.broadcasted_iota(jnp.int32, (WINDOW, 2 * WINDOW), 0)
    key_idx = lax.broadcasted_iota(jnp.int32, (WINDOW, 2 * WINDOW), 1)
    gap = query_idx + WINDOW - key_idx
    band = (gap >= 0) & (gap < WINDOW)
    lane = lax.broadcasted_iota(jnp.int32, (2 * WINDOW, LANES), 1)
    low = lane < HEAD_DIM
    stat_lane = lax.broadcasted_iota(jnp.int32, (WINDOW, LANES), 1)

    def attend(b, kept):
        base = pl.multiple_of(b * WINDOW, WINDOW)
        both = kv[pl.ds(base, 2 * WINDOW), :].astype(f32)
        turned = pltpu.roll(both, HEAD_DIM, 1)
        zero = jnp.zeros_like(both)
        keys = (jnp.where(low, both, zero).astype(bf16), jnp.where(low, zero, turned).astype(bf16))
        vals = (jnp.where(low, turned, zero).astype(bf16), jnp.where(low, zero, both).astype(bf16))
        stats = jnp.zeros((WINDOW, LANES), f32)
        for pair in range(heads // 2):
            cols = pl.ds(pair * LANES, LANES)
            q = query[pl.ds(base, WINDOW), cols]
            out = None
            for side in range(2):
                head = 2 * pair + side
                scores = lax.dot_general(
                    q, keys[side], (((1,), (1,)), ((), ())), preferred_element_type=f32
                ) * HEAD_DIM ** (-0.5)
                scores = jnp.where(kept, scores, -jnp.inf)
                sink = jnp.full((WINDOW, 1), sink_ref[head], f32)
                top = jnp.maximum(jnp.max(scores, axis=-1, keepdims=True), sink)
                raised = jnp.exp(scores - top)
                total = jnp.sum(raised, axis=-1, keepdims=True) + jnp.exp(sink - top)
                weights = (raised * (1.0 / total)).astype(bf16)
                part = jnp.dot(weights, vals[side], preferred_element_type=f32)
                out = part if out is None else out + part
                stats = jnp.where(stat_lane == head, top + jnp.log(total), stats)
            attended[pl.ds(base, WINDOW), cols] = out
        log_ref[:, pl.ds(base, WINDOW)] = jnp.transpose(stats)[:heads]

    def attend_range(first, last):
        @pl.loop(first, last)
        def _(b):
            attend(b, band)

    cut = [1 + (n - 1) * i // 3 for i in range(4)]
    mid = 1 + (blocks - 1) // 2
    attend_range(1, mid)
    pass_on(CONV, cut[0], cut[1])
    attend_range(mid, blocks)
    pass_on(CONV, cut[1], cut[2])

    @pl.when(has_left)
    def _():
        halo(kv, WINDOW, 0).wait_recv()

    attend(0, band & ((key_idx >= WINDOW) | has_left))
    pass_on(CONV, cut[2], cut[3])

    def store_conv(base, value):
        conv_in[pl.ds(base + PAD, tile), :] = value.astype(bf16).astype(f32)

    project(CONV, store_conv)
    early = min(2, n - 1)
    pass_on(GATE, 1, early)

    @pl.when(has_right)
    def _():
        halo(conv_in, PAD, 1).start()

    pass_on(GATE, early, n - 1)

    far = jnp.where(2 * me >= n, 0, n - 1)

    def gate_part(base, shard):
        at = pl.ds(pl.multiple_of(shard * depth, depth), depth)
        return jnp.dot(
            normed[pl.ds(base, tile), at], cg_all[at, :], preferred_element_type=f32
        )

    if flip:

        @pl.loop(0, rows // tile)
        def _(i):
            base = pl.multiple_of(i * tile, tile)
            part = gate_part(base, lax.rem(far + 1, n))
            for j in range(2, n):
                part = part + gate_part(base, lax.rem(far + j, n))
            gate_sum[pl.ds(base, tile), :] = part

    pass_on(GATE, n - 1, n)

    @pl.when(has_left)
    def _():
        halo(conv_in, PAD, 1).wait_recv()

    def store_mixed(base, value):
        gate = value.astype(bf16).astype(f32)
        taps = taps_ref[...].astype(f32)
        near = conv_in[pl.ds(base, tile + PAD), :]
        total = jnp.zeros_like(gate)
        for k in range(TAPS):
            start = PAD - TAPS + 1 + k
            total = total + taps[k : k + 1] * near[start : start + tile]
        mixed_ref[pl.ds(base, tile), :] = (attended[pl.ds(base, tile), :] + gate * total).astype(bf16)

    if flip:

        @pl.loop(0, rows // tile)
        def _(i):
            base = pl.multiple_of(i * tile, tile)
            store_mixed(base, gate_sum[pl.ds(base, tile), :] + gate_part(base, far))

    else:
        project(GATE, store_mixed)

    @pl.when(has_right)
    def _():
        halo(kv, WINDOW, 0).wait_send()
        halo(conv_in, PAD, 1).wait_send()

    for a in range(arrays):

        @pl.when(has_right)
        def _():
            @pl.loop(0, me + 1)
            def _(s):
                hop(a, s, True).wait_send()

        @pl.when(has_left)
        def _():
            @pl.loop(me, n)
            def _(s):
                hop(a, s, False).wait_send()


def paired_kernel(tok_ref, gain_ref, *refs):
    shards = refs[:5]
    (
        taps_ref, sink_ref, mixed_ref, log_ref,
        tok, normed, other, kv_all, q_all, stage, conv_w, kv, query, q_part, attended,
        conv_in, convolved, sums, conv_out, conv_back, turned_taps, edge_out, edge_in,
        tok_sem, own_sem, recv_sem, sent_sem, halo_recv, x_recv, twin_recv, out_recv,
    ) = refs[5:]
    f32, bf16 = jnp.float32, jnp.bfloat16
    me, fs, tp = lax.axis_index("sp"), lax.axis_index("fs"), lax.axis_index("tp")
    low = me < 2
    end = (me == 0) | (me == 3)
    middle = jnp.logical_not(end)
    mate = me + 1 - 2 * lax.rem(me, 2)
    peer = jnp.where(end, 3 - mate, 3 - me)
    far = jnp.where(low, 3, 0)
    first = jnp.where(low, 0, 1)
    has_left, has_right = me > 0, me < 3
    right = jnp.minimum(me + 1, 3)
    across, along = fs + 1 - 2 * lax.rem(fs, 2), lax.rem(fs + 2, 4)
    diagonal = 3 - fs
    twin = 1 - tp
    rows = tok.shape[0]
    depth = shards[2].shape[0]
    blocks = rows // WINDOW
    width = q_all.shape[1]
    widths = (width // 4, width // 4, width // 4, width // 8, width // 8)
    groups = range(len(widths))
    channel = [sum(widths[:g]) for g in groups]
    K, V, Q, R, A, B, C, D, E = units = range(9)

    parts = 8
    part_rows = rows // parts
    pieces = 4
    piece = part_rows // pieces
    own_part = fs * 2 + tp

    def part_at(i):
        return lax.rem(own_part + i, parts)

    def rows_of(start, length):
        return pl.ds(pl.multiple_of(start, 16), length)

    tok_copies = []
    for i in range(parts):
        at = rows_of(part_at(i) * part_rows, part_rows)
        tok_copies.append(pltpu.make_async_copy(tok_ref.at[at], tok.at[at], tok_sem.at[min(i, 1)]))
    for copy in tok_copies:
        copy.start()

    def shard_at(shard):
        return pl.ds(pl.multiple_of(shard * depth, depth), depth)

    def place(u, shard):
        at = shard_at(shard)
        if u < Q:
            return kv_all.at[pl.ds(u * HEAD_DIM, HEAD_DIM), at]
        if u < A:
            return q_all.at[at, pl.ds((u - Q) * LANES, LANES)]
        return conv_w.at[pl.ds(2 * channel[u - A], 2 * widths[u - A]), at]

    own_copies = [pltpu.make_async_copy(shards[u], place(u, me), own_sem.at[0]) for u in (K, V)]
    own_copies.append(pltpu.make_async_copy(shards[2], q_all.at[shard_at(me)], own_sem.at[1]))
    own_copies += [pltpu.make_async_copy(shards[3 + j], stage.at[j], own_sem.at[2]) for j in range(2)]
    for copy in own_copies:
        copy.start()

    def norm_part(i):
        norm_rows = 64

        @pl.loop(0, part_rows // norm_rows)
        def _(j):
            at = rows_of(part_at(i) * part_rows + j * norm_rows, norm_rows)
            wide = tok[at, :].astype(f32)
            scale = lax.rsqrt(jnp.mean(wide * wide, axis=-1, keepdims=True) + EPS)
            normed[at, :] = (wide * scale * gain_ref[...]).astype(bf16)

    barrier = pltpu.get_barrier_semaphore()

    def greet(**device):
        pl.semaphore_signal(barrier, inc=1, device_id=device, device_id_type=MESH)

    greet(sp=mate)

    @pl.when(middle)
    def _():
        greet(sp=peer)
        greet(fs=across)
        greet(fs=along)
        greet(tp=twin)

    tok_copies[0].wait()
    norm_part(0)
    pltpu.make_async_copy(stage, stage, own_sem.at[2]).wait()
    for j in range(2):
        for block in range(depth // LANES):
            turned = jnp.transpose(stage[j, pl.ds(block * LANES, LANES), :].astype(f32)).astype(bf16)
            at = pl.ds(pl.multiple_of(me * depth + block * LANES, LANES), LANES)
            for g in groups:
                to = pl.ds(2 * channel[g] + j * widths[g], widths[g])
                conv_w[to, at] = turned[channel[g] : channel[g] + widths[g]]
    taps = taps_ref[...].astype(f32)
    turned_taps[...] = jnp.transpose(jnp.concatenate([taps, jnp.zeros((8 - TAPS, width), f32)], axis=0))
    own_kv = kv_all.at[:, shard_at(me)]
    pltpu.make_async_copy(own_kv, own_kv, own_sem.at[0]).wait()
    own_copies[2].wait()
    conv_in[:, pl.ds(0, LANES)] = jnp.zeros((width, LANES), f32)

    pl.semaphore_wait(barrier, jnp.where(middle, 5, 1))

    TO_MATE, TO_PEER, RELAYED, RETURNED, EDGES, HALO = range(6)

    def slot(shard, device):
        return shard - jnp.where(shard > device, 1, 0)

    def hop(u, shard, to_mate):
        target = mate if to_mate else peer
        return pltpu.make_async_remote_copy(
            src_ref=place(u, shard),
            dst_ref=place(u, shard),
            send_sem=sent_sem.at[TO_MATE if to_mate else TO_PEER],
            recv_sem=recv_sem.at[u, slot(shard, target)],
            device_id={"sp": target},
            device_id_type=MESH,
        )

    def arrived(u, shard):
        ref = place(u, shard)
        pltpu.make_async_copy(ref, ref, recv_sem.at[u, slot(shard, me)]).wait()

    def drain(kind, elements):
        ref = other.at[pl.ds(0, elements // other.shape[1])]
        pltpu.make_async_copy(ref, ref, sent_sem.at[kind]).wait()

    def piece_at(part, h):
        return rows_of(part * part_rows + h * piece, piece)

    def piece_copy(buffer, part, h, kind, arrival, **device):
        at = piece_at(part, h)
        return pltpu.make_async_remote_copy(
            src_ref=buffer.at[at],
            dst_ref=other.at[at],
            send_sem=sent_sem.at[kind],
            recv_sem=arrival,
            device_id=device,
            device_id_type=MESH,
        )

    def line_sem(part, h):
        return x_recv.at[part // 2, h]

    def piece_arrived(part, h):
        ref = other.at[piece_at(part, h)]
        pltpu.make_async_copy(ref, ref, line_sem(part, h)).wait()

    across_part, along_part, diagonal_part = across * 2 + tp, along * 2 + tp, diagonal * 2 + tp
    relays = [(own_part, h, ("tp", "fs_across", "fs_along")) for h in range(pieces)]
    relays += [(across_part, h, ("tp", "fs_along")[: 2 - h % 2]) for h in range(pieces)]
    relays += [(along_part, h, ("tp", "fs_across")[: 1 + h % 2]) for h in range(pieces)]
    relays += [(diagonal_part, h, ("tp",)) for h in range(pieces)]
    OWN_X, ACROSS, ALONG, DIAGONAL = (pieces * j for j in range(4))
    devices = {"tp": {"tp": twin}, "fs_across": {"fs": across}, "fs_along": {"fs": along}}

    def relay_copies(j):
        part, h, to = relays[j]
        return [
            piece_copy(other, part, h, RELAYED, twin_recv.at[0] if d == "tp" else line_sem(part, h), **devices[d])
            for d in to
        ]

    def relay(*which):
        for j in which:
            piece_arrived(relays[j][0], relays[j][1])
            for copy in relay_copies(j):
                copy.start()

    def send(to_mate, shard, *which):
        for u in which:
            hop(u, shard, to_mate).start()

    def forward(to_mate, shard, *which):
        for u in which:
            arrived(u, shard)
            hop(u, shard, to_mate).start()

    def pieces_out(*which):
        for h in which:
            piece_copy(normed, own_part, h, RELAYED, line_sem(own_part, h), sp=mate).start()

    @pl.when(end)
    def _():
        pieces_out(*range(pieces))
        send(True, me, K, V, Q, R, A, B, C)

    @pl.when(middle)
    def _():
        send(False, me, K, V, Q, R, A, B, C, D)
        send(True, me, K, V, Q, R)

    others = tok.at[pl.ds(0, rows - part_rows)]
    pltpu.make_async_copy(others, others, tok_sem.at[1]).wait()
    for i in range(1, parts):
        norm_part(i)

    tile = 512

    early = pl.ds(pl.multiple_of(first * depth, depth), 3 * depth)
    late = pl.ds(pl.multiple_of(far * depth, depth), depth)

    kv_halo = pltpu.make_async_remote_copy(
        src_ref=kv.at[pl.ds(rows, WINDOW)],
        dst_ref=kv.at[pl.ds(0, WINDOW)],
        send_sem=sent_sem.at[HALO],
        recv_sem=halo_recv.at[0],
        device_id={"sp": right},
        device_id_type=MESH,
    )

    own_base, mate_base = jnp.where(me == 1, rows, 0), jnp.where(me == 1, 0, rows)
    bases = (own_base, mate_base)
    sources = (normed, other)
    tiles = rows // tile
    OWN, MATE = 0, 1

    def tile_at(i):
        return pl.ds(i * tile if isinstance(i, int) else pl.multiple_of(i * tile, tile), tile)

    def out_copy(g, i):
        at = (pl.ds(channel[g], widths[g]), tile_at(i))
        return pltpu.make_async_remote_copy(
            src_ref=conv_out.at[at],
            dst_ref=conv_back.at[at],
            send_sem=sent_sem.at[RETURNED],
            recv_sem=out_recv.at[g * tiles + i],
            device_id={"sp": mate},
            device_id_type=MESH,
        )

    def edge_copy(g):
        return pltpu.make_async_remote_copy(
            src_ref=edge_out.at[g],
            dst_ref=edge_in.at[g],
            send_sem=sent_sem.at[EDGES],
            recv_sem=halo_recv.at[1 + g],
            device_id={"sp": right},
            device_id_type=MESH,
        )

    center = pl.ds(depth, 2 * depth)
    everything = pl.ds(0, conv_w.shape[1])

    def dot(which, tokens, start, length, at):
        return lax.dot_general(
            conv_w[pl.ds(start, length), at],
            sources[which][tokens, at],
            (((1,), (1,)), ((), ())),
            preferred_element_type=f32,
        )

    def partial(which, i, u, v, at, fresh=False):
        start = 2 * channel[u - A]
        span = pl.ds(start, 2 * channel[v - A] + 2 * widths[v - A] - start)
        value = dot(which, tile_at(i), span.start, span.size, at)
        sums[which, span, tile_at(i)] = value if fresh else sums[which, span, tile_at(i)] + value

    def product(which, tokens, start, length):
        if which == OWN and start == 2 * channel[-1]:
            return dot(which, tokens, start, length, everything)
        return sums[which, pl.ds(start, length), tokens] + dot(which, tokens, start, length, late)

    def keep(g, at, value):
        value = value.astype(bf16).astype(f32)
        conv_in[pl.ds(channel[g], widths[g]), pl.ds(pl.multiple_of(at + LANES, LANES), value.shape[1])] = value[: widths[g]]
        return value[widths[g] :]

    def convolve(g, at, gate):
        of = pl.ds(channel[g], widths[g])
        near = conv_in[of, pl.ds(pl.multiple_of(at, LANES), tile + LANES)]
        total = jnp.zeros((widths[g], tile), f32)
        for k in range(TAPS):
            moved = near if k == TAPS - 1 else pltpu.roll(near, TAPS - 1 - k, 1)
            total = total + turned_taps[of, k : k + 1] * moved[:, LANES:]
        return gate * total

    def mate_tiles(g):
        of = pl.ds(channel[g], widths[g])
        tokens = pl.ds(rows - LANES, LANES)
        keep(g, own_base + rows - LANES, product(OWN, tokens, 2 * channel[g], 2 * widths[g]))
        for i in range(tiles):
            at = mate_base + i * tile
            value = product(MATE, tile_at(i), 2 * channel[g], 2 * widths[g])
            conv_out[of, tile_at(i)] = convolve(g, at, keep(g, at, value)).astype(bf16)
            out_copy(g, i).start()

        @pl.when(me == 1)
        def _():
            edge = jnp.transpose(conv_in[of, pl.ds(2 * rows, LANES)])
            edge_out[g, :, pl.ds(0, widths[g])] = edge[LANES - PAD :]
            edge_copy(g).start()

    def own_tiles(*which):
        @pl.when(me == 2)
        def _():
            for g in which:
                of = pl.ds(channel[g], widths[g])
                edge_copy(g).wait_recv()
                edge = edge_in[g, :, pl.ds(0, widths[g])]
                edge = jnp.concatenate([jnp.zeros((LANES - PAD, widths[g]), f32), edge], axis=0)
                conv_in[of, pl.ds(0, LANES)] = jnp.transpose(edge)

        start = 2 * channel[which[0]]
        length = sum(2 * widths[g] for g in which)
        for i in range(tiles):
            at = own_base + i * tile
            value = product(OWN, tile_at(i), start, length)
            for g in which:
                row = 2 * channel[g] - start
                gate = keep(g, at, value[row : row + 2 * widths[g]])
                convolved[pl.ds(channel[g], widths[g]), tile_at(i)] = convolve(g, at, gate)

    def mix(half, i, source):
        cols = pl.ds(half * LANES, LANES)
        for j in range(tile // LANES):
            at = pl.ds(i * tile + j * LANES, LANES)
            extra = jnp.transpose(source[cols, at].astype(f32))
            mixed_ref[at, cols] = (attended[at, cols] + extra).astype(bf16)

    @pl.when(middle)
    def _():
        relay(OWN_X)
        forward(True, peer, K, V)
        relay(OWN_X + 1)
        forward(True, peer, Q)
        relay(ACROSS, ALONG)
        forward(True, peer, R)
        relay(OWN_X + 2, ACROSS + 1, ALONG + 1, OWN_X + 3)
        forward(False, mate, K, V)
        relay(ACROSS + 2, ALONG + 2)
        forward(False, mate, Q)
        relay(DIAGONAL, DIAGONAL + 1)
        forward(False, mate, R)
        for u in (A, B, C, D):
            arrived(u, peer)
        partial(OWN, 0, A, D, center, True)
        relay(ACROSS + 3, ALONG + 3)
        forward(True, far, K, V)
        forward(False, mate, A)

    @pl.when(end)
    def _():
        for shard in (mate, peer, far):
            for u in (K, V):
                arrived(u, shard)

    @pl.loop(0, rows // tile)
    def _(i):
        base = pl.multiple_of(i * tile, tile)
        kv[pl.ds(base + WINDOW, tile), :] = lax.dot_general(
            normed[pl.ds(base, tile), :], kv_all[...], (((1,), (1,)), ((), ())), preferred_element_type=f32
        ).astype(bf16)

    @pl.when(jnp.logical_not(has_left))
    def _():
        kv[pl.ds(0, WINDOW), :] = jnp.zeros((WINDOW, kv.shape[1]), bf16)

    @pl.when(has_right)
    def _():
        kv_halo.start()

    @pl.when(middle)
    def _():
        forward(True, far, Q)
        partial(OWN, 1, A, D, center, True)
        forward(False, mate, B)

    @pl.when(end)
    def _():
        send(True, me, D, E)
        for u in (Q, R):
            arrived(u, mate)
            arrived(u, peer)

    @pl.loop(0, rows // tile)
    def _(i):
        at = pl.ds(pl.multiple_of(i * tile, tile), tile)
        q_part[at, :] = jnp.dot(normed[at, early], q_all[early, :], preferred_element_type=f32)

    @pl.when(middle)
    def _():
        forward(True, far, R)

    @pl.when(end)
    def _():
        arrived(Q, far)
        arrived(R, far)

    @pl.loop(0, rows // tile)
    def _(i):
        at = pl.ds(pl.multiple_of(i * tile, tile), tile)
        query[at, :] = (
            q_part[at, :] + jnp.dot(normed[at, late], q_all[late, :], preferred_element_type=f32)
        ).astype(bf16)

    heads = query.shape[1] // HEAD_DIM
    query_idx = lax.broadcasted_iota(jnp.int32, (WINDOW, 2 * WINDOW), 0)
    key_idx = lax.broadcasted_iota(jnp.int32, (WINDOW, 2 * WINDOW), 1)
    gap = query_idx + WINDOW - key_idx
    band = (gap >= 0) & (gap < WINDOW)
    low_lanes = lax.broadcasted_iota(jnp.int32, (2 * WINDOW, LANES), 1) < HEAD_DIM
    lane = lax.broadcasted_iota(jnp.int32, (WINDOW, LANES), 1)
    low_half = lane < HEAD_DIM

    def attend(b, kept):
        base = pl.multiple_of(b * WINDOW, WINDOW)
        both = kv[pl.ds(base, 2 * WINDOW), :].astype(f32)
        turned = pltpu.roll(both, HEAD_DIM, 1)
        zero, one = jnp.zeros_like(both), jnp.ones_like(both)

        def lower(x):
            return jnp.where(low_lanes, x, zero)

        def upper(x):
            return jnp.where(low_lanes, zero, x)

        keys = jnp.concatenate([lower(both), upper(turned)], axis=0).astype(bf16)
        vals = jnp.concatenate([lower(turned), upper(both)], axis=0)
        ones = jnp.concatenate([lower(one), upper(one)], axis=0)
        vals = jnp.concatenate([vals, ones], axis=1).astype(bf16)
        stats = []
        for pair in range(heads // 2):
            cols = pl.ds(pair * LANES, LANES)
            scores = lax.dot_general(
                query[pl.ds(base, WINDOW), cols], keys, (((1,), (1,)), ((), ())), preferred_element_type=f32
            )
            sinks = [sink_ref[2 * pair + side] * LOG2_E for side in range(2)]
            tops, raised = [], []
            for side in range(2):
                part = scores[:, side * 2 * WINDOW : (side + 1) * 2 * WINDOW] * (HEAD_DIM ** (-0.5) * LOG2_E)
                part = jnp.where(kept, part, -jnp.inf)
                tops.append(jnp.maximum(jnp.max(part, axis=-1, keepdims=True), sinks[side]))
                raised.append(jnp.exp2(part - tops[side]).astype(bf16))
            out = jnp.dot(jnp.concatenate(raised, axis=1), vals, preferred_element_type=f32)
            top = jnp.where(low_half, tops[0], tops[1])
            total = out[:, LANES:] + jnp.exp2(jnp.where(low_half, sinks[0], sinks[1]) - top)
            attended[pl.ds(base, WINDOW), cols] = out[:, :LANES] / total
            stats.append(top * LN_2 + jnp.log(total))
        turned_stats = jnp.transpose(jnp.where(lax.rem(lane, 2) == 0, stats[0], stats[1]))
        for pair in range(2):
            for side in range(2):
                row = pair + side * HEAD_DIM
                head = 2 * pair + side
                log_ref[head : head + 1, pl.ds(base, WINDOW)] = turned_stats[row : row + 1]

    def finish(g):
        arrived(A + g, far)
        mate_tiles(g)

    @pl.when(middle)
    def _():
        relay(DIAGONAL + 2, DIAGONAL + 3)
        half_rows = other.at[pl.ds(0, rows // 2)]
        pltpu.make_async_copy(half_rows, half_rows, twin_recv.at[0]).wait()
        for i in range(tiles):
            partial(MATE, i, A, D, center, True)
        forward(False, mate, C)
        send(False, me, E)
        for which in (MATE, OWN):
            for i in range(tiles):
                partial(which, i, A, B, shard_at(mate))
        finish(0)

    def attend_pairs(start, stop):
        @pl.loop(start, stop)
        def _(j):
            attend(2 * j + 1, band)
            attend(2 * j + 2, band)

    cut = (blocks // 2 - 1) * 2 // 3
    attend_pairs(0, cut)

    @pl.when(middle)
    def _():
        finish(1)

    attend_pairs(cut, blocks // 2 - 1)

    @pl.when(middle)
    def _():
        forward(False, mate, D, E)

    @pl.when(has_left)
    def _():
        kv_halo.wait_recv()

    attend(blocks - 1, band)
    attend(0, band & ((key_idx >= WINDOW) | has_left))

    @pl.when(middle)
    def _():
        for which in (MATE, OWN):
            for i in range(tiles):
                partial(which, i, C, D, shard_at(mate))
        finish(2)
        arrived(E, peer)
        for i in range(tiles):
            partial(MATE, i, E, E, early, True)
        finish(3)
        finish(4)
        own_tiles(0, 1)
        own_tiles(2, 3)
        own_tiles(4)
        for half in range(2):
            for i in range(tiles):
                mix(half, i, convolved)

    @pl.when(end)
    def _():
        for half in range(2):
            for i in range(tiles):
                for g in (groups[:2], groups[2:])[half]:
                    out_copy(g, i).wait_recv()
                mix(half, i, conv_back)

    @pl.when(has_right)
    def _():
        kv_halo.wait_send()

    attention_shard = depth * (2 * HEAD_DIM + width)
    whole_shard = attention_shard + depth * 2 * width

    @pl.when(end)
    def _():
        drain(TO_MATE, whole_shard)
        drain(RELAYED, part_rows * other.shape[1])

    @pl.when(middle)
    def _():
        drain(TO_MATE, 3 * attention_shard)
        drain(TO_PEER, 2 * whole_shard)
        drain(RELAYED, sum(len(to) for _, _, to in relays) * piece * other.shape[1])
        pltpu.make_async_copy(conv_out, conv_out, sent_sem.at[RETURNED]).wait()

        @pl.when(me == 1)
        def _():
            pltpu.make_async_copy(edge_out, edge_out, sent_sem.at[EDGES]).wait()


def paired_body(tokens, norm_gain, w_query, w_key, w_value, w_conv_in, w_conv_gate, conv_taps, sink_logits):
    rows, features = tokens.shape
    width = w_query.shape[1]
    f32, bf16 = jnp.float32, jnp.bfloat16
    hbm = pl.BlockSpec(memory_space=pltpu.HBM)
    vmem = pl.BlockSpec(memory_space=pltpu.VMEM)
    smem = pl.BlockSpec(memory_space=pltpu.SMEM)
    dma = pltpu.SemaphoreType.DMA
    tiles = rows // 512
    return pl.pallas_call(
        paired_kernel,
        out_shape=(
            pltpu.VMEM((rows, width), bf16),
            pltpu.VMEM((width // HEAD_DIM, rows), f32),
        ),
        in_specs=[hbm, vmem] + [hbm] * 5 + [vmem, smem],
        out_specs=(vmem, vmem),
        scratch_shapes=[
            pltpu.VMEM((rows, features), bf16),
            pltpu.VMEM((rows, features), bf16),
            pltpu.VMEM((rows, features), bf16),
            pltpu.VMEM((2 * HEAD_DIM, features), bf16),
            pltpu.VMEM((features, width), bf16),
            pltpu.VMEM((2, w_query.shape[0], width), bf16),
            pltpu.VMEM((2 * width, features), bf16),
            pltpu.VMEM((rows + WINDOW, 2 * HEAD_DIM), bf16),
            pltpu.VMEM((rows, width), bf16),
            pltpu.VMEM((rows, width), f32),
            pltpu.VMEM((rows, width), f32),
            pltpu.VMEM((width, LANES + 2 * rows), f32),
            pltpu.VMEM((width, rows), f32),
            pltpu.VMEM((2, 2 * width, rows), f32),
            pltpu.VMEM((width, rows), bf16),
            pltpu.VMEM((width, rows), bf16),
            pltpu.VMEM((width, 8), f32),
            pltpu.VMEM((5, PAD, LANES), f32),
            pltpu.VMEM((5, PAD, LANES), f32),
            dma((2,)),
            dma((3,)),
            dma((9, 3)),
            dma((6,)),
            dma((6,)),
            dma((4, 4)),
            dma((1,)),
            dma((5 * tiles,)),
        ],
        compiler_params=pltpu.CompilerParams(
            collective_id=0, has_side_effects=True, vmem_limit_bytes=59 << 20
        ),
        name="paired_attend_convolve",
    )(tokens, norm_gain.reshape(1, -1), w_key.T, w_value.T, w_query, w_conv_in, w_conv_gate, conv_taps, sink_logits)


def line_body(n, tokens, norm_gain, w_query, w_key, w_value, w_conv_in, w_conv_gate, conv_taps, sink_logits):
    rows, features = tokens.shape
    width, kv_width = w_query.shape[1], w_key.shape[1] + w_value.shape[1]
    assert w_key.shape[1] == HEAD_DIM and width % LANES == 0
    depth = w_query.shape[0]
    flip = depth % LANES == 0 and 2 < n <= 16
    if flip:
        w_kv, kv_shape = (w_key.T, w_value.T), (kv_width, features)
    else:
        w_kv, kv_shape = (jnp.concatenate([w_key, w_value], axis=1),), (features, kv_width)
    arrays = 3 + len(w_kv)
    f32, bf16 = jnp.float32, jnp.bfloat16
    hbm = pl.BlockSpec(memory_space=pltpu.HBM)
    vmem = pl.BlockSpec(memory_space=pltpu.VMEM)
    smem = pl.BlockSpec(memory_space=pltpu.SMEM)
    dma = pltpu.SemaphoreType.DMA
    return pl.pallas_call(
        functools.partial(line_kernel, n, flip),
        out_shape=(
            pltpu.VMEM((rows, width), bf16),
            pltpu.VMEM((width // HEAD_DIM, rows), f32),
        ),
        in_specs=[hbm, vmem] + [hbm] * arrays + [vmem, smem],
        out_specs=(vmem, vmem),
        scratch_shapes=[
            pltpu.VMEM((rows, features), bf16),
            pltpu.VMEM((rows, features), bf16),
            pltpu.VMEM(kv_shape, bf16),
            pltpu.VMEM((features, width), bf16),
            pltpu.VMEM((features, width), bf16),
            pltpu.VMEM((features, width), bf16),
            pltpu.VMEM((rows + WINDOW, kv_width), bf16),
            pltpu.VMEM((rows, width), bf16),
            pltpu.VMEM((rows, width), f32),
            pltpu.VMEM((rows + PAD, width), f32),
            pltpu.VMEM((rows, width), f32),
            dma((4,)),
            dma((arrays,)),
            dma((arrays, n)),
            dma((arrays, n)),
            dma((arrays, n)),
            dma((2,)),
            dma((2,)),
        ],
        compiler_params=pltpu.CompilerParams(
            collective_id=0, has_side_effects=True, vmem_limit_bytes=59 << 20
        ),
        name="gather_attend_convolve",
    )(tokens, norm_gain.reshape(1, -1), *w_kv, w_query, w_conv_in, w_conv_gate, conv_taps, sink_logits)


def body(n, fs, tp, *arrays):
    rows, width, depth = arrays[0].shape[0], arrays[2].shape[1], arrays[2].shape[0]
    square = n == 4 and fs == 4 and tp == 2
    if square and width == 2 * LANES and depth % LANES == 0 and rows % (8 * LANES) == 0:
        return paired_body(*arrays)
    return line_body(n, *arrays)


def solution(mesh):
    return jax.shard_map(
        functools.partial(body, mesh.shape["sp"], mesh.shape["fs"], mesh.shape["tp"]),
        mesh=mesh,
        in_specs=(
            P("sp", None),
            P(),
            P("sp", ("fs", "tp")),
            P("sp", ("fs", "tp")),
            P("sp", ("fs", "tp")),
            P("sp", ("fs", "tp")),
            P("sp", ("fs", "tp")),
            P(None, ("fs", "tp")),
            P(("fs", "tp")),
        ),
        out_specs=(P("sp", ("fs", "tp")), P(("fs", "tp"), "sp")),
        check_vma=False,
    )
```

```python
import functools
import math

import jax
import jax.numpy as jnp
from jax import lax
from jax.experimental import pallas as pl
from jax.experimental.pallas import tpu as pltpu
from jax.sharding import PartitionSpec as P

HEAD_DIM = 64
WINDOW = 128
TAPS = 3
EPS = 1e-06
LANES = 128
PAD = 8
LOG2_E = math.log2(math.e)
LN_2 = math.log(2)
MESH = pl.DeviceIdType.MESH


def line_kernel(
    n, flip, tok_ref, gain_ref, *refs
):
    arrays = 5 if flip else 4
    shards = refs[:arrays]
    (
        taps_ref, sink_ref, mixed_ref, log_ref,
        tok, normed, kv_all, q_all, ci_all, cg_all, kv, query, attended, conv_in, gate_sum,
        tok_sem, own_sem, recv_sem, right_sem, left_sem, halo_send, halo_recv,
    ) = refs[arrays:]
    QUERY, CONV, GATE = arrays - 3, arrays - 2, arrays - 1
    me = lax.axis_index("sp")
    rows = tok.shape[0]
    depth = shards[QUERY].shape[0]
    wholes = (kv_all, kv_all, q_all, ci_all, cg_all)[5 - arrays :]
    has_left, has_right = me > 0, me < n - 1
    left, right = jnp.maximum(me - 1, 0), jnp.minimum(me + 1, n - 1)
    blocks = rows // WINDOW
    f32, bf16 = jnp.float32, jnp.bfloat16

    step_rows = rows // 4
    tok_copies = [
        pltpu.make_async_copy(
            tok_ref.at[pl.ds(i * step_rows, step_rows)], tok.at[pl.ds(i * step_rows, step_rows)], tok_sem.at[i]
        )
        for i in range(4)
    ]
    for copy in tok_copies:
        copy.start()

    def place(a, shard):
        at = pl.ds(pl.multiple_of(shard * depth, depth), depth)
        if flip and a < QUERY:
            return kv_all.at[pl.ds(a * HEAD_DIM, HEAD_DIM), at]
        return wholes[a].at[at]

    own_copies = [pltpu.make_async_copy(shards[a], place(a, me), own_sem.at[a]) for a in range(arrays)]
    for copy in own_copies:
        copy.start()

    barrier = pltpu.get_barrier_semaphore()

    @pl.when(has_left)
    def _():
        pl.semaphore_signal(barrier, inc=1, device_id={"sp": left}, device_id_type=MESH)

    @pl.when(has_right)
    def _():
        pl.semaphore_signal(barrier, inc=1, device_id={"sp": right}, device_id_type=MESH)

    pl.semaphore_wait(barrier, has_left.astype(jnp.int32) + has_right.astype(jnp.int32))

    def hop(a, shard, to_right, own=False):
        return pltpu.make_async_remote_copy(
            src_ref=shards[a] if own else place(a, shard),
            dst_ref=place(a, shard),
            send_sem=(right_sem if to_right else left_sem).at[a, shard],
            recv_sem=recv_sem.at[a, shard],
            device_id={"sp": right if to_right else left},
            device_id_type=MESH,
        )

    def send_own(a):
        @pl.when(has_right)
        def _():
            hop(a, me, True, True).start()

        @pl.when(has_left)
        def _():
            hop(a, me, False, True).start()

    def pass_on(a, first, last):
        def step(k, carry):
            @pl.when(me - k >= 0)
            def _():
                shard = me - k
                hop(a, shard, False).wait_recv()

                @pl.when(has_right)
                def _():
                    hop(a, shard, True).start()

            @pl.when(me + k < n)
            def _():
                shard = me + k
                hop(a, shard, True).wait_recv()

                @pl.when(has_left)
                def _():
                    hop(a, shard, False).start()

            return carry

        lax.fori_loop(first, last, step, 0)

    for a in range(GATE):
        send_own(a)

    norm_rows = 64
    for i in range(4):
        tok_copies[i].wait()

        @pl.loop(0, step_rows // norm_rows)
        def _(j):
            at = pl.ds(pl.multiple_of(i * step_rows + j * norm_rows, norm_rows), norm_rows)
            wide = tok[at, :].astype(f32)
            scale = lax.rsqrt(jnp.mean(wide * wide, axis=-1, keepdims=True) + EPS)
            normed[at, :] = (wide * scale * gain_ref[...]).astype(bf16)

    for copy in own_copies:
        copy.wait()

    tile = 256

    def project(a, store):
        @pl.loop(0, rows // tile)
        def _(i):
            base = pl.multiple_of(i * tile, tile)
            side = 1 if flip and a < QUERY else 0
            store(
                base,
                lax.dot_general(
                    normed[pl.ds(base, tile), :],
                    wholes[a][...],
                    (((1,), (side,)), ((), ())),
                    preferred_element_type=f32,
                ),
            )

    def halo(buffer, length, i):
        return pltpu.make_async_remote_copy(
            src_ref=buffer.at[pl.ds(rows, length)],
            dst_ref=buffer.at[pl.ds(0, length)],
            send_sem=halo_send.at[i],
            recv_sem=halo_recv.at[i],
            device_id={"sp": right},
            device_id_type=MESH,
        )

    for a in range(QUERY):
        pass_on(a, 1, n)
    send_own(GATE)

    def store_kv(base, value):
        kv[pl.ds(base + WINDOW, tile), :] = value.astype(bf16)

    project(0, store_kv)

    @pl.when(jnp.logical_not(has_left))
    def _():
        kv[pl.ds(0, WINDOW), :] = jnp.zeros((WINDOW, kv.shape[1]), bf16)
        conv_in[pl.ds(0, PAD), :] = jnp.zeros((PAD, conv_in.shape[1]), f32)

    pass_on(QUERY, 1, n)

    @pl.when(has_right)
    def _():
        halo(kv, WINDOW, 0).start()

    def store_query(base, value):
        query[pl.ds(base, tile), :] = value.astype(bf16)

    project(QUERY, store_query)

    heads = query.shape[1] // HEAD_DIM
    query_idx = lax.broadcasted_iota(jnp.int32, (WINDOW, 2 * WINDOW), 0)
    key_idx = lax.broadcasted_iota(jnp.int32, (WINDOW, 2 * WINDOW), 1)
    gap = query_idx + WINDOW - key_idx
    band = (gap >= 0) & (gap < WINDOW)
    lane = lax.broadcasted_iota(jnp.int32, (2 * WINDOW, LANES), 1)
    low = lane < HEAD_DIM
    stat_lane = lax.broadcasted_iota(jnp.int32, (WINDOW, LANES), 1)

    def attend(b, kept):
        base = pl.multiple_of(b * WINDOW, WINDOW)
        both = kv[pl.ds(base, 2 * WINDOW), :].astype(f32)
        turned = pltpu.roll(both, HEAD_DIM, 1)
        zero = jnp.zeros_like(both)
        keys = (jnp.where(low, both, zero).astype(bf16), jnp.where(low, zero, turned).astype(bf16))
        vals = (jnp.where(low, turned, zero).astype(bf16), jnp.where(low, zero, both).astype(bf16))
        stats = jnp.zeros((WINDOW, LANES), f32)
        for pair in range(heads // 2):
            cols = pl.ds(pair * LANES, LANES)
            q = query[pl.ds(base, WINDOW), cols]
            out = None
            for side in range(2):
                head = 2 * pair + side
                scores = lax.dot_general(
                    q, keys[side], (((1,), (1,)), ((), ())), preferred_element_type=f32
                ) * HEAD_DIM ** (-0.5)
                scores = jnp.where(kept, scores, -jnp.inf)
                sink = jnp.full((WINDOW, 1), sink_ref[head], f32)
                top = jnp.maximum(jnp.max(scores, axis=-1, keepdims=True), sink)
                raised = jnp.exp(scores - top)
                total = jnp.sum(raised, axis=-1, keepdims=True) + jnp.exp(sink - top)
                weights = (raised * (1.0 / total)).astype(bf16)
                part = jnp.dot(weights, vals[side], preferred_element_type=f32)
                out = part if out is None else out + part
                stats = jnp.where(stat_lane == head, top + jnp.log(total), stats)
            attended[pl.ds(base, WINDOW), cols] = out
        log_ref[:, pl.ds(base, WINDOW)] = jnp.transpose(stats)[:heads]

    def attend_range(first, last):
        @pl.loop(first, last)
        def _(b):
            attend(b, band)

    cut = [1 + (n - 1) * i // 3 for i in range(4)]
    mid = 1 + (blocks - 1) // 2
    attend_range(1, mid)
    pass_on(CONV, cut[0], cut[1])
    attend_range(mid, blocks)
    pass_on(CONV, cut[1], cut[2])

    @pl.when(has_left)
    def _():
        halo(kv, WINDOW, 0).wait_recv()

    attend(0, band & ((key_idx >= WINDOW) | has_left))
    pass_on(CONV, cut[2], cut[3])

    def store_conv(base, value):
        conv_in[pl.ds(base + PAD, tile), :] = value.astype(bf16).astype(f32)

    project(CONV, store_conv)
    early = min(2, n - 1)
    pass_on(GATE, 1, early)

    @pl.when(has_right)
    def _():
        halo(conv_in, PAD, 1).start()

    pass_on(GATE, early, n - 1)

    far = jnp.where(2 * me >= n, 0, n - 1)

    def gate_part(base, shard):
        at = pl.ds(pl.multiple_of(shard * depth, depth), depth)
        return jnp.dot(
            normed[pl.ds(base, tile), at], cg_all[at, :], preferred_element_type=f32
        )

    if flip:

        @pl.loop(0, rows // tile)
        def _(i):
            base = pl.multiple_of(i * tile, tile)
            part = gate_part(base, lax.rem(far + 1, n))
            for j in range(2, n):
                part = part + gate_part(base, lax.rem(far + j, n))
            gate_sum[pl.ds(base, tile), :] = part

    pass_on(GATE, n - 1, n)

    @pl.when(has_left)
    def _():
        halo(conv_in, PAD, 1).wait_recv()

    def store_mixed(base, value):
        gate = value.astype(bf16).astype(f32)
        taps = taps_ref[...].astype(f32)
        near = conv_in[pl.ds(base, tile + PAD), :]
        total = jnp.zeros_like(gate)
        for k in range(TAPS):
            start = PAD - TAPS + 1 + k
            total = total + taps[k : k + 1] * near[start : start + tile]
        mixed_ref[pl.ds(base, tile), :] = (attended[pl.ds(base, tile), :] + gate * total).astype(bf16)

    if flip:

        @pl.loop(0, rows // tile)
        def _(i):
            base = pl.multiple_of(i * tile, tile)
            store_mixed(base, gate_sum[pl.ds(base, tile), :] + gate_part(base, far))

    else:
        project(GATE, store_mixed)

    @pl.when(has_right)
    def _():
        halo(kv, WINDOW, 0).wait_send()
        halo(conv_in, PAD, 1).wait_send()

    for a in range(arrays):

        @pl.when(has_right)
        def _():
            @pl.loop(0, me + 1)
            def _(s):
                hop(a, s, True).wait_send()

        @pl.when(has_left)
        def _():
            @pl.loop(me, n)
            def _(s):
                hop(a, s, False).wait_send()


def write_out(mixed_ref, log_ref, mixed_out, log_out, sems):
    copies = [
        pltpu.make_async_copy(mixed_ref, mixed_out, sems.at[0]),
        pltpu.make_async_copy(log_ref, log_out, sems.at[1]),
    ]
    for copy in copies:
        copy.start()
    for copy in copies:
        copy.wait()


def paired_kernel(tok_ref, gain_ref, *refs):
    shards = refs[:5]
    (
        taps_ref, sink_ref, mixed_ref, log_ref,
        tok, normed, other, kv_all, q_all, stage, conv_w, kv, query, q_part, attended,
        conv_in, convolved, sums, conv_out, conv_back, turned_taps, edge_out, edge_in,
        tok_sem, own_sem, recv_sem, sent_sem, halo_recv, x_recv, twin_recv, out_recv,
    ) = refs[5:]
    f32, bf16 = jnp.float32, jnp.bfloat16
    me, fs, tp = lax.axis_index("sp"), lax.axis_index("fs"), lax.axis_index("tp")
    low = me < 2
    end = (me == 0) | (me == 3)
    middle = jnp.logical_not(end)
    mate = me + 1 - 2 * lax.rem(me, 2)
    peer = jnp.where(end, 3 - mate, 3 - me)
    far = jnp.where(low, 3, 0)
    first = jnp.where(low, 0, 1)
    has_left, has_right = me > 0, me < 3
    right = jnp.minimum(me + 1, 3)
    across, along = fs + 1 - 2 * lax.rem(fs, 2), lax.rem(fs + 2, 4)
    diagonal = 3 - fs
    twin = 1 - tp
    rows = tok.shape[0]
    depth = shards[2].shape[0]
    blocks = rows // WINDOW
    width = q_all.shape[1]
    widths = (width // 4, width // 4, width // 4, width // 8, width // 8)
    groups = range(len(widths))
    channel = [sum(widths[:g]) for g in groups]
    K, V, Q, R, A, B, C, D, E = units = range(9)

    parts = 8
    part_rows = rows // parts
    pieces = 4
    piece = part_rows // pieces
    own_part = fs * 2 + tp

    def part_at(i):
        return lax.rem(own_part + i, parts)

    def rows_of(start, length):
        return pl.ds(pl.multiple_of(start, 16), length)

    tok_copies = []
    for i in range(parts):
        at = rows_of(part_at(i) * part_rows, part_rows)
        tok_copies.append(pltpu.make_async_copy(tok_ref.at[at], tok.at[at], tok_sem.at[min(i, 1)]))

    def shard_at(shard):
        return pl.ds(pl.multiple_of(shard * depth, depth), depth)

    def place(u, shard):
        at = shard_at(shard)
        if u < Q:
            return kv_all.at[pl.ds(u * HEAD_DIM, HEAD_DIM), at]
        if u < A:
            return q_all.at[at, pl.ds((u - Q) * LANES, LANES)]
        return conv_w.at[pl.ds(2 * channel[u - A], 2 * widths[u - A]), at]

    own_copies = [pltpu.make_async_copy(shards[u], place(u, me), own_sem.at[0]) for u in (K, V)]
    own_copies.append(pltpu.make_async_copy(shards[2], q_all.at[shard_at(me)], own_sem.at[1]))
    own_copies += [pltpu.make_async_copy(shards[3 + j], stage.at[j], own_sem.at[2]) for j in range(2)]
    for copy in own_copies[:3] + tok_copies[:1] + own_copies[3:] + tok_copies[1:]:
        copy.start()

    def norm_part(i):
        norm_rows = 64

        @pl.loop(0, part_rows // norm_rows)
        def _(j):
            at = rows_of(part_at(i) * part_rows + j * norm_rows, norm_rows)
            wide = tok[at, :].astype(f32)
            scale = lax.rsqrt(jnp.mean(wide * wide, axis=-1, keepdims=True) + EPS)
            normed[at, :] = (wide * scale * gain_ref[...]).astype(bf16)

    barrier = pltpu.get_barrier_semaphore()

    def greet(**device):
        pl.semaphore_signal(barrier, inc=1, device_id=device, device_id_type=MESH)

    greet(sp=mate)

    @pl.when(middle)
    def _():
        greet(sp=peer)
        greet(fs=across)
        greet(fs=along)
        greet(tp=twin)

    pl.semaphore_wait(barrier, jnp.where(middle, 5, 1))

    TO_MATE, TO_PEER, RELAYED, RETURNED, EDGES, HALO = range(6)

    def slot(shard, device):
        return shard - jnp.where(shard > device, 1, 0)

    def source(u):
        return shards[u] if u < Q else shards[2].at[:, pl.ds((u - Q) * LANES, LANES)]

    def hop(u, shard, to_mate):
        target = mate if to_mate else peer
        return pltpu.make_async_remote_copy(
            src_ref=source(u) if shard is me and u < A else place(u, shard),
            dst_ref=place(u, shard),
            send_sem=sent_sem.at[TO_MATE if to_mate else TO_PEER],
            recv_sem=recv_sem.at[u, slot(shard, target)],
            device_id={"sp": target},
            device_id_type=MESH,
        )

    def arrived(u, shard):
        ref = place(u, shard)
        pltpu.make_async_copy(ref, ref, recv_sem.at[u, slot(shard, me)]).wait()

    def drain(kind, elements):
        ref = other.at[pl.ds(0, elements // other.shape[1])]
        pltpu.make_async_copy(ref, ref, sent_sem.at[kind]).wait()

    def piece_at(part, h):
        return rows_of(part * part_rows + h * piece, piece)

    def piece_copy(buffer, part, h, kind, arrival, **device):
        at = piece_at(part, h)
        return pltpu.make_async_remote_copy(
            src_ref=buffer.at[at],
            dst_ref=other.at[at],
            send_sem=sent_sem.at[kind],
            recv_sem=arrival,
            device_id=device,
            device_id_type=MESH,
        )

    def line_sem(part, h):
        return x_recv.at[part // 2, h]

    def piece_arrived(part, h):
        ref = other.at[piece_at(part, h)]
        pltpu.make_async_copy(ref, ref, line_sem(part, h)).wait()

    across_part, along_part, diagonal_part = across * 2 + tp, along * 2 + tp, diagonal * 2 + tp
    relays = [(own_part, h, ("tp", "fs_across", "fs_along")) for h in range(pieces)]
    relays += [(across_part, h, ("tp", "fs_along")[: 2 - h % 2]) for h in range(pieces)]
    relays += [(along_part, h, ("tp", "fs_across")[: 1 + h % 2]) for h in range(pieces)]
    relays += [(diagonal_part, h, ("tp",)) for h in range(pieces)]
    OWN_X, ACROSS, ALONG, DIAGONAL = (pieces * j for j in range(4))
    devices = {"tp": {"tp": twin}, "fs_across": {"fs": across}, "fs_along": {"fs": along}}

    def relay_copies(j):
        part, h, to = relays[j]
        return [
            piece_copy(other, part, h, RELAYED, twin_recv.at[0] if d == "tp" else line_sem(part, h), **devices[d])
            for d in to
        ]

    def relay(*which):
        for j in which:
            piece_arrived(relays[j][0], relays[j][1])
            for copy in relay_copies(j):
                copy.start()

    def send(to_mate, shard, *which):
        for u in which:
            hop(u, shard, to_mate).start()

    def forward(to_mate, shard, *which):
        for u in which:
            arrived(u, shard)
            hop(u, shard, to_mate).start()

    def pieces_out(*which):
        for h in which:
            piece_copy(normed, own_part, h, RELAYED, line_sem(own_part, h), sp=mate).start()

    @pl.when(middle)
    def _():
        send(False, me, K, V, Q, R)
        send(True, me, K, V, Q, R)

    tok_copies[0].wait()
    norm_part(0)

    @pl.when(end)
    def _():
        pieces_out(*range(pieces))
        send(True, me, K, V, Q, R)

    pltpu.make_async_copy(stage, stage, own_sem.at[2]).wait()
    for j in range(2):
        for block in range(depth // LANES):
            turned = jnp.transpose(stage[j, pl.ds(block * LANES, LANES), :].astype(f32)).astype(bf16)
            at = pl.ds(pl.multiple_of(me * depth + block * LANES, LANES), LANES)
            for g in groups:
                to = pl.ds(2 * channel[g] + j * widths[g], widths[g])
                conv_w[to, at] = turned[channel[g] : channel[g] + widths[g]]
    taps = taps_ref[...].astype(f32)
    turned_taps[...] = jnp.transpose(jnp.concatenate([taps, jnp.zeros((8 - TAPS, width), f32)], axis=0))
    conv_in[:, pl.ds(0, LANES)] = jnp.zeros((width, LANES), f32)

    @pl.when(end)
    def _():
        send(True, me, A, B, C)

    @pl.when(middle)
    def _():
        send(False, me, A, B, C, D)

    own_kv = kv_all.at[:, shard_at(me)]
    pltpu.make_async_copy(own_kv, own_kv, own_sem.at[0]).wait()
    own_copies[2].wait()

    others = tok.at[pl.ds(0, rows - part_rows)]
    pltpu.make_async_copy(others, others, tok_sem.at[1]).wait()
    for i in range(1, parts):
        norm_part(i)

    tile = 512

    early = pl.ds(pl.multiple_of(first * depth, depth), 3 * depth)
    late = pl.ds(pl.multiple_of(far * depth, depth), depth)

    kv_halo = pltpu.make_async_remote_copy(
        src_ref=kv.at[pl.ds(rows, WINDOW)],
        dst_ref=kv.at[pl.ds(0, WINDOW)],
        send_sem=sent_sem.at[HALO],
        recv_sem=halo_recv.at[0],
        device_id={"sp": right},
        device_id_type=MESH,
    )

    own_base, mate_base = jnp.where(me == 1, rows, 0), jnp.where(me == 1, 0, rows)
    bases = (own_base, mate_base)
    sources = (normed, other)
    tiles = rows // tile
    OWN, MATE = 0, 1

    def tile_at(i):
        return pl.ds(i * tile if isinstance(i, int) else pl.multiple_of(i * tile, tile), tile)

    def out_copy(g, i):
        at = (pl.ds(channel[g], widths[g]), tile_at(i))
        return pltpu.make_async_remote_copy(
            src_ref=conv_out.at[at],
            dst_ref=conv_back.at[at],
            send_sem=sent_sem.at[RETURNED],
            recv_sem=out_recv.at[g * tiles + i],
            device_id={"sp": mate},
            device_id_type=MESH,
        )

    def edge_copy(g):
        return pltpu.make_async_remote_copy(
            src_ref=edge_out.at[g],
            dst_ref=edge_in.at[g],
            send_sem=sent_sem.at[EDGES],
            recv_sem=halo_recv.at[1 + g],
            device_id={"sp": right},
            device_id_type=MESH,
        )

    center = pl.ds(depth, 2 * depth)
    everything = pl.ds(0, conv_w.shape[1])
    edge_tokens = pl.ds(rows - LANES, LANES)

    def dot(which, tokens, start, length, at):
        return lax.dot_general(
            conv_w[pl.ds(start, length), at],
            sources[which][tokens, at],
            (((1,), (1,)), ((), ())),
            preferred_element_type=f32,
        )

    def partial(which, i, u, v, at, fresh=False):
        start = 2 * channel[u - A]
        span = pl.ds(start, 2 * channel[v - A] + 2 * widths[v - A] - start)
        value = dot(which, tile_at(i), span.start, span.size, at)
        sums[which, span, tile_at(i)] = value if fresh else sums[which, span, tile_at(i)] + value

    def product(which, tokens, start, length):
        if which == OWN and start == 2 * channel[-1] and tokens is not edge_tokens:
            return dot(which, tokens, start, length, everything)
        return sums[which, pl.ds(start, length), tokens] + dot(which, tokens, start, length, late)

    def keep(g, at, value):
        value = value.astype(bf16).astype(f32)
        conv_in[pl.ds(channel[g], widths[g]), pl.ds(pl.multiple_of(at + LANES, LANES), value.shape[1])] = value[: widths[g]]
        return value[widths[g] :]

    def convolve(g, at, gate):
        of = pl.ds(channel[g], widths[g])
        near = conv_in[of, pl.ds(pl.multiple_of(at, LANES), tile + LANES)]
        total = jnp.zeros((widths[g], tile), f32)
        for k in range(TAPS):
            moved = near if k == TAPS - 1 else pltpu.roll(near, TAPS - 1 - k, 1)
            total = total + turned_taps[of, k : k + 1] * moved[:, LANES:]
        return gate * total

    def mate_tiles(g):
        of = pl.ds(channel[g], widths[g])
        keep(g, own_base + rows - LANES, product(OWN, edge_tokens, 2 * channel[g], 2 * widths[g]))
        for i in range(tiles):
            at = mate_base + i * tile
            value = product(MATE, tile_at(i), 2 * channel[g], 2 * widths[g])
            conv_out[of, tile_at(i)] = convolve(g, at, keep(g, at, value)).astype(bf16)
            out_copy(g, i).start()

        @pl.when(me == 1)
        def _():
            edge = jnp.transpose(conv_in[of, pl.ds(2 * rows, LANES)])
            edge_out[g, :, pl.ds(0, widths[g])] = edge[LANES - PAD :]
            edge_copy(g).start()

    def own_tiles(*which):
        @pl.when(me == 2)
        def _():
            for g in which:
                of = pl.ds(channel[g], widths[g])
                edge_copy(g).wait_recv()
                edge = edge_in[g, :, pl.ds(0, widths[g])]
                edge = jnp.concatenate([jnp.zeros((LANES - PAD, widths[g]), f32), edge], axis=0)
                conv_in[of, pl.ds(0, LANES)] = jnp.transpose(edge)

        start = 2 * channel[which[0]]
        length = sum(2 * widths[g] for g in which)
        for i in range(tiles):
            at = own_base + i * tile
            value = product(OWN, tile_at(i), start, length)
            for g in which:
                row = 2 * channel[g] - start
                gate = keep(g, at, value[row : row + 2 * widths[g]])
                convolved[pl.ds(channel[g], widths[g]), tile_at(i)] = convolve(g, at, gate)

    def mix(half, i, source):
        cols = pl.ds(half * LANES, LANES)
        for j in range(tile // LANES):
            at = pl.ds(i * tile + j * LANES, LANES)
            extra = jnp.transpose(source[cols, at].astype(f32))
            mixed_ref[at, cols] = (attended[at, cols] + extra).astype(bf16)

    @pl.when(middle)
    def _():
        relay(OWN_X)
        forward(True, peer, K, V)
        relay(OWN_X + 1)
        forward(True, peer, Q)
        relay(ACROSS, ALONG)
        forward(True, peer, R)
        relay(OWN_X + 2, ACROSS + 1, ALONG + 1, OWN_X + 3)
        forward(False, mate, K, V)
        relay(ACROSS + 2, ALONG + 2)
        forward(False, mate, Q)
        relay(DIAGONAL, DIAGONAL + 1)
        forward(False, mate, R)
        for u in (A, B, C, D):
            arrived(u, peer)
        partial(OWN, 0, A, D, center, True)
        relay(ACROSS + 3, ALONG + 3)
        forward(True, far, K, V)
        forward(False, mate, A)

    @pl.when(end)
    def _():
        for shard in (mate, peer, far):
            for u in (K, V):
                arrived(u, shard)

    @pl.loop(0, rows // tile)
    def _(i):
        base = pl.multiple_of(i * tile, tile)
        kv[pl.ds(base + WINDOW, tile), :] = lax.dot_general(
            normed[pl.ds(base, tile), :], kv_all[...], (((1,), (1,)), ((), ())), preferred_element_type=f32
        ).astype(bf16)

    @pl.when(jnp.logical_not(has_left))
    def _():
        kv[pl.ds(0, WINDOW), :] = jnp.zeros((WINDOW, kv.shape[1]), bf16)

    @pl.when(has_right)
    def _():
        kv_halo.start()

    @pl.when(middle)
    def _():
        forward(True, far, Q)
        partial(OWN, 1, A, D, center, True)
        forward(False, mate, B)

    @pl.when(end)
    def _():
        send(True, me, D, E)
        for u in (Q, R):
            arrived(u, mate)
            arrived(u, peer)

    @pl.loop(0, rows // tile)
    def _(i):
        at = pl.ds(pl.multiple_of(i * tile, tile), tile)
        q_part[at, :] = jnp.dot(normed[at, early], q_all[early, :], preferred_element_type=f32)

    @pl.when(middle)
    def _():
        forward(True, far, R)

    @pl.when(end)
    def _():
        arrived(Q, far)
        arrived(R, far)

    @pl.loop(0, rows // tile)
    def _(i):
        at = pl.ds(pl.multiple_of(i * tile, tile), tile)
        query[at, :] = (
            q_part[at, :] + jnp.dot(normed[at, late], q_all[late, :], preferred_element_type=f32)
        ).astype(bf16)

    heads = query.shape[1] // HEAD_DIM
    query_idx = lax.broadcasted_iota(jnp.int32, (WINDOW, 2 * WINDOW), 0)
    key_idx = lax.broadcasted_iota(jnp.int32, (WINDOW, 2 * WINDOW), 1)
    gap = query_idx + WINDOW - key_idx
    band = (gap >= 0) & (gap < WINDOW)
    low_lanes = lax.broadcasted_iota(jnp.int32, (2 * WINDOW, LANES), 1) < HEAD_DIM
    lane = lax.broadcasted_iota(jnp.int32, (WINDOW, LANES), 1)
    low_half = lane < HEAD_DIM

    def attend(b, kept):
        base = pl.multiple_of(b * WINDOW, WINDOW)
        both = kv[pl.ds(base, 2 * WINDOW), :].astype(f32)
        turned = pltpu.roll(both, HEAD_DIM, 1)
        zero, one = jnp.zeros_like(both), jnp.ones_like(both)

        def lower(x):
            return jnp.where(low_lanes, x, zero)

        def upper(x):
            return jnp.where(low_lanes, zero, x)

        keys = jnp.concatenate([lower(both), upper(turned)], axis=0).astype(bf16)
        vals = jnp.concatenate([lower(turned), upper(both)], axis=0)
        ones = jnp.concatenate([lower(one), upper(one)], axis=0)
        vals = jnp.concatenate([vals, ones], axis=1).astype(bf16)
        stats = []
        for pair in range(heads // 2):
            cols = pl.ds(pair * LANES, LANES)
            scores = lax.dot_general(
                query[pl.ds(base, WINDOW), cols], keys, (((1,), (1,)), ((), ())), preferred_element_type=f32
            )
            sinks = [sink_ref[2 * pair + side] * LOG2_E for side in range(2)]
            tops, raised = [], []
            for side in range(2):
                part = scores[:, side * 2 * WINDOW : (side + 1) * 2 * WINDOW] * (HEAD_DIM ** (-0.5) * LOG2_E)
                part = jnp.where(kept, part, -jnp.inf)
                tops.append(jnp.maximum(jnp.max(part, axis=-1, keepdims=True), sinks[side]))
                raised.append(jnp.exp2(part - tops[side]).astype(bf16))
            out = jnp.dot(jnp.concatenate(raised, axis=1), vals, preferred_element_type=f32)
            top = jnp.where(low_half, tops[0], tops[1])
            total = out[:, LANES:] + jnp.exp2(jnp.where(low_half, sinks[0], sinks[1]) - top)
            attended[pl.ds(base, WINDOW), cols] = out[:, :LANES] / total
            stats.append(top * LN_2 + jnp.log(total))
        turned_stats = jnp.transpose(jnp.where(lax.rem(lane, 2) == 0, stats[0], stats[1]))
        for pair in range(2):
            for side in range(2):
                row = pair + side * HEAD_DIM
                head = 2 * pair + side
                log_ref[head : head + 1, pl.ds(base, WINDOW)] = turned_stats[row : row + 1]

    def finish(g):
        arrived(A + g, far)
        mate_tiles(g)

    @pl.when(middle)
    def _():
        relay(DIAGONAL + 2, DIAGONAL + 3)
        half_rows = other.at[pl.ds(0, rows // 2)]
        pltpu.make_async_copy(half_rows, half_rows, twin_recv.at[0]).wait()
        for i in range(tiles):
            partial(MATE, i, A, D, center, True)
        forward(False, mate, C)
        send(False, me, E)
        for i in range(tiles):
            partial(MATE, i, A, B, shard_at(mate))
        partial(OWN, tiles - 1, A, B, shard_at(mate))
        finish(0)
        for i in range(tiles - 1):
            partial(OWN, i, A, B, shard_at(mate))

    def attend_pairs(start, stop):
        @pl.loop(start, stop)
        def _(j):
            attend(2 * j + 1, band)
            attend(2 * j + 2, band)

    cut = (blocks // 2 - 1) * 2 // 3
    attend_pairs(0, cut)

    @pl.when(middle)
    def _():
        forward(False, mate, D, E)
        finish(1)

    attend_pairs(cut, blocks // 2 - 1)

    @pl.when(has_left)
    def _():
        kv_halo.wait_recv()

    @pl.when(middle)
    def _():
        for i in range(tiles):
            partial(MATE, i, C, D, shard_at(mate))
        partial(OWN, tiles - 1, C, D, shard_at(mate))
        finish(2)
        arrived(E, peer)
        for i in range(tiles):
            partial(MATE, i, E, E, early, True)
        sums[OWN, pl.ds(2 * channel[4], 2 * widths[4]), edge_tokens] = dot(
            OWN, edge_tokens, 2 * channel[4], 2 * widths[4], early
        )
        finish(3)
        finish(4)
        for i in range(tiles - 1):
            partial(OWN, i, C, D, shard_at(mate))

    attend(blocks - 1, band)
    attend(0, band & ((key_idx >= WINDOW) | has_left))

    @pl.when(middle)
    def _():
        own_tiles(0, 1)
        own_tiles(2, 3)
        own_tiles(4)
        for half in range(2):
            for i in range(tiles):
                mix(half, i, convolved)

    @pl.when(end)
    def _():
        for half in range(2):
            for i in range(tiles):
                for g in (groups[:2], groups[2:])[half]:
                    out_copy(g, i).wait_recv()
                mix(half, i, conv_back)

    @pl.when(has_right)
    def _():
        kv_halo.wait_send()

    attention_shard = depth * (2 * HEAD_DIM + width)
    whole_shard = attention_shard + depth * 2 * width

    @pl.when(end)
    def _():
        drain(TO_MATE, whole_shard)
        drain(RELAYED, part_rows * other.shape[1])

    @pl.when(middle)
    def _():
        drain(TO_MATE, 3 * attention_shard)
        drain(TO_PEER, 2 * whole_shard)
        drain(RELAYED, sum(len(to) for _, _, to in relays) * piece * other.shape[1])
        pltpu.make_async_copy(conv_out, conv_out, sent_sem.at[RETURNED]).wait()

        @pl.when(me == 1)
        def _():
            pltpu.make_async_copy(edge_out, edge_out, sent_sem.at[EDGES]).wait()


def paired_body(tokens, norm_gain, w_query, w_key, w_value, w_conv_in, w_conv_gate, conv_taps, sink_logits):
    rows, features = tokens.shape
    width = w_query.shape[1]
    f32, bf16 = jnp.float32, jnp.bfloat16
    hbm = pl.BlockSpec(memory_space=pltpu.HBM)
    vmem = pl.BlockSpec(memory_space=pltpu.VMEM)
    smem = pl.BlockSpec(memory_space=pltpu.SMEM)
    dma = pltpu.SemaphoreType.DMA
    tiles = rows // 512
    results = pl.pallas_call(
        paired_kernel,
        out_shape=(
            pltpu.VMEM((rows, width), bf16),
            pltpu.VMEM((width // HEAD_DIM, rows), f32),
        ),
        in_specs=[hbm, vmem] + [hbm] * 5 + [vmem, smem],
        out_specs=(vmem, vmem),
        scratch_shapes=[
            pltpu.VMEM((rows, features), bf16),
            pltpu.VMEM((rows, features), bf16),
            pltpu.VMEM((rows, features), bf16),
            pltpu.VMEM((2 * HEAD_DIM, features), bf16),
            pltpu.VMEM((features, width), bf16),
            pltpu.VMEM((2, w_query.shape[0], width), bf16),
            pltpu.VMEM((2 * width, features), bf16),
            pltpu.VMEM((rows + WINDOW, 2 * HEAD_DIM), bf16),
            pltpu.VMEM((rows, width), bf16),
            pltpu.VMEM((rows, width), f32),
            pltpu.VMEM((rows, width), f32),
            pltpu.VMEM((width, LANES + 2 * rows), f32),
            pltpu.VMEM((width, rows), f32),
            pltpu.VMEM((2, 2 * width, rows), f32),
            pltpu.VMEM((width, rows), bf16),
            pltpu.VMEM((width, rows), bf16),
            pltpu.VMEM((width, 8), f32),
            pltpu.VMEM((5, PAD, LANES), f32),
            pltpu.VMEM((5, PAD, LANES), f32),
            dma((2,)),
            dma((3,)),
            dma((9, 3)),
            dma((6,)),
            dma((6,)),
            dma((4, 4)),
            dma((1,)),
            dma((5 * tiles,)),
        ],
        compiler_params=pltpu.CompilerParams(
            collective_id=0, has_side_effects=True, vmem_limit_bytes=59 << 20
        ),
        name="paired_attend_convolve",
    )(tokens, norm_gain.reshape(1, -1), w_key.T, w_value.T, w_query, w_conv_in, w_conv_gate, conv_taps, sink_logits)
    return pl.pallas_call(
        write_out,
        out_shape=(
            jax.ShapeDtypeStruct((rows, width), bf16),
            jax.ShapeDtypeStruct((width // HEAD_DIM, rows), f32),
        ),
        in_specs=[vmem, vmem],
        out_specs=(hbm, hbm),
        scratch_shapes=[dma((2,))],
        name="write_out",
    )(*[pltpu.with_memory_space_constraint(result, pltpu.VMEM) for result in results])


def line_body(n, tokens, norm_gain, w_query, w_key, w_value, w_conv_in, w_conv_gate, conv_taps, sink_logits):
    rows, features = tokens.shape
    width, kv_width = w_query.shape[1], w_key.shape[1] + w_value.shape[1]
    assert w_key.shape[1] == HEAD_DIM and width % LANES == 0
    depth = w_query.shape[0]
    flip = depth % LANES == 0 and 2 < n <= 16
    if flip:
        w_kv, kv_shape = (w_key.T, w_value.T), (kv_width, features)
    else:
        w_kv, kv_shape = (jnp.concatenate([w_key, w_value], axis=1),), (features, kv_width)
    arrays = 3 + len(w_kv)
    f32, bf16 = jnp.float32, jnp.bfloat16
    hbm = pl.BlockSpec(memory_space=pltpu.HBM)
    vmem = pl.BlockSpec(memory_space=pltpu.VMEM)
    smem = pl.BlockSpec(memory_space=pltpu.SMEM)
    dma = pltpu.SemaphoreType.DMA
    return pl.pallas_call(
        functools.partial(line_kernel, n, flip),
        out_shape=(
            pltpu.VMEM((rows, width), bf16),
            pltpu.VMEM((width // HEAD_DIM, rows), f32),
        ),
        in_specs=[hbm, vmem] + [hbm] * arrays + [vmem, smem],
        out_specs=(vmem, vmem),
        scratch_shapes=[
            pltpu.VMEM((rows, features), bf16),
            pltpu.VMEM((rows, features), bf16),
            pltpu.VMEM(kv_shape, bf16),
            pltpu.VMEM((features, width), bf16),
            pltpu.VMEM((features, width), bf16),
            pltpu.VMEM((features, width), bf16),
            pltpu.VMEM((rows + WINDOW, kv_width), bf16),
            pltpu.VMEM((rows, width), bf16),
            pltpu.VMEM((rows, width), f32),
            pltpu.VMEM((rows + PAD, width), f32),
            pltpu.VMEM((rows, width), f32),
            dma((4,)),
            dma((arrays,)),
            dma((arrays, n)),
            dma((arrays, n)),
            dma((arrays, n)),
            dma((2,)),
            dma((2,)),
        ],
        compiler_params=pltpu.CompilerParams(
            collective_id=0, has_side_effects=True, vmem_limit_bytes=59 << 20
        ),
        name="gather_attend_convolve",
    )(tokens, norm_gain.reshape(1, -1), *w_kv, w_query, w_conv_in, w_conv_gate, conv_taps, sink_logits)


def body(n, fs, tp, *arrays):
    rows, width, depth = arrays[0].shape[0], arrays[2].shape[1], arrays[2].shape[0]
    square = n == 4 and fs == 4 and tp == 2
    if square and width == 2 * LANES and depth % LANES == 0 and rows % (8 * LANES) == 0:
        return paired_body(*arrays)
    return line_body(n, *arrays)


def solution(mesh):
    return jax.shard_map(
        functools.partial(body, mesh.shape["sp"], mesh.shape["fs"], mesh.shape["tp"]),
        mesh=mesh,
        in_specs=(
            P("sp", None),
            P(),
            P("sp", ("fs", "tp")),
            P("sp", ("fs", "tp")),
            P("sp", ("fs", "tp")),
            P("sp", ("fs", "tp")),
            P("sp", ("fs", "tp")),
            P(None, ("fs", "tp")),
            P(("fs", "tp")),
        ),
        out_specs=(P("sp", ("fs", "tp")), P(("fs", "tp"), "sp")),
        check_vma=False,
    )
```

```python
import functools
import math

import jax
import jax.numpy as jnp
from jax import lax
from jax.experimental import pallas as pl
from jax.experimental.pallas import tpu as pltpu
from jax.sharding import PartitionSpec as P

HEAD_DIM = 64
WINDOW = 128
TAPS = 3
EPS = 1e-06
LANES = 128
PAD = 8
LOG2_E = math.log2(math.e)
LN_2 = math.log(2)
MESH = pl.DeviceIdType.MESH


def line_kernel(
    n, flip, tok_ref, gain_ref, *refs
):
    arrays = 5 if flip else 4
    shards = refs[:arrays]
    (
        taps_ref, sink_ref, mixed_ref, log_ref,
        tok, normed, kv_all, q_all, ci_all, cg_all, kv, query, attended, conv_in, gate_sum,
        tok_sem, own_sem, recv_sem, right_sem, left_sem, halo_send, halo_recv,
    ) = refs[arrays:]
    QUERY, CONV, GATE = arrays - 3, arrays - 2, arrays - 1
    me = lax.axis_index("sp")
    rows = tok.shape[0]
    depth = shards[QUERY].shape[0]
    wholes = (kv_all, kv_all, q_all, ci_all, cg_all)[5 - arrays :]
    has_left, has_right = me > 0, me < n - 1
    left, right = jnp.maximum(me - 1, 0), jnp.minimum(me + 1, n - 1)
    blocks = rows // WINDOW
    f32, bf16 = jnp.float32, jnp.bfloat16

    step_rows = rows // 4
    tok_copies = [
        pltpu.make_async_copy(
            tok_ref.at[pl.ds(i * step_rows, step_rows)], tok.at[pl.ds(i * step_rows, step_rows)], tok_sem.at[i]
        )
        for i in range(4)
    ]
    for copy in tok_copies:
        copy.start()

    def place(a, shard):
        at = pl.ds(pl.multiple_of(shard * depth, depth), depth)
        if flip and a < QUERY:
            return kv_all.at[pl.ds(a * HEAD_DIM, HEAD_DIM), at]
        return wholes[a].at[at]

    own_copies = [pltpu.make_async_copy(shards[a], place(a, me), own_sem.at[a]) for a in range(arrays)]
    for copy in own_copies:
        copy.start()

    barrier = pltpu.get_barrier_semaphore()

    @pl.when(has_left)
    def _():
        pl.semaphore_signal(barrier, inc=1, device_id={"sp": left}, device_id_type=MESH)

    @pl.when(has_right)
    def _():
        pl.semaphore_signal(barrier, inc=1, device_id={"sp": right}, device_id_type=MESH)

    pl.semaphore_wait(barrier, has_left.astype(jnp.int32) + has_right.astype(jnp.int32))

    def hop(a, shard, to_right, own=False):
        return pltpu.make_async_remote_copy(
            src_ref=shards[a] if own else place(a, shard),
            dst_ref=place(a, shard),
            send_sem=(right_sem if to_right else left_sem).at[a, shard],
            recv_sem=recv_sem.at[a, shard],
            device_id={"sp": right if to_right else left},
            device_id_type=MESH,
        )

    def send_own(a):
        @pl.when(has_right)
        def _():
            hop(a, me, True, True).start()

        @pl.when(has_left)
        def _():
            hop(a, me, False, True).start()

    def pass_on(a, first, last):
        def step(k, carry):
            @pl.when(me - k >= 0)
            def _():
                shard = me - k
                hop(a, shard, False).wait_recv()

                @pl.when(has_right)
                def _():
                    hop(a, shard, True).start()

            @pl.when(me + k < n)
            def _():
                shard = me + k
                hop(a, shard, True).wait_recv()

                @pl.when(has_left)
                def _():
                    hop(a, shard, False).start()

            return carry

        lax.fori_loop(first, last, step, 0)

    for a in range(GATE):
        send_own(a)

    norm_rows = 64
    for i in range(4):
        tok_copies[i].wait()

        @pl.loop(0, step_rows // norm_rows)
        def _(j):
            at = pl.ds(pl.multiple_of(i * step_rows + j * norm_rows, norm_rows), norm_rows)
            wide = tok[at, :].astype(f32)
            scale = lax.rsqrt(jnp.mean(wide * wide, axis=-1, keepdims=True) + EPS)
            normed[at, :] = (wide * scale * gain_ref[...]).astype(bf16)

    for copy in own_copies:
        copy.wait()

    tile = 256

    def project(a, store):
        @pl.loop(0, rows // tile)
        def _(i):
            base = pl.multiple_of(i * tile, tile)
            side = 1 if flip and a < QUERY else 0
            store(
                base,
                lax.dot_general(
                    normed[pl.ds(base, tile), :],
                    wholes[a][...],
                    (((1,), (side,)), ((), ())),
                    preferred_element_type=f32,
                ),
            )

    def halo(buffer, length, i):
        return pltpu.make_async_remote_copy(
            src_ref=buffer.at[pl.ds(rows, length)],
            dst_ref=buffer.at[pl.ds(0, length)],
            send_sem=halo_send.at[i],
            recv_sem=halo_recv.at[i],
            device_id={"sp": right},
            device_id_type=MESH,
        )

    for a in range(QUERY):
        pass_on(a, 1, n)
    send_own(GATE)

    def store_kv(base, value):
        kv[pl.ds(base + WINDOW, tile), :] = value.astype(bf16)

    project(0, store_kv)

    @pl.when(jnp.logical_not(has_left))
    def _():
        kv[pl.ds(0, WINDOW), :] = jnp.zeros((WINDOW, kv.shape[1]), bf16)
        conv_in[pl.ds(0, PAD), :] = jnp.zeros((PAD, conv_in.shape[1]), f32)

    pass_on(QUERY, 1, n)

    @pl.when(has_right)
    def _():
        halo(kv, WINDOW, 0).start()

    def store_query(base, value):
        query[pl.ds(base, tile), :] = value.astype(bf16)

    project(QUERY, store_query)

    heads = query.shape[1] // HEAD_DIM
    query_idx = lax.broadcasted_iota(jnp.int32, (WINDOW, 2 * WINDOW), 0)
    key_idx = lax.broadcasted_iota(jnp.int32, (WINDOW, 2 * WINDOW), 1)
    gap = query_idx + WINDOW - key_idx
    band = (gap >= 0) & (gap < WINDOW)
    lane = lax.broadcasted_iota(jnp.int32, (2 * WINDOW, LANES), 1)
    low = lane < HEAD_DIM
    stat_lane = lax.broadcasted_iota(jnp.int32, (WINDOW, LANES), 1)

    def attend(b, kept):
        base = pl.multiple_of(b * WINDOW, WINDOW)
        both = kv[pl.ds(base, 2 * WINDOW), :].astype(f32)
        turned = pltpu.roll(both, HEAD_DIM, 1)
        zero = jnp.zeros_like(both)
        keys = (jnp.where(low, both, zero).astype(bf16), jnp.where(low, zero, turned).astype(bf16))
        vals = (jnp.where(low, turned, zero).astype(bf16), jnp.where(low, zero, both).astype(bf16))
        stats = jnp.zeros((WINDOW, LANES), f32)
        for pair in range(heads // 2):
            cols = pl.ds(pair * LANES, LANES)
            q = query[pl.ds(base, WINDOW), cols]
            out = None
            for side in range(2):
                head = 2 * pair + side
                scores = lax.dot_general(
                    q, keys[side], (((1,), (1,)), ((), ())), preferred_element_type=f32
                ) * HEAD_DIM ** (-0.5)
                scores = jnp.where(kept, scores, -jnp.inf)
                sink = jnp.full((WINDOW, 1), sink_ref[head], f32)
                top = jnp.maximum(jnp.max(scores, axis=-1, keepdims=True), sink)
                raised = jnp.exp(scores - top)
                total = jnp.sum(raised, axis=-1, keepdims=True) + jnp.exp(sink - top)
                weights = (raised * (1.0 / total)).astype(bf16)
                part = jnp.dot(weights, vals[side], preferred_element_type=f32)
                out = part if out is None else out + part
                stats = jnp.where(stat_lane == head, top + jnp.log(total), stats)
            attended[pl.ds(base, WINDOW), cols] = out
        log_ref[:, pl.ds(base, WINDOW)] = jnp.transpose(stats)[:heads]

    def attend_range(first, last):
        @pl.loop(first, last)
        def _(b):
            attend(b, band)

    cut = [1 + (n - 1) * i // 3 for i in range(4)]
    mid = 1 + (blocks - 1) // 2
    attend_range(1, mid)
    pass_on(CONV, cut[0], cut[1])
    attend_range(mid, blocks)
    pass_on(CONV, cut[1], cut[2])

    @pl.when(has_left)
    def _():
        halo(kv, WINDOW, 0).wait_recv()

    attend(0, band & ((key_idx >= WINDOW) | has_left))
    pass_on(CONV, cut[2], cut[3])

    def store_conv(base, value):
        conv_in[pl.ds(base + PAD, tile), :] = value.astype(bf16).astype(f32)

    project(CONV, store_conv)
    early = min(2, n - 1)
    pass_on(GATE, 1, early)

    @pl.when(has_right)
    def _():
        halo(conv_in, PAD, 1).start()

    pass_on(GATE, early, n - 1)

    far = jnp.where(2 * me >= n, 0, n - 1)

    def gate_part(base, shard):
        at = pl.ds(pl.multiple_of(shard * depth, depth), depth)
        return jnp.dot(
            normed[pl.ds(base, tile), at], cg_all[at, :], preferred_element_type=f32
        )

    if flip:

        @pl.loop(0, rows // tile)
        def _(i):
            base = pl.multiple_of(i * tile, tile)
            part = gate_part(base, lax.rem(far + 1, n))
            for j in range(2, n):
                part = part + gate_part(base, lax.rem(far + j, n))
            gate_sum[pl.ds(base, tile), :] = part

    pass_on(GATE, n - 1, n)

    @pl.when(has_left)
    def _():
        halo(conv_in, PAD, 1).wait_recv()

    def store_mixed(base, value):
        gate = value.astype(bf16).astype(f32)
        taps = taps_ref[...].astype(f32)
        near = conv_in[pl.ds(base, tile + PAD), :]
        total = jnp.zeros_like(gate)
        for k in range(TAPS):
            start = PAD - TAPS + 1 + k
            total = total + taps[k : k + 1] * near[start : start + tile]
        mixed_ref[pl.ds(base, tile), :] = (attended[pl.ds(base, tile), :] + gate * total).astype(bf16)

    if flip:

        @pl.loop(0, rows // tile)
        def _(i):
            base = pl.multiple_of(i * tile, tile)
            store_mixed(base, gate_sum[pl.ds(base, tile), :] + gate_part(base, far))

    else:
        project(GATE, store_mixed)

    @pl.when(has_right)
    def _():
        halo(kv, WINDOW, 0).wait_send()
        halo(conv_in, PAD, 1).wait_send()

    for a in range(arrays):

        @pl.when(has_right)
        def _():
            @pl.loop(0, me + 1)
            def _(s):
                hop(a, s, True).wait_send()

        @pl.when(has_left)
        def _():
            @pl.loop(me, n)
            def _(s):
                hop(a, s, False).wait_send()


def write_out(mixed_ref, log_ref, mixed_out, log_out, sems):
    copies = [
        pltpu.make_async_copy(mixed_ref, mixed_out, sems.at[0]),
        pltpu.make_async_copy(log_ref, log_out, sems.at[1]),
    ]
    for copy in copies:
        copy.start()
    for copy in copies:
        copy.wait()


def paired_kernel(tok_ref, gain_in, *refs):
    shards = refs[:5]
    (
        taps_in, sink_in, mixed_ref, log_ref, gain_ref, taps_ref, sink_ref,
        tok, normed, other, kv_all, q_all, stage, conv_w, kv, query, q_part, attended,
        conv_in, convolved, sums, conv_out, conv_back, turned_taps, edge_out, edge_in,
        tok_sem, own_sem, recv_sem, sent_sem, halo_recv, x_recv, twin_recv, out_recv,
    ) = refs[5:]
    f32, bf16 = jnp.float32, jnp.bfloat16
    me, fs, tp = lax.axis_index("sp"), lax.axis_index("fs"), lax.axis_index("tp")
    low = me < 2
    end = (me == 0) | (me == 3)
    middle = jnp.logical_not(end)
    mate = me + 1 - 2 * lax.rem(me, 2)
    peer = jnp.where(end, 3 - mate, 3 - me)
    far = jnp.where(low, 3, 0)
    first = jnp.where(low, 0, 1)
    has_left, has_right = me > 0, me < 3
    right = jnp.minimum(me + 1, 3)
    across, along = fs + 1 - 2 * lax.rem(fs, 2), lax.rem(fs + 2, 4)
    diagonal = 3 - fs
    twin = 1 - tp
    rows = tok.shape[0]
    depth = shards[2].shape[0]
    blocks = rows // WINDOW
    width = q_all.shape[1]
    widths = (width // 4, width // 4, width * 5 // 16, width // 8, width // 16)
    groups = range(len(widths))
    channel = [sum(widths[:g]) for g in groups]
    K, V, Q, R, A, B, C, D, E = units = range(9)

    parts = 8
    part_rows = rows // parts
    pieces = 4
    piece = part_rows // pieces
    own_part = fs * 2 + tp

    def part_at(i):
        return lax.rem(own_part + i, parts)

    def rows_of(start, length):
        return pl.ds(pl.multiple_of(start, 16), length)

    tok_copies = []
    for i in range(parts):
        at = rows_of(part_at(i) * part_rows, part_rows)
        tok_copies.append(pltpu.make_async_copy(tok_ref.at[at], tok.at[at], tok_sem.at[min(i, 1)]))

    def shard_at(shard):
        return pl.ds(pl.multiple_of(shard * depth, depth), depth)

    def place(u, shard):
        at = shard_at(shard)
        if u < Q:
            return kv_all.at[pl.ds(u * HEAD_DIM, HEAD_DIM), at]
        if u < A:
            return q_all.at[at, pl.ds((u - Q) * LANES, LANES)]
        return conv_w.at[pl.ds(2 * channel[u - A], 2 * widths[u - A]), at]

    own_copies = [pltpu.make_async_copy(shards[u], place(u, me), own_sem.at[0]) for u in (K, V)]
    own_copies.append(pltpu.make_async_copy(shards[2], q_all.at[shard_at(me)], own_sem.at[1]))
    own_copies += [pltpu.make_async_copy(shards[3 + j], stage.at[j], own_sem.at[2]) for j in range(2)]
    small_copies = [
        pltpu.make_async_copy(src, dst, own_sem.at[3 + j])
        for j, (src, dst) in enumerate(((gain_in, gain_ref), (taps_in, taps_ref), (sink_in, sink_ref)))
    ]
    for copy in small_copies[:1] + tok_copies[:1] + own_copies + small_copies[1:] + tok_copies[1:]:
        copy.start()

    def norm_part(i):
        norm_rows = 64

        @pl.loop(0, part_rows // norm_rows)
        def _(j):
            at = rows_of(part_at(i) * part_rows + j * norm_rows, norm_rows)
            wide = tok[at, :].astype(f32)
            scale = lax.rsqrt(jnp.mean(wide * wide, axis=-1, keepdims=True) + EPS)
            normed[at, :] = (wide * scale * gain_ref[...]).astype(bf16)

    barrier = pltpu.get_barrier_semaphore()

    def greet(**device):
        pl.semaphore_signal(barrier, inc=1, device_id=device, device_id_type=MESH)

    greet(sp=mate)

    @pl.when(middle)
    def _():
        greet(sp=peer)
        greet(fs=across)
        greet(fs=along)
        greet(tp=twin)


    TO_MATE, TO_PEER, RELAYED, RETURNED, EDGES, HALO = range(6)

    def slot(shard, device):
        return shard - jnp.where(shard > device, 1, 0)

    def source(u):
        return shards[u] if u < Q else shards[2].at[:, pl.ds((u - Q) * LANES, LANES)]

    def hop(u, shard, to_mate):
        target = mate if to_mate else peer
        return pltpu.make_async_remote_copy(
            src_ref=source(u) if shard is me and u < A else place(u, shard),
            dst_ref=place(u, shard),
            send_sem=sent_sem.at[TO_MATE if to_mate else TO_PEER],
            recv_sem=recv_sem.at[u, slot(shard, target)],
            device_id={"sp": target},
            device_id_type=MESH,
        )

    def arrived(u, shard):
        ref = place(u, shard)
        pltpu.make_async_copy(ref, ref, recv_sem.at[u, slot(shard, me)]).wait()

    def drain(kind, elements):
        ref = other.at[pl.ds(0, elements // other.shape[1])]
        pltpu.make_async_copy(ref, ref, sent_sem.at[kind]).wait()

    def piece_at(part, h):
        return rows_of(part * part_rows + h * piece, piece)

    def piece_copy(buffer, part, h, kind, arrival, **device):
        at = piece_at(part, h)
        return pltpu.make_async_remote_copy(
            src_ref=buffer.at[at],
            dst_ref=other.at[at],
            send_sem=sent_sem.at[kind],
            recv_sem=arrival,
            device_id=device,
            device_id_type=MESH,
        )

    def line_sem(part, h):
        return x_recv.at[part // 2, h]

    def piece_arrived(part, h):
        ref = other.at[piece_at(part, h)]
        pltpu.make_async_copy(ref, ref, line_sem(part, h)).wait()

    across_part, along_part, diagonal_part = across * 2 + tp, along * 2 + tp, diagonal * 2 + tp
    relays = [(own_part, h, ("tp", "fs_across", "fs_along")) for h in range(pieces)]
    relays += [(across_part, h, ("tp", "fs_along")[: 2 - h % 2]) for h in range(pieces)]
    relays += [(along_part, h, ("tp", "fs_across")[: 1 + h % 2]) for h in range(pieces)]
    relays += [(diagonal_part, h, ("tp",)) for h in range(pieces)]
    OWN_X, ACROSS, ALONG, DIAGONAL = (pieces * j for j in range(4))
    devices = {"tp": {"tp": twin}, "fs_across": {"fs": across}, "fs_along": {"fs": along}}

    def relay_copies(j):
        part, h, to = relays[j]
        return [
            piece_copy(other, part, h, RELAYED, twin_recv.at[0] if d == "tp" else line_sem(part, h), **devices[d])
            for d in to
        ]

    def relay(*which):
        for j in which:
            piece_arrived(relays[j][0], relays[j][1])
            for copy in relay_copies(j):
                copy.start()

    def send(to_mate, shard, *which):
        for u in which:
            hop(u, shard, to_mate).start()

    def forward(to_mate, shard, *which):
        for u in which:
            arrived(u, shard)
            hop(u, shard, to_mate).start()

    def pieces_out(*which):
        for h in which:
            piece_copy(normed, own_part, h, RELAYED, line_sem(own_part, h), sp=mate).start()

    pl.semaphore_wait(barrier, jnp.where(middle, 5, 1))

    @pl.when(middle)
    def _():
        send(False, me, K, V, Q, R)
        send(True, me, K, V, Q, R)

    small_copies[0].wait()
    tok_copies[0].wait()
    norm_part(0)

    @pl.when(end)
    def _():
        pieces_out(*range(pieces))
        send(True, me, K, V, Q, R)

    pltpu.make_async_copy(stage, stage, own_sem.at[2]).wait()
    for j in range(2):
        for block in range(depth // LANES):
            turned = jnp.transpose(stage[j, pl.ds(block * LANES, LANES), :].astype(f32)).astype(bf16)
            at = pl.ds(pl.multiple_of(me * depth + block * LANES, LANES), LANES)
            for g in groups:
                to = pl.ds(2 * channel[g] + j * widths[g], widths[g])
                conv_w[to, at] = turned[channel[g] : channel[g] + widths[g]]
    small_copies[1].wait()
    small_copies[2].wait()
    taps = taps_ref[...].astype(f32)
    turned_taps[...] = jnp.transpose(jnp.concatenate([taps, jnp.zeros((8 - TAPS, width), f32)], axis=0))
    conv_in[:, pl.ds(0, LANES)] = jnp.zeros((width, LANES), f32)

    @pl.when(end)
    def _():
        send(True, me, A, B, C)

    @pl.when(middle)
    def _():
        send(False, me, A, B, C)

    own_kv = kv_all.at[:, shard_at(me)]
    pltpu.make_async_copy(own_kv, own_kv, own_sem.at[0]).wait()
    own_copies[2].wait()

    others = tok.at[pl.ds(0, rows - part_rows)]
    pltpu.make_async_copy(others, others, tok_sem.at[1]).wait()
    for i in range(1, parts):
        norm_part(i)

    tile = 512

    early = pl.ds(pl.multiple_of(first * depth, depth), 3 * depth)
    late = pl.ds(pl.multiple_of(far * depth, depth), depth)

    kv_halo = pltpu.make_async_remote_copy(
        src_ref=kv.at[pl.ds(rows, WINDOW)],
        dst_ref=kv.at[pl.ds(0, WINDOW)],
        send_sem=sent_sem.at[HALO],
        recv_sem=halo_recv.at[0],
        device_id={"sp": right},
        device_id_type=MESH,
    )

    own_base, mate_base = jnp.where(me == 1, rows, 0), jnp.where(me == 1, 0, rows)
    bases = (own_base, mate_base)
    sources = (normed, other)
    tiles = rows // tile
    OWN, MATE = 0, 1

    def tile_at(i):
        return pl.ds(i * tile if isinstance(i, int) else pl.multiple_of(i * tile, tile), tile)

    def out_copy(g, i):
        at = (pl.ds(channel[g], widths[g]), tile_at(i))
        return pltpu.make_async_remote_copy(
            src_ref=conv_out.at[at],
            dst_ref=conv_back.at[at],
            send_sem=sent_sem.at[RETURNED],
            recv_sem=out_recv.at[channel[g] // LANES * tiles + i],
            device_id={"sp": mate},
            device_id_type=MESH,
        )

    def edge_copy(g):
        return pltpu.make_async_remote_copy(
            src_ref=edge_out.at[g],
            dst_ref=edge_in.at[g],
            send_sem=sent_sem.at[EDGES],
            recv_sem=halo_recv.at[1],
            device_id={"sp": right},
            device_id_type=MESH,
        )

    center = pl.ds(depth, 2 * depth)
    everything = pl.ds(0, conv_w.shape[1])
    edge_tokens = pl.ds(rows - LANES, LANES)

    def dot(which, tokens, start, length, at):
        return lax.dot_general(
            conv_w[pl.ds(start, length), at],
            sources[which][tokens, at],
            (((1,), (1,)), ((), ())),
            preferred_element_type=f32,
        )

    def partial(which, i, u, v, at, fresh=False):
        start = 2 * channel[u - A]
        span = pl.ds(start, 2 * channel[v - A] + 2 * widths[v - A] - start)
        value = dot(which, tile_at(i), span.start, span.size, at)
        sums[which, span, tile_at(i)] = value if fresh else sums[which, span, tile_at(i)] + value

    def product(which, tokens, start, length):
        if which == OWN and start >= 2 * channel[3] and tokens is not edge_tokens:
            return dot(which, tokens, start, length, everything)
        return sums[which, pl.ds(start, length), tokens] + dot(which, tokens, start, length, late)

    def keep(g, at, value):
        value = value.astype(bf16).astype(f32)
        conv_in[pl.ds(channel[g], widths[g]), pl.ds(pl.multiple_of(at + LANES, LANES), value.shape[1])] = value[: widths[g]]
        return value[widths[g] :]

    def convolve(g, at, gate):
        of = pl.ds(channel[g], widths[g])
        near = conv_in[of, pl.ds(pl.multiple_of(at, LANES), tile + LANES)]
        total = jnp.zeros((widths[g], tile), f32)
        for k in range(TAPS):
            moved = near if k == TAPS - 1 else pltpu.roll(near, TAPS - 1 - k, 1)
            total = total + turned_taps[of, k : k + 1] * moved[:, LANES:]
        return gate * total

    def mate_tiles(g):
        of = pl.ds(channel[g], widths[g])
        keep(g, own_base + rows - LANES, product(OWN, edge_tokens, 2 * channel[g], 2 * widths[g]))
        for i in range(tiles):
            at = mate_base + i * tile
            value = product(MATE, tile_at(i), 2 * channel[g], 2 * widths[g])
            conv_out[of, tile_at(i)] = convolve(g, at, keep(g, at, value)).astype(bf16)
            out_copy(g, i).start()

        @pl.when(me == 1)
        def _():
            edge = jnp.transpose(conv_in[of, pl.ds(2 * rows, LANES)])
            edge_out[g, :, pl.ds(0, widths[g])] = edge[LANES - PAD :]
            edge_copy(g).start()

    def own_tiles(*which):
        @pl.when(me == 2)
        def _():
            for g in which:
                of = pl.ds(channel[g], widths[g])
                edge = edge_in[g, :, pl.ds(0, widths[g])]
                edge = jnp.concatenate([jnp.zeros((LANES - PAD, widths[g]), f32), edge], axis=0)
                conv_in[of, pl.ds(0, LANES)] = jnp.transpose(edge)

        start = 2 * channel[which[0]]
        length = sum(2 * widths[g] for g in which)
        for i in range(tiles):
            at = own_base + i * tile
            value = product(OWN, tile_at(i), start, length)
            for g in which:
                row = 2 * channel[g] - start
                gate = keep(g, at, value[row : row + 2 * widths[g]])
                convolved[pl.ds(channel[g], widths[g]), tile_at(i)] = convolve(g, at, gate)

    def mix(half, i, source):
        cols = pl.ds(half * LANES, LANES)
        for j in range(tile // LANES):
            at = pl.ds(i * tile + j * LANES, LANES)
            extra = jnp.transpose(source[cols, at].astype(f32))
            mixed_ref[at, cols] = (attended[at, cols] + extra).astype(bf16)

    @pl.when(middle)
    def _():
        relay(OWN_X)
        forward(True, peer, K, V)
        relay(OWN_X + 1)
        forward(True, peer, Q)
        relay(ACROSS, ALONG)
        forward(True, peer, R)
        relay(OWN_X + 2, ACROSS + 1, ALONG + 1, OWN_X + 3)
        forward(False, mate, K, V)
        relay(ACROSS + 2, ALONG + 2)
        forward(False, mate, Q)
        relay(DIAGONAL, DIAGONAL + 1)
        forward(False, mate, R)
        for u in (A, B, C):
            arrived(u, peer)
        partial(OWN, 0, A, C, center, True)
        relay(ACROSS + 3, ALONG + 3)
        forward(True, far, K, V)
        forward(False, mate, A)

    @pl.when(end)
    def _():
        for shard in (mate, peer, far):
            for u in (K, V):
                arrived(u, shard)

    @pl.loop(0, rows // tile)
    def _(i):
        base = pl.multiple_of(i * tile, tile)
        kv[pl.ds(base + WINDOW, tile), :] = lax.dot_general(
            normed[pl.ds(base, tile), :], kv_all[...], (((1,), (1,)), ((), ())), preferred_element_type=f32
        ).astype(bf16)

    @pl.when(jnp.logical_not(has_left))
    def _():
        kv[pl.ds(0, WINDOW), :] = jnp.zeros((WINDOW, kv.shape[1]), bf16)

    @pl.when(has_right)
    def _():
        kv_halo.start()

    @pl.when(middle)
    def _():
        forward(True, far, Q)
        partial(OWN, 1, A, C, center, True)
        forward(False, mate, B)

    @pl.when(end)
    def _():
        send(True, me, D, E)
        for u in (Q, R):
            arrived(u, mate)
            arrived(u, peer)

    @pl.loop(0, rows // tile)
    def _(i):
        at = pl.ds(pl.multiple_of(i * tile, tile), tile)
        q_part[at, :] = jnp.dot(normed[at, early], q_all[early, :], preferred_element_type=f32)

    @pl.when(middle)
    def _():
        forward(True, far, R)

    @pl.when(end)
    def _():
        arrived(Q, far)
        arrived(R, far)

    @pl.loop(0, rows // tile)
    def _(i):
        at = pl.ds(pl.multiple_of(i * tile, tile), tile)
        query[at, :] = (
            q_part[at, :] + jnp.dot(normed[at, late], q_all[late, :], preferred_element_type=f32)
        ).astype(bf16)

    heads = query.shape[1] // HEAD_DIM
    query_idx = lax.broadcasted_iota(jnp.int32, (WINDOW, 2 * WINDOW), 0)
    key_idx = lax.broadcasted_iota(jnp.int32, (WINDOW, 2 * WINDOW), 1)
    gap = query_idx + WINDOW - key_idx
    band = (gap >= 0) & (gap < WINDOW)
    low_lanes = lax.broadcasted_iota(jnp.int32, (2 * WINDOW, LANES), 1) < HEAD_DIM
    lane = lax.broadcasted_iota(jnp.int32, (WINDOW, LANES), 1)
    low_half = lane < HEAD_DIM

    def attend(b, kept):
        base = pl.multiple_of(b * WINDOW, WINDOW)
        both = kv[pl.ds(base, 2 * WINDOW), :].astype(f32)
        turned = pltpu.roll(both, HEAD_DIM, 1)
        zero, one = jnp.zeros_like(both), jnp.ones_like(both)

        def lower(x):
            return jnp.where(low_lanes, x, zero)

        def upper(x):
            return jnp.where(low_lanes, zero, x)

        keys = jnp.concatenate([lower(both), upper(turned)], axis=0).astype(bf16)
        vals = jnp.concatenate([lower(turned), upper(both)], axis=0)
        ones = jnp.concatenate([lower(one), upper(one)], axis=0)
        vals = jnp.concatenate([vals, ones], axis=1).astype(bf16)
        stats = []
        for pair in range(heads // 2):
            cols = pl.ds(pair * LANES, LANES)
            scores = lax.dot_general(
                query[pl.ds(base, WINDOW), cols], keys, (((1,), (1,)), ((), ())), preferred_element_type=f32
            )
            sinks = [sink_ref[2 * pair + side] * LOG2_E for side in range(2)]
            tops, raised = [], []
            for side in range(2):
                part = scores[:, side * 2 * WINDOW : (side + 1) * 2 * WINDOW] * (HEAD_DIM ** (-0.5) * LOG2_E)
                part = jnp.where(kept, part, -jnp.inf)
                tops.append(jnp.maximum(jnp.max(part, axis=-1, keepdims=True), sinks[side]))
                raised.append(jnp.exp2(part - tops[side]).astype(bf16))
            out = jnp.dot(jnp.concatenate(raised, axis=1), vals, preferred_element_type=f32)
            top = jnp.where(low_half, tops[0], tops[1])
            total = out[:, LANES:] + jnp.exp2(jnp.where(low_half, sinks[0], sinks[1]) - top)
            attended[pl.ds(base, WINDOW), cols] = out[:, :LANES] / total
            stats.append(top * LN_2 + jnp.log(total))
        turned_stats = jnp.transpose(jnp.where(lax.rem(lane, 2) == 0, stats[0], stats[1]))
        for pair in range(2):
            for side in range(2):
                row = pair + side * HEAD_DIM
                head = 2 * pair + side
                log_ref[head : head + 1, pl.ds(base, WINDOW)] = turned_stats[row : row + 1]

    def finish(g):
        arrived(A + g, far)
        mate_tiles(g)

    @pl.when(middle)
    def _():
        relay(DIAGONAL + 2, DIAGONAL + 3)
        half_rows = other.at[pl.ds(0, rows // 2)]
        pltpu.make_async_copy(half_rows, half_rows, twin_recv.at[0]).wait()
        for i in range(tiles):
            partial(MATE, i, A, C, center, True)
        forward(False, mate, C)
        send(False, me, D, E)
        for i in range(tiles):
            partial(MATE, i, A, B, shard_at(mate))
        partial(OWN, tiles - 1, A, B, shard_at(mate))
        finish(0)
        for i in range(tiles - 1):
            partial(OWN, i, A, B, shard_at(mate))

    def attend_pairs(start, stop):
        @pl.loop(start, stop)
        def _(j):
            attend(2 * j + 1, band)
            attend(2 * j + 2, band)

    cut = (blocks // 2 - 1) * 2 // 3
    attend_pairs(0, cut)

    @pl.when(middle)
    def _():
        forward(False, mate, D, E)
        finish(1)

    attend_pairs(cut, blocks // 2 - 1)

    @pl.when(has_left)
    def _():
        kv_halo.wait_recv()

    @pl.when(middle)
    def _():
        for i in range(tiles):
            partial(MATE, i, C, C, shard_at(mate))
        partial(OWN, tiles - 1, C, C, shard_at(mate))
        finish(2)
        arrived(D, peer)
        arrived(E, peer)
        for i in range(tiles):
            partial(MATE, i, D, E, early, True)
        late_rows = pl.ds(2 * channel[3], 2 * (widths[3] + widths[4]))
        sums[OWN, late_rows, edge_tokens] = dot(OWN, edge_tokens, late_rows.start, late_rows.size, early)
        finish(3)
        finish(4)
        for i in range(tiles - 1):
            partial(OWN, i, C, C, shard_at(mate))

    attend(blocks - 1, band)
    attend(0, band & ((key_idx >= WINDOW) | has_left))

    @pl.when(middle)
    def _():
        @pl.when(me == 2)
        def _():
            pltpu.make_async_copy(edge_in, edge_in, halo_recv.at[1]).wait()

        own_tiles(0, 1)
        own_tiles(2)
        own_tiles(3, 4)
        for half in range(2):
            for i in range(tiles):
                mix(half, i, convolved)

    @pl.when(end)
    def _():
        for half in range(2):
            for i in range(tiles):
                back = conv_back.at[pl.ds(half * LANES, LANES), tile_at(i)]
                pltpu.make_async_copy(back, back, out_recv.at[half * tiles + i]).wait()
                mix(half, i, conv_back)

    @pl.when(has_right)
    def _():
        kv_halo.wait_send()

    attention_shard = depth * (2 * HEAD_DIM + width)
    whole_shard = attention_shard + depth * 2 * width

    @pl.when(end)
    def _():
        drain(TO_MATE, whole_shard)
        drain(RELAYED, part_rows * other.shape[1])

    @pl.when(middle)
    def _():
        drain(TO_MATE, 3 * attention_shard)
        drain(TO_PEER, 2 * whole_shard)
        drain(RELAYED, sum(len(to) for _, _, to in relays) * piece * other.shape[1])
        pltpu.make_async_copy(conv_out, conv_out, sent_sem.at[RETURNED]).wait()

        @pl.when(me == 1)
        def _():
            pltpu.make_async_copy(edge_out, edge_out, sent_sem.at[EDGES]).wait()


def paired_body(tokens, norm_gain, w_query, w_key, w_value, w_conv_in, w_conv_gate, conv_taps, sink_logits):
    rows, features = tokens.shape
    width = w_query.shape[1]
    f32, bf16 = jnp.float32, jnp.bfloat16
    hbm = pl.BlockSpec(memory_space=pltpu.HBM)
    vmem = pl.BlockSpec(memory_space=pltpu.VMEM)
    dma = pltpu.SemaphoreType.DMA
    tiles = rows // 512
    results = pl.pallas_call(
        paired_kernel,
        out_shape=(
            pltpu.VMEM((rows, width), bf16),
            pltpu.VMEM((width // HEAD_DIM, rows), f32),
        ),
        in_specs=[hbm] * 9,
        out_specs=(vmem, vmem),
        scratch_shapes=[
            pltpu.VMEM((1, features), f32),
            pltpu.VMEM(conv_taps.shape, bf16),
            pltpu.SMEM((width // HEAD_DIM,), f32),
            pltpu.VMEM((rows, features), bf16),
            pltpu.VMEM((rows, features), bf16),
            pltpu.VMEM((rows, features), bf16),
            pltpu.VMEM((2 * HEAD_DIM, features), bf16),
            pltpu.VMEM((features, width), bf16),
            pltpu.VMEM((2, w_query.shape[0], width), bf16),
            pltpu.VMEM((2 * width, features), bf16),
            pltpu.VMEM((rows + WINDOW, 2 * HEAD_DIM), bf16),
            pltpu.VMEM((rows, width), bf16),
            pltpu.VMEM((rows, width), f32),
            pltpu.VMEM((rows, width), f32),
            pltpu.VMEM((width, LANES + 2 * rows), f32),
            pltpu.VMEM((width, rows), f32),
            pltpu.VMEM((2, 2 * width, rows), f32),
            pltpu.VMEM((width, rows), bf16),
            pltpu.VMEM((width, rows), bf16),
            pltpu.VMEM((width, 8), f32),
            pltpu.VMEM((5, PAD, LANES), f32),
            pltpu.VMEM((5, PAD, LANES), f32),
            dma((2,)),
            dma((6,)),
            dma((9, 3)),
            dma((6,)),
            dma((2,)),
            dma((4, 4)),
            dma((1,)),
            dma((2 * tiles,)),
        ],
        compiler_params=pltpu.CompilerParams(
            collective_id=0, has_side_effects=True, vmem_limit_bytes=59 << 20
        ),
        name="paired_attend_convolve",
    )(tokens, norm_gain.reshape(1, -1), w_key.T, w_value.T, w_query, w_conv_in, w_conv_gate, conv_taps, sink_logits)
    return pl.pallas_call(
        write_out,
        out_shape=(
            jax.ShapeDtypeStruct((rows, width), bf16),
            jax.ShapeDtypeStruct((width // HEAD_DIM, rows), f32),
        ),
        in_specs=[vmem, vmem],
        out_specs=(hbm, hbm),
        scratch_shapes=[dma((2,))],
        name="write_out",
    )(*[pltpu.with_memory_space_constraint(result, pltpu.VMEM) for result in results])


def line_body(n, tokens, norm_gain, w_query, w_key, w_value, w_conv_in, w_conv_gate, conv_taps, sink_logits):
    rows, features = tokens.shape
    width, kv_width = w_query.shape[1], w_key.shape[1] + w_value.shape[1]
    assert w_key.shape[1] == HEAD_DIM and width % LANES == 0
    depth = w_query.shape[0]
    flip = depth % LANES == 0 and 2 < n <= 16
    if flip:
        w_kv, kv_shape = (w_key.T, w_value.T), (kv_width, features)
    else:
        w_kv, kv_shape = (jnp.concatenate([w_key, w_value], axis=1),), (features, kv_width)
    arrays = 3 + len(w_kv)
    f32, bf16 = jnp.float32, jnp.bfloat16
    hbm = pl.BlockSpec(memory_space=pltpu.HBM)
    vmem = pl.BlockSpec(memory_space=pltpu.VMEM)
    smem = pl.BlockSpec(memory_space=pltpu.SMEM)
    dma = pltpu.SemaphoreType.DMA
    return pl.pallas_call(
        functools.partial(line_kernel, n, flip),
        out_shape=(
            pltpu.VMEM((rows, width), bf16),
            pltpu.VMEM((width // HEAD_DIM, rows), f32),
        ),
        in_specs=[hbm, vmem] + [hbm] * arrays + [vmem, smem],
        out_specs=(vmem, vmem),
        scratch_shapes=[
            pltpu.VMEM((rows, features), bf16),
            pltpu.VMEM((rows, features), bf16),
            pltpu.VMEM(kv_shape, bf16),
            pltpu.VMEM((features, width), bf16),
            pltpu.VMEM((features, width), bf16),
            pltpu.VMEM((features, width), bf16),
            pltpu.VMEM((rows + WINDOW, kv_width), bf16),
            pltpu.VMEM((rows, width), bf16),
            pltpu.VMEM((rows, width), f32),
            pltpu.VMEM((rows + PAD, width), f32),
            pltpu.VMEM((rows, width), f32),
            dma((4,)),
            dma((arrays,)),
            dma((arrays, n)),
            dma((arrays, n)),
            dma((arrays, n)),
            dma((2,)),
            dma((2,)),
        ],
        compiler_params=pltpu.CompilerParams(
            collective_id=0, has_side_effects=True, vmem_limit_bytes=59 << 20
        ),
        name="gather_attend_convolve",
    )(tokens, norm_gain.reshape(1, -1), *w_kv, w_query, w_conv_in, w_conv_gate, conv_taps, sink_logits)


def body(n, fs, tp, *arrays):
    rows, width, depth = arrays[0].shape[0], arrays[2].shape[1], arrays[2].shape[0]
    square = n == 4 and fs == 4 and tp == 2
    if square and width == 2 * LANES and depth % LANES == 0 and rows % (8 * LANES) == 0:
        return paired_body(*arrays)
    return line_body(n, *arrays)


def solution(mesh):
    return jax.shard_map(
        functools.partial(body, mesh.shape["sp"], mesh.shape["fs"], mesh.shape["tp"]),
        mesh=mesh,
        in_specs=(
            P("sp", None),
            P(),
            P("sp", ("fs", "tp")),
            P("sp", ("fs", "tp")),
            P("sp", ("fs", "tp")),
            P("sp", ("fs", "tp")),
            P("sp", ("fs", "tp")),
            P(None, ("fs", "tp")),
            P(("fs", "tp")),
        ),
        out_specs=(P("sp", ("fs", "tp")), P(("fs", "tp"), "sp")),
        check_vma=False,
    )
```

```python
import functools
import math

import jax
import jax.numpy as jnp
from jax import lax
from jax.experimental import pallas as pl
from jax.experimental.pallas import tpu as pltpu
from jax.sharding import PartitionSpec as P

HEAD_DIM = 64
WINDOW = 128
TAPS = 3
EPS = 1e-06
LANES = 128
PAD = 8
LOG2_E = math.log2(math.e)
LN_2 = math.log(2)
MESH = pl.DeviceIdType.MESH


def line_kernel(
    n, flip, tok_ref, gain_ref, *refs
):
    arrays = 5 if flip else 4
    shards = refs[:arrays]
    (
        taps_ref, sink_ref, mixed_ref, log_ref,
        tok, normed, kv_all, q_all, ci_all, cg_all, kv, query, attended, conv_in, gate_sum,
        tok_sem, own_sem, recv_sem, right_sem, left_sem, halo_send, halo_recv,
    ) = refs[arrays:]
    QUERY, CONV, GATE = arrays - 3, arrays - 2, arrays - 1
    me = lax.axis_index("sp")
    rows = tok.shape[0]
    depth = shards[QUERY].shape[0]
    wholes = (kv_all, kv_all, q_all, ci_all, cg_all)[5 - arrays :]
    has_left, has_right = me > 0, me < n - 1
    left, right = jnp.maximum(me - 1, 0), jnp.minimum(me + 1, n - 1)
    blocks = rows // WINDOW
    f32, bf16 = jnp.float32, jnp.bfloat16

    step_rows = rows // 4
    tok_copies = [
        pltpu.make_async_copy(
            tok_ref.at[pl.ds(i * step_rows, step_rows)], tok.at[pl.ds(i * step_rows, step_rows)], tok_sem.at[i]
        )
        for i in range(4)
    ]
    for copy in tok_copies:
        copy.start()

    def place(a, shard):
        at = pl.ds(pl.multiple_of(shard * depth, depth), depth)
        if flip and a < QUERY:
            return kv_all.at[pl.ds(a * HEAD_DIM, HEAD_DIM), at]
        return wholes[a].at[at]

    own_copies = [pltpu.make_async_copy(shards[a], place(a, me), own_sem.at[a]) for a in range(arrays)]
    for copy in own_copies:
        copy.start()

    barrier = pltpu.get_barrier_semaphore()

    @pl.when(has_left)
    def _():
        pl.semaphore_signal(barrier, inc=1, device_id={"sp": left}, device_id_type=MESH)

    @pl.when(has_right)
    def _():
        pl.semaphore_signal(barrier, inc=1, device_id={"sp": right}, device_id_type=MESH)

    pl.semaphore_wait(barrier, has_left.astype(jnp.int32) + has_right.astype(jnp.int32))

    def hop(a, shard, to_right, own=False):
        return pltpu.make_async_remote_copy(
            src_ref=shards[a] if own else place(a, shard),
            dst_ref=place(a, shard),
            send_sem=(right_sem if to_right else left_sem).at[a, shard],
            recv_sem=recv_sem.at[a, shard],
            device_id={"sp": right if to_right else left},
            device_id_type=MESH,
        )

    def send_own(a):
        @pl.when(has_right)
        def _():
            hop(a, me, True, True).start()

        @pl.when(has_left)
        def _():
            hop(a, me, False, True).start()

    def pass_on(a, first, last):
        def step(k, carry):
            @pl.when(me - k >= 0)
            def _():
                shard = me - k
                hop(a, shard, False).wait_recv()

                @pl.when(has_right)
                def _():
                    hop(a, shard, True).start()

            @pl.when(me + k < n)
            def _():
                shard = me + k
                hop(a, shard, True).wait_recv()

                @pl.when(has_left)
                def _():
                    hop(a, shard, False).start()

            return carry

        lax.fori_loop(first, last, step, 0)

    for a in range(GATE):
        send_own(a)

    norm_rows = 64
    for i in range(4):
        tok_copies[i].wait()

        @pl.loop(0, step_rows // norm_rows)
        def _(j):
            at = pl.ds(pl.multiple_of(i * step_rows + j * norm_rows, norm_rows), norm_rows)
            wide = tok[at, :].astype(f32)
            scale = lax.rsqrt(jnp.mean(wide * wide, axis=-1, keepdims=True) + EPS)
            normed[at, :] = (wide * scale * gain_ref[...]).astype(bf16)

    for copy in own_copies:
        copy.wait()

    tile = 256

    def project(a, store):
        @pl.loop(0, rows // tile)
        def _(i):
            base = pl.multiple_of(i * tile, tile)
            side = 1 if flip and a < QUERY else 0
            store(
                base,
                lax.dot_general(
                    normed[pl.ds(base, tile), :],
                    wholes[a][...],
                    (((1,), (side,)), ((), ())),
                    preferred_element_type=f32,
                ),
            )

    def halo(buffer, length, i):
        return pltpu.make_async_remote_copy(
            src_ref=buffer.at[pl.ds(rows, length)],
            dst_ref=buffer.at[pl.ds(0, length)],
            send_sem=halo_send.at[i],
            recv_sem=halo_recv.at[i],
            device_id={"sp": right},
            device_id_type=MESH,
        )

    for a in range(QUERY):
        pass_on(a, 1, n)
    send_own(GATE)

    def store_kv(base, value):
        kv[pl.ds(base + WINDOW, tile), :] = value.astype(bf16)

    project(0, store_kv)

    @pl.when(jnp.logical_not(has_left))
    def _():
        kv[pl.ds(0, WINDOW), :] = jnp.zeros((WINDOW, kv.shape[1]), bf16)
        conv_in[pl.ds(0, PAD), :] = jnp.zeros((PAD, conv_in.shape[1]), f32)

    pass_on(QUERY, 1, n)

    @pl.when(has_right)
    def _():
        halo(kv, WINDOW, 0).start()

    def store_query(base, value):
        query[pl.ds(base, tile), :] = value.astype(bf16)

    project(QUERY, store_query)

    heads = query.shape[1] // HEAD_DIM
    query_idx = lax.broadcasted_iota(jnp.int32, (WINDOW, 2 * WINDOW), 0)
    key_idx = lax.broadcasted_iota(jnp.int32, (WINDOW, 2 * WINDOW), 1)
    gap = query_idx + WINDOW - key_idx
    band = (gap >= 0) & (gap < WINDOW)
    lane = lax.broadcasted_iota(jnp.int32, (2 * WINDOW, LANES), 1)
    low = lane < HEAD_DIM
    stat_lane = lax.broadcasted_iota(jnp.int32, (WINDOW, LANES), 1)

    def attend(b, kept):
        base = pl.multiple_of(b * WINDOW, WINDOW)
        both = kv[pl.ds(base, 2 * WINDOW), :].astype(f32)
        turned = pltpu.roll(both, HEAD_DIM, 1)
        zero = jnp.zeros_like(both)
        keys = (jnp.where(low, both, zero).astype(bf16), jnp.where(low, zero, turned).astype(bf16))
        vals = (jnp.where(low, turned, zero).astype(bf16), jnp.where(low, zero, both).astype(bf16))
        stats = jnp.zeros((WINDOW, LANES), f32)
        for pair in range(heads // 2):
            cols = pl.ds(pair * LANES, LANES)
            q = query[pl.ds(base, WINDOW), cols]
            out = None
            for side in range(2):
                head = 2 * pair + side
                scores = lax.dot_general(
                    q, keys[side], (((1,), (1,)), ((), ())), preferred_element_type=f32
                ) * HEAD_DIM ** (-0.5)
                scores = jnp.where(kept, scores, -jnp.inf)
                sink = jnp.full((WINDOW, 1), sink_ref[head], f32)
                top = jnp.maximum(jnp.max(scores, axis=-1, keepdims=True), sink)
                raised = jnp.exp(scores - top)
                total = jnp.sum(raised, axis=-1, keepdims=True) + jnp.exp(sink - top)
                weights = (raised * (1.0 / total)).astype(bf16)
                part = jnp.dot(weights, vals[side], preferred_element_type=f32)
                out = part if out is None else out + part
                stats = jnp.where(stat_lane == head, top + jnp.log(total), stats)
            attended[pl.ds(base, WINDOW), cols] = out
        log_ref[:, pl.ds(base, WINDOW)] = jnp.transpose(stats)[:heads]

    def attend_range(first, last):
        @pl.loop(first, last)
        def _(b):
            attend(b, band)

    cut = [1 + (n - 1) * i // 3 for i in range(4)]
    mid = 1 + (blocks - 1) // 2
    attend_range(1, mid)
    pass_on(CONV, cut[0], cut[1])
    attend_range(mid, blocks)
    pass_on(CONV, cut[1], cut[2])

    @pl.when(has_left)
    def _():
        halo(kv, WINDOW, 0).wait_recv()

    attend(0, band & ((key_idx >= WINDOW) | has_left))
    pass_on(CONV, cut[2], cut[3])

    def store_conv(base, value):
        conv_in[pl.ds(base + PAD, tile), :] = value.astype(bf16).astype(f32)

    project(CONV, store_conv)
    early = min(2, n - 1)
    pass_on(GATE, 1, early)

    @pl.when(has_right)
    def _():
        halo(conv_in, PAD, 1).start()

    pass_on(GATE, early, n - 1)

    far = jnp.where(2 * me >= n, 0, n - 1)

    def gate_part(base, shard):
        at = pl.ds(pl.multiple_of(shard * depth, depth), depth)
        return jnp.dot(
            normed[pl.ds(base, tile), at], cg_all[at, :], preferred_element_type=f32
        )

    if flip:

        @pl.loop(0, rows // tile)
        def _(i):
            base = pl.multiple_of(i * tile, tile)
            part = gate_part(base, lax.rem(far + 1, n))
            for j in range(2, n):
                part = part + gate_part(base, lax.rem(far + j, n))
            gate_sum[pl.ds(base, tile), :] = part

    pass_on(GATE, n - 1, n)

    @pl.when(has_left)
    def _():
        halo(conv_in, PAD, 1).wait_recv()

    def store_mixed(base, value):
        gate = value.astype(bf16).astype(f32)
        taps = taps_ref[...].astype(f32)
        near = conv_in[pl.ds(base, tile + PAD), :]
        total = jnp.zeros_like(gate)
        for k in range(TAPS):
            start = PAD - TAPS + 1 + k
            total = total + taps[k : k + 1] * near[start : start + tile]
        mixed_ref[pl.ds(base, tile), :] = (attended[pl.ds(base, tile), :] + gate * total).astype(bf16)

    if flip:

        @pl.loop(0, rows // tile)
        def _(i):
            base = pl.multiple_of(i * tile, tile)
            store_mixed(base, gate_sum[pl.ds(base, tile), :] + gate_part(base, far))

    else:
        project(GATE, store_mixed)

    @pl.when(has_right)
    def _():
        halo(kv, WINDOW, 0).wait_send()
        halo(conv_in, PAD, 1).wait_send()

    for a in range(arrays):

        @pl.when(has_right)
        def _():
            @pl.loop(0, me + 1)
            def _(s):
                hop(a, s, True).wait_send()

        @pl.when(has_left)
        def _():
            @pl.loop(me, n)
            def _(s):
                hop(a, s, False).wait_send()


def write_out(mixed_ref, log_ref, mixed_out, log_out, sems):
    copies = [
        pltpu.make_async_copy(mixed_ref, mixed_out, sems.at[0]),
        pltpu.make_async_copy(log_ref, log_out, sems.at[1]),
    ]
    for copy in copies:
        copy.start()
    for copy in copies:
        copy.wait()


def paired_kernel(tok_ref, gain_in, *refs):
    shards = refs[:5]
    (
        taps_in, sink_in, mixed_ref, log_ref, gain_ref, taps_ref, sink_ref,
        tok, normed, other, kv_all, q_all, stage, conv_w, kv, query, q_part, attended,
        conv_in, convolved, sums, conv_out, conv_back, turned_taps, edge_out, edge_in,
        tok_sem, own_sem, recv_sem, sent_sem, halo_recv, x_recv, twin_recv, out_recv,
    ) = refs[5:]
    f32, bf16 = jnp.float32, jnp.bfloat16
    me, fs, tp = lax.axis_index("sp"), lax.axis_index("fs"), lax.axis_index("tp")
    low = me < 2
    end = (me == 0) | (me == 3)
    middle = jnp.logical_not(end)
    mate = me + 1 - 2 * lax.rem(me, 2)
    peer = jnp.where(end, 3 - mate, 3 - me)
    far = jnp.where(low, 3, 0)
    first = jnp.where(low, 0, 1)
    has_left, has_right = me > 0, me < 3
    right = jnp.minimum(me + 1, 3)
    across, along = fs + 1 - 2 * lax.rem(fs, 2), lax.rem(fs + 2, 4)
    diagonal = 3 - fs
    twin = 1 - tp
    rows = tok.shape[0]
    depth = shards[2].shape[0]
    blocks = rows // WINDOW
    width = q_all.shape[1]
    widths = (width // 4, width // 4, width * 5 // 16, width // 8, width // 16)
    groups = range(len(widths))
    channel = [sum(widths[:g]) for g in groups]
    K, V, Q, R, A, B, C, D, E = units = range(9)

    parts = 8
    part_rows = rows // parts
    pieces = 4
    piece = part_rows // pieces
    own_part = fs * 2 + tp

    def part_at(i):
        return lax.rem(own_part + i, parts)

    def rows_of(start, length):
        return pl.ds(pl.multiple_of(start, 16), length)

    tok_copies = []
    for i in range(parts):
        at = rows_of(part_at(i) * part_rows, part_rows)
        tok_copies.append(pltpu.make_async_copy(tok_ref.at[at], tok.at[at], tok_sem.at[min(i, 1)]))

    def shard_at(shard):
        return pl.ds(pl.multiple_of(shard * depth, depth), depth)

    def place(u, shard):
        at = shard_at(shard)
        if u < Q:
            return kv_all.at[pl.ds(u * HEAD_DIM, HEAD_DIM), at]
        if u < A:
            return q_all.at[at, pl.ds((u - Q) * LANES, LANES)]
        return conv_w.at[pl.ds(2 * channel[u - A], 2 * widths[u - A]), at]

    own_copies = [pltpu.make_async_copy(shards[u], place(u, me), own_sem.at[0]) for u in (K, V)]
    own_copies.append(pltpu.make_async_copy(shards[2], q_all.at[shard_at(me)], own_sem.at[1]))
    own_copies += [pltpu.make_async_copy(shards[3 + j], stage.at[j], own_sem.at[2]) for j in range(2)]
    small_copies = [
        pltpu.make_async_copy(src, dst, own_sem.at[3 + j])
        for j, (src, dst) in enumerate(((gain_in, gain_ref), (taps_in, taps_ref), (sink_in, sink_ref)))
    ]
    for copy in small_copies[:1] + tok_copies[:1] + own_copies + small_copies[1:] + tok_copies[1:]:
        copy.start()

    def norm_part(i):
        norm_rows = 64

        @pl.loop(0, part_rows // norm_rows)
        def _(j):
            at = rows_of(part_at(i) * part_rows + j * norm_rows, norm_rows)
            wide = tok[at, :].astype(f32)
            scale = lax.rsqrt(jnp.mean(wide * wide, axis=-1, keepdims=True) + EPS)
            normed[at, :] = (wide * scale * gain_ref[...]).astype(bf16)

    barrier = pltpu.get_barrier_semaphore()

    def greet(**device):
        pl.semaphore_signal(barrier, inc=1, device_id=device, device_id_type=MESH)

    greet(sp=mate)

    @pl.when(middle)
    def _():
        greet(sp=peer)
        greet(fs=across)
        greet(fs=along)
        greet(tp=twin)


    TO_MATE, TO_PEER, RELAYED, RETURNED, EDGES, HALO = range(6)

    def slot(shard, device):
        return shard - jnp.where(shard > device, 1, 0)

    def source(u):
        return shards[u] if u < Q else shards[2].at[:, pl.ds((u - Q) * LANES, LANES)]

    def hop(u, shard, to_mate):
        target = mate if to_mate else peer
        return pltpu.make_async_remote_copy(
            src_ref=source(u) if shard is me and u < A else place(u, shard),
            dst_ref=place(u, shard),
            send_sem=sent_sem.at[TO_MATE if to_mate else TO_PEER],
            recv_sem=recv_sem.at[u, slot(shard, target)],
            device_id={"sp": target},
            device_id_type=MESH,
        )

    def arrived(u, shard):
        ref = place(u, shard)
        pltpu.make_async_copy(ref, ref, recv_sem.at[u, slot(shard, me)]).wait()

    def drain(kind, elements):
        ref = other.at[pl.ds(0, elements // other.shape[1])]
        pltpu.make_async_copy(ref, ref, sent_sem.at[kind]).wait()

    def piece_at(part, h):
        return rows_of(part * part_rows + h * piece, piece)

    def piece_copy(buffer, part, h, kind, arrival, **device):
        at = piece_at(part, h)
        return pltpu.make_async_remote_copy(
            src_ref=buffer.at[at],
            dst_ref=other.at[at],
            send_sem=sent_sem.at[kind],
            recv_sem=arrival,
            device_id=device,
            device_id_type=MESH,
        )

    def line_sem(part, h):
        return x_recv.at[part // 2, h]

    def piece_arrived(part, h):
        ref = other.at[piece_at(part, h)]
        pltpu.make_async_copy(ref, ref, line_sem(part, h)).wait()

    across_part, along_part, diagonal_part = across * 2 + tp, along * 2 + tp, diagonal * 2 + tp
    relays = [(own_part, h, ("tp", "fs_across", "fs_along")) for h in range(pieces)]
    relays += [(across_part, h, ("tp", "fs_along")[: 2 - h % 2]) for h in range(pieces)]
    relays += [(along_part, h, ("tp", "fs_across")[: 1 + h % 2]) for h in range(pieces)]
    relays += [(diagonal_part, h, ("tp",)) for h in range(pieces)]
    OWN_X, ACROSS, ALONG, DIAGONAL = (pieces * j for j in range(4))
    devices = {"tp": {"tp": twin}, "fs_across": {"fs": across}, "fs_along": {"fs": along}}

    def relay_copies(j):
        part, h, to = relays[j]
        return [
            piece_copy(other, part, h, RELAYED, twin_recv.at[0] if d == "tp" else line_sem(part, h), **devices[d])
            for d in to
        ]

    def relay(*which):
        for j in which:
            piece_arrived(relays[j][0], relays[j][1])
            for copy in relay_copies(j):
                copy.start()

    def send(to_mate, shard, *which):
        for u in which:
            hop(u, shard, to_mate).start()

    def forward(to_mate, shard, *which):
        for u in which:
            arrived(u, shard)
            hop(u, shard, to_mate).start()

    def pieces_out(*which):
        for h in which:
            piece_copy(normed, own_part, h, RELAYED, line_sem(own_part, h), sp=mate).start()

    pl.semaphore_wait(barrier, jnp.where(middle, 5, 1))

    @pl.when(middle)
    def _():
        send(False, me, K, V, Q, R)
        send(True, me, K, V, Q, R)

    small_copies[0].wait()
    tok_copies[0].wait()
    norm_part(0)

    @pl.when(end)
    def _():
        pieces_out(*range(pieces))
        send(True, me, K, V, Q, R)

    pltpu.make_async_copy(stage, stage, own_sem.at[2]).wait()
    for j in range(2):
        for block in range(depth // LANES):
            turned = jnp.transpose(stage[j, pl.ds(block * LANES, LANES), :].astype(f32)).astype(bf16)
            at = pl.ds(pl.multiple_of(me * depth + block * LANES, LANES), LANES)
            for g in groups:
                to = pl.ds(2 * channel[g] + j * widths[g], widths[g])
                conv_w[to, at] = turned[channel[g] : channel[g] + widths[g]]
    small_copies[1].wait()
    small_copies[2].wait()
    taps = taps_ref[...].astype(f32)
    turned_taps[...] = jnp.transpose(jnp.concatenate([taps, jnp.zeros((8 - TAPS, width), f32)], axis=0))
    conv_in[:, pl.ds(0, LANES)] = jnp.zeros((width, LANES), f32)

    @pl.when(end)
    def _():
        send(True, me, A, B, C)

    @pl.when(middle)
    def _():
        send(False, me, A, B, C)

    own_kv = kv_all.at[:, shard_at(me)]
    pltpu.make_async_copy(own_kv, own_kv, own_sem.at[0]).wait()
    own_copies[2].wait()

    others = tok.at[pl.ds(0, rows - part_rows)]
    pltpu.make_async_copy(others, others, tok_sem.at[1]).wait()
    for i in range(1, parts):
        norm_part(i)

    tile = 512

    early = pl.ds(pl.multiple_of(first * depth, depth), 3 * depth)
    late = pl.ds(pl.multiple_of(far * depth, depth), depth)

    kv_halo = pltpu.make_async_remote_copy(
        src_ref=kv.at[pl.ds(rows, WINDOW)],
        dst_ref=kv.at[pl.ds(0, WINDOW)],
        send_sem=sent_sem.at[HALO],
        recv_sem=halo_recv.at[0],
        device_id={"sp": right},
        device_id_type=MESH,
    )

    own_base, mate_base = jnp.where(me == 1, rows, 0), jnp.where(me == 1, 0, rows)
    bases = (own_base, mate_base)
    sources = (normed, other)
    tiles = rows // tile
    OWN, MATE = 0, 1

    def tile_at(i):
        return pl.ds(i * tile if isinstance(i, int) else pl.multiple_of(i * tile, tile), tile)

    def out_copy(g, i):
        at = (pl.ds(channel[g], widths[g]), tile_at(i))
        return pltpu.make_async_remote_copy(
            src_ref=conv_out.at[at],
            dst_ref=conv_back.at[at],
            send_sem=sent_sem.at[RETURNED],
            recv_sem=out_recv.at[channel[g] // LANES * tiles + i],
            device_id={"sp": mate},
            device_id_type=MESH,
        )

    def edge_copy(g):
        return pltpu.make_async_remote_copy(
            src_ref=edge_out.at[g],
            dst_ref=edge_in.at[g],
            send_sem=sent_sem.at[EDGES],
            recv_sem=halo_recv.at[1],
            device_id={"sp": right},
            device_id_type=MESH,
        )

    center = pl.ds(depth, 2 * depth)
    everything = pl.ds(0, conv_w.shape[1])
    edge_tokens = pl.ds(rows - LANES, LANES)

    def dot(which, tokens, start, length, at):
        return lax.dot_general(
            conv_w[pl.ds(start, length), at],
            sources[which][tokens, at],
            (((1,), (1,)), ((), ())),
            preferred_element_type=f32,
        )

    def partial(which, i, u, v, at, fresh=False):
        start = 2 * channel[u - A]
        span = pl.ds(start, 2 * channel[v - A] + 2 * widths[v - A] - start)
        value = dot(which, tile_at(i), span.start, span.size, at)
        sums[which, span, tile_at(i)] = value if fresh else sums[which, span, tile_at(i)] + value

    def product(which, tokens, start, length):
        if which == OWN and start >= 2 * channel[3] and tokens is not edge_tokens:
            return dot(which, tokens, start, length, everything)
        return sums[which, pl.ds(start, length), tokens] + dot(which, tokens, start, length, late)

    def keep(g, at, value):
        value = value.astype(bf16).astype(f32)
        conv_in[pl.ds(channel[g], widths[g]), pl.ds(pl.multiple_of(at + LANES, LANES), value.shape[1])] = value[: widths[g]]
        return value[widths[g] :]

    def convolve(g, at, gate):
        of = pl.ds(channel[g], widths[g])
        near = conv_in[of, pl.ds(pl.multiple_of(at, LANES), tile + LANES)]
        total = jnp.zeros((widths[g], tile), f32)
        for k in range(TAPS):
            moved = near if k == TAPS - 1 else pltpu.roll(near, TAPS - 1 - k, 1)
            total = total + turned_taps[of, k : k + 1] * moved[:, LANES:]
        return gate * total

    def mate_tiles(g):
        of = pl.ds(channel[g], widths[g])
        keep(g, own_base + rows - LANES, product(OWN, edge_tokens, 2 * channel[g], 2 * widths[g]))
        step = 1 if g < 3 else tiles
        for start in range(0, tiles, step):
            these = range(start, start + step)
            values = [product(MATE, tile_at(i), 2 * channel[g], 2 * widths[g]) for i in these]
            made = [keep(g, mate_base + i * tile, value) for i, value in zip(these, values)]
            for i, gate in zip(these, made):
                conv_out[of, tile_at(i)] = convolve(g, mate_base + i * tile, gate).astype(bf16)
                out_copy(g, i).start()

        @pl.when(me == 1)
        def _():
            edge = jnp.transpose(conv_in[of, pl.ds(2 * rows, LANES)])
            edge_out[g, :, pl.ds(0, widths[g])] = edge[LANES - PAD :]
            edge_copy(g).start()

    def own_tiles(*which):
        @pl.when(me == 2)
        def _():
            for g in which:
                of = pl.ds(channel[g], widths[g])
                edge = edge_in[g, :, pl.ds(0, widths[g])]
                edge = jnp.concatenate([jnp.zeros((LANES - PAD, widths[g]), f32), edge], axis=0)
                conv_in[of, pl.ds(0, LANES)] = jnp.transpose(edge)

        start = 2 * channel[which[0]]
        length = sum(2 * widths[g] for g in which)
        for i in range(tiles):
            at = own_base + i * tile
            value = product(OWN, tile_at(i), start, length)
            for g in which:
                row = 2 * channel[g] - start
                gate = keep(g, at, value[row : row + 2 * widths[g]])
                convolved[pl.ds(channel[g], widths[g]), tile_at(i)] = convolve(g, at, gate)

    def mix(half, i, source):
        cols = pl.ds(half * LANES, LANES)
        for j in range(tile // LANES):
            at = pl.ds(i * tile + j * LANES, LANES)
            extra = jnp.transpose(source[cols, at].astype(f32))
            mixed_ref[at, cols] = (attended[at, cols] + extra).astype(bf16)

    @pl.when(middle)
    def _():
        relay(OWN_X)
        forward(True, peer, K, V)
        relay(OWN_X + 1)
        forward(True, peer, Q)
        relay(ACROSS, ALONG)
        forward(True, peer, R)
        relay(OWN_X + 2, ACROSS + 1, ALONG + 1, OWN_X + 3)
        forward(False, mate, K, V)
        relay(ACROSS + 2, ALONG + 2)
        forward(False, mate, Q)
        relay(DIAGONAL, DIAGONAL + 1)
        forward(False, mate, R)
        for u in (A, B, C):
            arrived(u, peer)
        partial(OWN, 0, A, C, center, True)
        relay(ACROSS + 3, ALONG + 3)
        forward(True, far, K, V)
        forward(False, mate, A)

    @pl.when(end)
    def _():
        for shard in (mate, peer, far):
            for u in (K, V):
                arrived(u, shard)

    @pl.loop(0, rows // tile)
    def _(i):
        base = pl.multiple_of(i * tile, tile)
        kv[pl.ds(base + WINDOW, tile), :] = lax.dot_general(
            normed[pl.ds(base, tile), :], kv_all[...], (((1,), (1,)), ((), ())), preferred_element_type=f32
        ).astype(bf16)

    @pl.when(jnp.logical_not(has_left))
    def _():
        kv[pl.ds(0, WINDOW), :] = jnp.zeros((WINDOW, kv.shape[1]), bf16)

    @pl.when(has_right)
    def _():
        kv_halo.start()

    @pl.when(middle)
    def _():
        forward(True, far, Q)
        partial(OWN, 1, A, C, center, True)
        forward(False, mate, B)

    @pl.when(end)
    def _():
        send(True, me, D, E)
        for u in (Q, R):
            arrived(u, mate)
            arrived(u, peer)

    @pl.loop(0, rows // tile)
    def _(i):
        at = pl.ds(pl.multiple_of(i * tile, tile), tile)
        q_part[at, :] = jnp.dot(normed[at, early], q_all[early, :], preferred_element_type=f32)

    @pl.when(middle)
    def _():
        forward(True, far, R)

    @pl.when(end)
    def _():
        arrived(Q, far)
        arrived(R, far)

    @pl.loop(0, rows // tile)
    def _(i):
        at = pl.ds(pl.multiple_of(i * tile, tile), tile)
        query[at, :] = (
            q_part[at, :] + jnp.dot(normed[at, late], q_all[late, :], preferred_element_type=f32)
        ).astype(bf16)

    heads = query.shape[1] // HEAD_DIM
    query_idx = lax.broadcasted_iota(jnp.int32, (WINDOW, 2 * WINDOW), 0)
    key_idx = lax.broadcasted_iota(jnp.int32, (WINDOW, 2 * WINDOW), 1)
    gap = query_idx + WINDOW - key_idx
    band = (gap >= 0) & (gap < WINDOW)
    low_lanes = lax.broadcasted_iota(jnp.int32, (2 * WINDOW, LANES), 1) < HEAD_DIM
    lane = lax.broadcasted_iota(jnp.int32, (WINDOW, LANES), 1)
    low_half = lane < HEAD_DIM

    def attend(b, kept):
        base = pl.multiple_of(b * WINDOW, WINDOW)
        both = kv[pl.ds(base, 2 * WINDOW), :].astype(f32)
        turned = pltpu.roll(both, HEAD_DIM, 1)
        zero, one = jnp.zeros_like(both), jnp.ones_like(both)

        def lower(x):
            return jnp.where(low_lanes, x, zero)

        def upper(x):
            return jnp.where(low_lanes, zero, x)

        keys = jnp.concatenate([lower(both), upper(turned)], axis=0).astype(bf16)
        vals = jnp.concatenate([lower(turned), upper(both)], axis=0)
        ones = jnp.concatenate([lower(one), upper(one)], axis=0)
        vals = jnp.concatenate([vals, ones], axis=1).astype(bf16)
        stats = []
        for pair in range(heads // 2):
            cols = pl.ds(pair * LANES, LANES)
            scores = lax.dot_general(
                query[pl.ds(base, WINDOW), cols], keys, (((1,), (1,)), ((), ())), preferred_element_type=f32
            )
            sinks = [sink_ref[2 * pair + side] * LOG2_E for side in range(2)]
            tops, raised = [], []
            for side in range(2):
                part = scores[:, side * 2 * WINDOW : (side + 1) * 2 * WINDOW] * (HEAD_DIM ** (-0.5) * LOG2_E)
                part = jnp.where(kept, part, -jnp.inf)
                tops.append(jnp.maximum(jnp.max(part, axis=-1, keepdims=True), sinks[side]))
                raised.append(jnp.exp2(part - tops[side]).astype(bf16))
            out = jnp.dot(jnp.concatenate(raised, axis=1), vals, preferred_element_type=f32)
            top = jnp.where(low_half, tops[0], tops[1])
            total = out[:, LANES:] + jnp.exp2(jnp.where(low_half, sinks[0], sinks[1]) - top)
            attended[pl.ds(base, WINDOW), cols] = out[:, :LANES] / total
            stats.append(top * LN_2 + jnp.log(total))
        turned_stats = jnp.transpose(jnp.where(lax.rem(lane, 2) == 0, stats[0], stats[1]))
        for pair in range(2):
            for side in range(2):
                row = pair + side * HEAD_DIM
                head = 2 * pair + side
                log_ref[head : head + 1, pl.ds(base, WINDOW)] = turned_stats[row : row + 1]

    def finish(g):
        arrived(A + g, far)
        mate_tiles(g)

    @pl.when(middle)
    def _():
        relay(DIAGONAL + 2, DIAGONAL + 3)
        half_rows = other.at[pl.ds(0, rows // 2)]
        pltpu.make_async_copy(half_rows, half_rows, twin_recv.at[0]).wait()
        for i in range(tiles):
            partial(MATE, i, A, C, center, True)
        forward(False, mate, C)
        send(False, me, D, E)
        for i in range(tiles):
            partial(MATE, i, A, B, shard_at(mate))
        partial(OWN, tiles - 1, A, B, shard_at(mate))
        finish(0)
        for i in range(tiles - 1):
            partial(OWN, i, A, B, shard_at(mate))

    def attend_pairs(start, stop):
        @pl.loop(start, stop)
        def _(j):
            attend(2 * j + 1, band)
            attend(2 * j + 2, band)

    cut = (blocks // 2 - 1) * 2 // 3
    attend_pairs(0, cut)

    @pl.when(middle)
    def _():
        forward(False, mate, D, E)
        finish(1)

    attend_pairs(cut, blocks // 2 - 1)

    @pl.when(has_left)
    def _():
        kv_halo.wait_recv()

    @pl.when(middle)
    def _():
        for i in range(tiles):
            partial(MATE, i, C, C, shard_at(mate))
        partial(OWN, tiles - 1, C, C, shard_at(mate))
        finish(2)
        arrived(D, peer)
        arrived(E, peer)
        for i in range(tiles):
            partial(MATE, i, D, E, early, True)
        late_rows = pl.ds(2 * channel[3], 2 * (widths[3] + widths[4]))
        sums[OWN, late_rows, edge_tokens] = dot(OWN, edge_tokens, late_rows.start, late_rows.size, early)
        finish(3)
        finish(4)
        for i in range(tiles - 1):
            partial(OWN, i, C, C, shard_at(mate))

    attend(blocks - 1, band)
    attend(0, band & ((key_idx >= WINDOW) | has_left))

    @pl.when(middle)
    def _():
        @pl.when(me == 2)
        def _():
            pltpu.make_async_copy(edge_in, edge_in, halo_recv.at[1]).wait()

        own_tiles(0, 1)
        own_tiles(2)
        own_tiles(3, 4)
        for half in range(2):
            for i in range(tiles):
                mix(half, i, convolved)

    @pl.when(end)
    def _():
        for half in range(2):
            for i in range(tiles):
                back = conv_back.at[pl.ds(half * LANES, LANES), tile_at(i)]
                pltpu.make_async_copy(back, back, out_recv.at[half * tiles + i]).wait()
                mix(half, i, conv_back)

    @pl.when(has_right)
    def _():
        kv_halo.wait_send()

    attention_shard = depth * (2 * HEAD_DIM + width)
    whole_shard = attention_shard + depth * 2 * width

    @pl.when(end)
    def _():
        drain(TO_MATE, whole_shard)
        drain(RELAYED, part_rows * other.shape[1])

    @pl.when(middle)
    def _():
        drain(TO_MATE, 3 * attention_shard)
        drain(TO_PEER, 2 * whole_shard)
        drain(RELAYED, sum(len(to) for _, _, to in relays) * piece * other.shape[1])
        pltpu.make_async_copy(conv_out, conv_out, sent_sem.at[RETURNED]).wait()

        @pl.when(me == 1)
        def _():
            pltpu.make_async_copy(edge_out, edge_out, sent_sem.at[EDGES]).wait()


def paired_body(tokens, norm_gain, w_query, w_key, w_value, w_conv_in, w_conv_gate, conv_taps, sink_logits):
    rows, features = tokens.shape
    width = w_query.shape[1]
    f32, bf16 = jnp.float32, jnp.bfloat16
    hbm = pl.BlockSpec(memory_space=pltpu.HBM)
    vmem = pl.BlockSpec(memory_space=pltpu.VMEM)
    dma = pltpu.SemaphoreType.DMA
    tiles = rows // 512
    results = pl.pallas_call(
        paired_kernel,
        out_shape=(
            pltpu.VMEM((rows, width), bf16),
            pltpu.VMEM((width // HEAD_DIM, rows), f32),
        ),
        in_specs=[hbm] * 9,
        out_specs=(vmem, vmem),
        scratch_shapes=[
            pltpu.VMEM((1, features), f32),
            pltpu.VMEM(conv_taps.shape, bf16),
            pltpu.SMEM((width // HEAD_DIM,), f32),
            pltpu.VMEM((rows, features), bf16),
            pltpu.VMEM((rows, features), bf16),
            pltpu.VMEM((rows, features), bf16),
            pltpu.VMEM((2 * HEAD_DIM, features), bf16),
            pltpu.VMEM((features, width), bf16),
            pltpu.VMEM((2, w_query.shape[0], width), bf16),
            pltpu.VMEM((2 * width, features), bf16),
            pltpu.VMEM((rows + WINDOW, 2 * HEAD_DIM), bf16),
            pltpu.VMEM((rows, width), bf16),
            pltpu.VMEM((rows, width), f32),
            pltpu.VMEM((rows, width), f32),
            pltpu.VMEM((width, LANES + 2 * rows), f32),
            pltpu.VMEM((width, rows), f32),
            pltpu.VMEM((2, 2 * width, rows), f32),
            pltpu.VMEM((width, rows), bf16),
            pltpu.VMEM((width, rows), bf16),
            pltpu.VMEM((width, 8), f32),
            pltpu.VMEM((5, PAD, LANES), f32),
            pltpu.VMEM((5, PAD, LANES), f32),
            dma((2,)),
            dma((6,)),
            dma((9, 3)),
            dma((6,)),
            dma((2,)),
            dma((4, 4)),
            dma((1,)),
            dma((2 * tiles,)),
        ],
        compiler_params=pltpu.CompilerParams(
            collective_id=0, has_side_effects=True, vmem_limit_bytes=59 << 20
        ),
        name="paired_attend_convolve",
    )(tokens, norm_gain.reshape(1, -1), w_key.T, w_value.T, w_query, w_conv_in, w_conv_gate, conv_taps, sink_logits)
    return pl.pallas_call(
        write_out,
        out_shape=(
            jax.ShapeDtypeStruct((rows, width), bf16),
            jax.ShapeDtypeStruct((width // HEAD_DIM, rows), f32),
        ),
        in_specs=[vmem, vmem],
        out_specs=(hbm, hbm),
        scratch_shapes=[dma((2,))],
        name="write_out",
    )(*[pltpu.with_memory_space_constraint(result, pltpu.VMEM) for result in results])


def line_body(n, tokens, norm_gain, w_query, w_key, w_value, w_conv_in, w_conv_gate, conv_taps, sink_logits):
    rows, features = tokens.shape
    width, kv_width = w_query.shape[1], w_key.shape[1] + w_value.shape[1]
    assert w_key.shape[1] == HEAD_DIM and width % LANES == 0
    depth = w_query.shape[0]
    flip = depth % LANES == 0 and 2 < n <= 16
    if flip:
        w_kv, kv_shape = (w_key.T, w_value.T), (kv_width, features)
    else:
        w_kv, kv_shape = (jnp.concatenate([w_key, w_value], axis=1),), (features, kv_width)
    arrays = 3 + len(w_kv)
    f32, bf16 = jnp.float32, jnp.bfloat16
    hbm = pl.BlockSpec(memory_space=pltpu.HBM)
    vmem = pl.BlockSpec(memory_space=pltpu.VMEM)
    smem = pl.BlockSpec(memory_space=pltpu.SMEM)
    dma = pltpu.SemaphoreType.DMA
    return pl.pallas_call(
        functools.partial(line_kernel, n, flip),
        out_shape=(
            pltpu.VMEM((rows, width), bf16),
            pltpu.VMEM((width // HEAD_DIM, rows), f32),
        ),
        in_specs=[hbm, vmem] + [hbm] * arrays + [vmem, smem],
        out_specs=(vmem, vmem),
        scratch_shapes=[
            pltpu.VMEM((rows, features), bf16),
            pltpu.VMEM((rows, features), bf16),
            pltpu.VMEM(kv_shape, bf16),
            pltpu.VMEM((features, width), bf16),
            pltpu.VMEM((features, width), bf16),
            pltpu.VMEM((features, width), bf16),
            pltpu.VMEM((rows + WINDOW, kv_width), bf16),
            pltpu.VMEM((rows, width), bf16),
            pltpu.VMEM((rows, width), f32),
            pltpu.VMEM((rows + PAD, width), f32),
            pltpu.VMEM((rows, width), f32),
            dma((4,)),
            dma((arrays,)),
            dma((arrays, n)),
            dma((arrays, n)),
            dma((arrays, n)),
            dma((2,)),
            dma((2,)),
        ],
        compiler_params=pltpu.CompilerParams(
            collective_id=0, has_side_effects=True, vmem_limit_bytes=59 << 20
        ),
        name="gather_attend_convolve",
    )(tokens, norm_gain.reshape(1, -1), *w_kv, w_query, w_conv_in, w_conv_gate, conv_taps, sink_logits)


def body(n, fs, tp, *arrays):
    rows, width, depth = arrays[0].shape[0], arrays[2].shape[1], arrays[2].shape[0]
    square = n == 4 and fs == 4 and tp == 2
    if square and width == 2 * LANES and depth % LANES == 0 and rows % (8 * LANES) == 0:
        return paired_body(*arrays)
    return line_body(n, *arrays)


def solution(mesh):
    return jax.shard_map(
        functools.partial(body, mesh.shape["sp"], mesh.shape["fs"], mesh.shape["tp"]),
        mesh=mesh,
        in_specs=(
            P("sp", None),
            P(),
            P("sp", ("fs", "tp")),
            P("sp", ("fs", "tp")),
            P("sp", ("fs", "tp")),
            P("sp", ("fs", "tp")),
            P("sp", ("fs", "tp")),
            P(None, ("fs", "tp")),
            P(("fs", "tp")),
        ),
        out_specs=(P("sp", ("fs", "tp")), P(("fs", "tp"), "sp")),
        check_vma=False,
    )
```
